32 devices in a mesh: grp: 2 (over y), sp: 4 (over z), tp: 4 (over x, core).
Axes of the slice: x: 2, y: 2, z: 4, core: 2. Of those that a mesh axis runs over, the one named last changes fastest.
Arguments:
- latent: bfloat16 [12288, 2048], P(('grp', 'sp')), parts along dimension 0, may hold values from -6 to 6
- condition: bfloat16 [4096], P('grp'), parts along dimension 0, may hold values from -6 to 6
- context_tokens: bfloat16 [512, 2048], P(('grp', 'sp')), parts along dimension 0, may hold values from -6 to 6
- context_condition: bfloat16 [2048], replicated, may hold values from -6 to 6
- shift_weight: bfloat16 [2048, 2048], P('sp', 'tp'), may hold values from -0.25 to 0.25
- scale_weight: bfloat16 [2048, 2048], P('sp', 'tp'), may hold values from -0.25 to 0.25
- gate_weight: bfloat16 [2048, 2048], P('sp', 'tp'), may hold values from -0.25 to 0.25
- norm_gain: bfloat16 [2048], replicated, may hold values from 0.099609375 to 1.8984375
- query_weight: bfloat16 [2048, 1024], P(None, 'tp'), may hold values from -0.125 to 0.125
- key_weight: bfloat16 [2048, 1024], P(None, 'tp'), may hold values from -0.125 to 0.125
- value_weight: bfloat16 [2048, 1024], P(None, 'tp'), may hold values from -0.125 to 0.125
- out_weight: bfloat16 [1024, 2048], replicated, may hold values from -0.1875 to 0.1875
- offset_bias: float32 [16, 15, 31], P('tp'), may hold values from 0.5 to 260
Outputs:
- mixed_latent: bfloat16 [12288, 2048], P(('grp', 'sp', 'tp')), parts along dimension 0
The draws below stay inside these ranges and needn't reach their ends.
There are 2 independent parts, one for each index of `grp`. The reference program is written for one: setup_inputs(seed, part) draws one part's arguments, and reference() takes and returns one part's arrays. A program takes and returns all parts, laid end to end along the dimension named above; an argument that names none is the same for every part. Nothing has to cross between parts.
All inputs are finite; a program needn't handle non-finite values.
Results may differ from the reference program's by a relative error of at most 0.011.
Values may be sent and summed in bfloat16 or wider, within the bound.
A program may use at most 192 MiB of HBM per device.

```python
import jax
import jax.numpy as jnp
import numpy as np
from jax import lax

D = 2048
HEADS = 16
HEAD_DIM = 64
ATT = 1024
GRID_W = 64
WIN_ROWS = 8
WIN_COLS = 16
COL_BLOCK = 16
CTX = 256
TOKENS = 6144


def draw_offset_bias(key, part):
    keys_all = jax.random.split(key, 1)
    table_shape = (HEADS, 2 * WIN_ROWS - 1, 2 * WIN_COLS - 1)
    bias_table = jax.random.uniform(keys_all[0], table_shape, jnp.float32, 0.5, 2.5)
    return bias_table


def shard_levels(key, dims, cuts, least, top_value):
    level, own = 1.0, jax.random.fold_in(key, 6)
    for dim, blocks in cuts:
        steps = jnp.exp(jax.random.uniform(jax.random.fold_in(own, dim), (blocks,), jnp.float32, least / len(cuts), top_value / len(cuts)))
        level = level * jnp.repeat(steps, dims[dim] // blocks).reshape([-1 if axis == dim else 1 for axis in range(len(dims))])
    return level


def centred(stream_key, shape, width, limit, cuts=(), kind=jnp.bfloat16):
    loudness = shard_levels(stream_key, shape, cuts, -0.22, 0.18) if cuts else 1.0
    array = jax.random.normal(stream_key, shape, jnp.float32) * width * loudness
    return jnp.minimum(jnp.maximum(array, -limit), limit).astype(kind)


def setup_inputs(seed: int = 0, part: int = 0) -> dict:
    key_of = jax.random.split(jax.random.key(seed), 14)
    part_keys = jax.random.split(jax.random.fold_in(key_of[13], part), 14)
    return {
        "latent": centred(part_keys[0], (TOKENS, D), 1.0, 6.0, ((0, 4),)),
        "condition": centred(part_keys[1], (D,), 1.0, 6.0),
        "context_tokens": centred(part_keys[2], (CTX, D), 1.0, 6.0, ((0, 4),)),
        "context_condition": centred(key_of[3], (D,), 1.0, 6.0),
        "shift_weight": centred(key_of[4], (D, D), (D // 4) ** -0.5, 0.25, ((0, 4), (1, 4))),
        "scale_weight": centred(key_of[5], (D, D), (D // 4) ** -0.5, 0.25, ((0, 4), (1, 4))),
        "gate_weight": centred(key_of[6], (D, D), (D // 4) ** -0.5, 0.25, ((0, 4), (1, 4))),
        "norm_gain": jnp.clip(1.0 + 0.18 * jax.random.normal(key_of[7], (D,), jnp.float32), 0.099609375, 1.8984375).astype(jnp.bfloat16),
        "query_weight": centred(key_of[8], (D, ATT), D ** -0.5, 0.125, ((1, 4),)),
        "key_weight": centred(key_of[9], (D, ATT), D ** -0.5, 0.125, ((1, 4),)),
        "value_weight": centred(key_of[10], (D, ATT), D ** -0.5, 0.125, ((1, 4),)),
        "out_weight": centred(key_of[11], (ATT, D), ATT ** -0.5, 0.1875),
        "offset_bias": draw_offset_bias(jax.random.fold_in(key_of[13], 71), part),
    }


epsilon = 1e-06
masked_score = -1e+30

def column_tables():
    block_count = GRID_W // COL_BLOCK
    strip_width = COL_BLOCK + WIN_COLS
    query_column = np.arange(GRID_W).reshape(block_count, COL_BLOCK)
    strip_start = np.clip(np.arange(block_count) * COL_BLOCK - WIN_COLS // 2, 0, GRID_W - strip_width)
    key_column = strip_start[:, None] + np.arange(strip_width)
    window_start = np.clip(query_column - WIN_COLS // 2, 0, GRID_W - WIN_COLS)
    inside = (key_column[:, None, :] >= window_start[..., None]) & (key_column[:, None, :] < window_start[..., None] + WIN_COLS)
    column_offset = np.clip(key_column[:, None, :] - query_column[..., None] + WIN_COLS - 1, 0, 2 * WIN_COLS - 2)
    return (strip_start, inside, column_offset)

def modulate_rows(tokens, norm_gain, shift_vector, scale_vector):
    values = tokens.astype(jnp.float32)
    normed = values * lax.rsqrt(lax.optimization_barrier(jnp.mean(values * values, axis=-1, keepdims=True)) + epsilon)
    return (normed * norm_gain.astype(jnp.float32) * (1.0 + scale_vector) + shift_vector).astype(jnp.bfloat16)

def neighbour_attention(queries, key_rows, value_rows, context_keys, context_values, offset_bias):
    heads_total = offset_bias.shape[0]
    grid_rows = queries.shape[0] // GRID_W
    block_count = GRID_W // COL_BLOCK
    strip_width = COL_BLOCK + WIN_COLS
    strip_start, inside, column_offset = column_tables()
    query_grid = queries.astype(jnp.float32).reshape(grid_rows, block_count, COL_BLOCK, heads_total, HEAD_DIM)
    key_grid = key_rows.astype(jnp.float32).reshape(grid_rows, GRID_W, heads_total, HEAD_DIM)
    value_grid = value_rows.astype(jnp.float32).reshape(grid_rows, GRID_W, heads_total, HEAD_DIM)
    far_keys = context_keys.astype(jnp.float32).reshape(-1, heads_total, HEAD_DIM)
    far_values = context_values.astype(jnp.float32).reshape(-1, heads_total, HEAD_DIM)
    factor = HEAD_DIM ** (-0.5)
    bias_table = offset_bias.astype(jnp.float32)

    def one_row(grid_row):
        first_row = jnp.clip(grid_row - WIN_ROWS // 2, 0, grid_rows - WIN_ROWS)
        key_window = lax.dynamic_slice_in_dim(key_grid, first_row, WIN_ROWS, 0)
        value_window = lax.dynamic_slice_in_dim(value_grid, first_row, WIN_ROWS, 0)
        key_strip = jnp.stack([key_window[:, int(column_begin):int(column_begin) + strip_width] for column_begin in strip_start], axis=1)
        value_strip = jnp.stack([value_window[:, int(column_begin):int(column_begin) + strip_width] for column_begin in strip_start], axis=1)
        query_row = lax.dynamic_index_in_dim(query_grid, grid_row, 0, keepdims=False)
        row_offset = first_row + jnp.arange(WIN_ROWS, dtype=jnp.int32) - grid_row + WIN_ROWS - 1
        bias_rows = bias_table[:, row_offset]
        bias_full = bias_rows[:, :, column_offset]
        near_scores = jnp.einsum('nqhd,wnkhd->hnqwk', query_row, key_strip) * factor + jnp.transpose(bias_full, (0, 2, 3, 1, 4))
        near_scores = jnp.where(inside[None, :, :, None, :], near_scores, masked_score)
        far_scores = jnp.einsum('nqhd,chd->hnqc', query_row, far_keys) * factor
        score_peak = jnp.maximum(lax.optimization_barrier(jnp.max(near_scores, axis=(3, 4))), lax.optimization_barrier(jnp.max(far_scores, axis=3)))
        near_exp = jnp.exp(near_scores - score_peak[..., None, None])
        far_exp = jnp.exp(far_scores - score_peak[..., None])
        denominator = lax.optimization_barrier(jnp.sum(near_exp, axis=(3, 4))) + lax.optimization_barrier(jnp.sum(far_exp, axis=3))
        near_weights = (near_exp / denominator[..., None, None]).astype(jnp.bfloat16).astype(jnp.float32)
        far_weights = (far_exp / denominator[..., None]).astype(jnp.bfloat16).astype(jnp.float32)
        output = jnp.einsum('hnqwk,wnkhd->nqhd', near_weights, value_strip) + jnp.einsum('hnqc,chd->nqhd', far_weights, far_values)
        return output.astype(jnp.bfloat16).reshape(GRID_W, heads_total * HEAD_DIM)
    rows_out = lax.map(one_row, jnp.arange(grid_rows, dtype=jnp.int32))
    return rows_out.reshape(grid_rows * GRID_W, heads_total * HEAD_DIM)

def reference(latent, condition, context_tokens, context_condition, shift_weight, scale_weight, gate_weight, norm_gain, query_weight, key_weight, value_weight, out_weight, offset_bias):
    cond_act = jax.nn.silu(condition.astype(jnp.float32)).astype(jnp.bfloat16)
    context_act = jax.nn.silu(context_condition.astype(jnp.float32)).astype(jnp.bfloat16)
    shift_vector = jnp.dot(cond_act, shift_weight, preferred_element_type=jnp.float32)
    scale_vector = jnp.dot(cond_act, scale_weight, preferred_element_type=jnp.float32)
    gate_vector = jnp.dot(cond_act, gate_weight, preferred_element_type=jnp.float32)
    context_shift = jnp.dot(context_act, shift_weight, preferred_element_type=jnp.float32)
    context_scale = jnp.dot(context_act, scale_weight, preferred_element_type=jnp.float32)
    hidden = modulate_rows(latent, norm_gain, shift_vector, scale_vector)
    context_hidden = modulate_rows(context_tokens, norm_gain, context_shift, context_scale)
    queries = jnp.dot(hidden, query_weight, preferred_element_type=jnp.float32).astype(jnp.bfloat16)
    key_rows = jnp.dot(hidden, key_weight, preferred_element_type=jnp.float32).astype(jnp.bfloat16)
    value_rows = jnp.dot(hidden, value_weight, preferred_element_type=jnp.float32).astype(jnp.bfloat16)
    context_keys = jnp.dot(context_hidden, key_weight, preferred_element_type=jnp.float32).astype(jnp.bfloat16)
    context_values = jnp.dot(context_hidden, value_weight, preferred_element_type=jnp.float32).astype(jnp.bfloat16)
    attended = neighbour_attention(queries, key_rows, value_rows, context_keys, context_values, offset_bias)
    branch = jnp.dot(attended, out_weight, preferred_element_type=jnp.float32)
    return (latent.astype(jnp.float32) + gate_vector * branch).astype(jnp.bfloat16)
```

```python
import functools

import jax
import jax.numpy as jnp
from jax import lax
from jax.experimental import pallas as pl
from jax.experimental.pallas import tpu as pltpu
from jax.sharding import PartitionSpec as P

HEAD_DIM = 64
GRID_W = 64
WIN_ROWS = 8
WIN_COLS = 16
HALO = WIN_ROWS // 2
BLOCK = 16
SHIFT = WIN_COLS // 2
STRIP = BLOCK + WIN_COLS
GROUP = 4
KEY_ROWS = GROUP + WIN_ROWS
LANES = 128
SEGMENTS = LANES // STRIP
TILES = KEY_ROWS // SEGMENTS
LOG2E = 1.4426950408889634
epsilon = 1e-06
masked_score = -1e30
F32 = jnp.float32
BF16 = jnp.bfloat16
MESH = pl.DeviceIdType.MESH


def to_peer(src, dst, send, recv, **place):
    return pltpu.make_async_remote_copy(
        src_ref=src, dst_ref=dst, send_sem=send, recv_sem=recv,
        device_id=place, device_id_type=MESH,
    )


def gcd(a, b):
    while b:
        a, b = b, a % b
    return a


def aligned(index, step):
    return pl.multiple_of(index * step, step)


def build_tables(bias_ref, braw, table, heads):
    offsets = bias_ref.shape[0]
    braw[...] = jnp.zeros_like(braw)
    for o in range(offsets):
        braw[o, :, : bias_ref.shape[2]] = bias_ref[o] * LOG2E
    lane_h = lax.broadcasted_iota(jnp.int32, (heads, LANES), 1) // STRIP
    first = HALO - 1
    combined = []
    for o in range(first - (GROUP - 1), first + (TILES - 1) * SEGMENTS + 1):
        row = braw[o]
        for j in range(1, SEGMENTS):
            row = jnp.where(lane_h == j, pltpu.roll(braw[o + j], STRIP * j, 1), row)
        combined.append(row)
    u = lax.broadcasted_iota(jnp.int32, (BLOCK, LANES), 0)
    lane = lax.broadcasted_iota(jnp.int32, (BLOCK, LANES), 1)
    v = lane % STRIP
    inner = (v >= u) & (v < u + WIN_COLS)
    edge = ((u < SHIFT) & (v < WIN_COLS)) | ((u >= SHIFT) & (v >= WIN_COLS))
    for t in range(TILES):
        for i in range(GROUP):
            j = t * SEGMENTS + lane // STRIP
            seen = (j >= i) & (j < i + WIN_ROWS)
            whole = t * SEGMENTS >= i and (t + 1) * SEGMENTS <= i + WIN_ROWS
            source = combined[t * SEGMENTS + GROUP - 1 - i]
            for h in range(heads):
                spread = jnp.broadcast_to(source[h : h + 1, :], (BLOCK, LANES))
                value = pltpu.roll(spread, LANES - (SHIFT - 1), 1, stride=1, stride_axis=0)
                place = slice((h * GROUP + i) * BLOCK, (h * GROUP + i + 1) * BLOCK)
                for kind, mask in enumerate((inner, edge)):
                    full = jnp.where(mask, value, masked_score)
                    table[kind, t, place, :] = (
                        full if whole else jnp.where(seen, full, masked_score)
                    )
                    if t != 1:
                        table[kind, 3 if t == 0 else 4, place, :] = full
    for kind in range(2):
        table[kind, 5] = jnp.full(table.shape[2:], masked_score, F32)


def kernel(
    cond_hbm, ctxcond_hbm, gain_hbm, shift_hbm, scale_hbm, gate_hbm, bias_hbm, ctx_hbm,
    lat_hbm, wq_hbm, wk_hbm, wv_hbm, wo_hbm,
    out_hbm,
    cond, ctxcond, gain, small, modw, bias, braw, table, ctx, cblk, lat, xs, wqkv, wo,
    terms, arrived, gterms, garrived, vectors, inv, q_s, kv, ctx_kv, stage, recv, obuf,
    load_sem, lat_sem, term_send, term_recv, gate_send, gate_recv, halo_send, halo_recv,
    ctx_send, ctx_recv, piece_send, piece_recv, out_sem,
):
    sp, tp = lax.axis_index("sp"), lax.axis_index("tp")
    sp_size, tp_size = lax.axis_size("sp"), lax.axis_size("tp")
    ranks = sp_size * tp_size
    me = sp * tp_size + tp
    tokens, depth = lat.shape
    width = wq_hbm.shape[1]
    heads = width // HEAD_DIM
    input_rows, piece_cols = modw.shape[1:]
    context_rows = ctx.shape[0]
    grid_rows = tokens // GRID_W
    groups = grid_rows // GROUP
    group_tokens = GROUP * GRID_W
    halo = HALO * GRID_W
    below = (HALO - 1) * GRID_W
    share = tokens // tp_size
    piece_rows = gcd(GROUP, share // GRID_W)
    piece = piece_rows * GRID_W
    pieces = share // piece
    per_group = GROUP // piece_rows

    def peer(d):
        other = (me + d) % ranks
        return dict(sp=other // tp_size, tp=other % tp_size)

    barrier = pltpu.get_barrier_semaphore()

    early = [
        pltpu.make_async_copy(cond_hbm, cond, load_sem.at[0]),
        pltpu.make_async_copy(ctxcond_hbm, ctxcond, load_sem.at[1]),
        pltpu.make_async_copy(gain_hbm, gain, load_sem.at[2]),
        pltpu.make_async_copy(shift_hbm, modw.at[0], load_sem.at[3]),
        pltpu.make_async_copy(scale_hbm, modw.at[1], load_sem.at[4]),
        pltpu.make_async_copy(gate_hbm, modw.at[2], load_sem.at[5]),
    ]
    load_bias = pltpu.make_async_copy(bias_hbm, bias, load_sem.at[6])
    load_ctx = pltpu.make_async_copy(ctx_hbm, ctx, load_sem.at[7])
    load_weights = [
        pltpu.make_async_copy(w, wqkv.at[:, pl.ds(i * width, width)], load_sem.at[8 + i])
        for i, w in enumerate((wq_hbm, wk_hbm, wv_hbm))
    ]
    load_wo = pltpu.make_async_copy(wo_hbm, wo, load_sem.at[11])

    def load_lat(i):
        rows = pl.ds(aligned(i, group_tokens), group_tokens)
        return pltpu.make_async_copy(lat_hbm.at[rows], lat.at[rows], lat_sem.at[i])

    for load in early:
        load.start()

    @pl.loop(1, ranks)
    def _(d):
        pl.semaphore_signal(barrier, inc=1, device_id=peer(d), device_id_type=MESH)

    load_bias.start()
    load_ctx.start()

    @pl.loop(0, groups)
    def _(i):
        load_lat(i).start()

    for load in load_weights:
        load.start()
    load_wo.start()

    for load in early:
        load.wait()
    small[0:1, :] = cond[...].astype(F32).reshape(1, depth)
    small[1:2, :] = ctxcond[...].astype(F32).reshape(1, depth)
    small[2:3, :] = gain[...].astype(F32).reshape(1, depth)
    row8 = lax.broadcasted_iota(jnp.int32, (8, input_rows), 0)
    own_inputs = pl.ds(aligned(sp, input_rows), input_rows)
    value = jnp.where(row8 == 0, small[0:1, own_inputs], small[1:2, own_inputs])
    act = (value / (1.0 + jnp.exp(-value))).astype(BF16)
    terms[0:2, :] = jnp.dot(act, modw[0], preferred_element_type=F32)[:2]
    terms[2:4, :] = jnp.dot(act, modw[1], preferred_element_type=F32)[:2]
    gterms[...] = jnp.dot(act, modw[2], preferred_element_type=F32)[:1]
    arrived[me] = terms[...]
    garrived[me] = gterms[...]

    def term_copy(d):
        return to_peer(terms, arrived.at[me], term_send.at[d], term_recv.at[d], **peer(d))

    def gate_copy(d):
        return to_peer(gterms, garrived.at[me], gate_send.at[d], gate_recv.at[d], **peer(d))

    load_bias.wait()
    build_tables(bias, braw, table, heads)
    pl.semaphore_wait(barrier, ranks - 1)

    @pl.loop(1, ranks)
    def _(d):
        term_copy(d).start()

    @pl.when(sp == 0)
    def _():
        kv[0:halo, :] = jnp.zeros((halo, 2 * width), BF16)

    @pl.when(sp == sp_size - 1)
    def _():
        kv[halo + tokens : halo + tokens + below, :] = jnp.zeros((below, 2 * width), BF16)

    kv[halo + tokens + below :, :] = jnp.zeros((halo - below, 2 * width), BF16)

    def inverse_of(x):
        x = x.astype(F32)
        return lax.rsqrt(jnp.mean(x * x, axis=-1, keepdims=True) + epsilon)

    load_ctx.wait()
    inv_ctx = inverse_of(ctx[...])

    @pl.loop(0, groups)
    def _(i):
        load_lat(i).wait()

        @pl.loop(0, group_tokens, step=32)
        def _(r):
            rows = pl.ds(aligned(i, group_tokens) + pl.multiple_of(r, 32), 32)
            inv[rows, :] = jnp.broadcast_to(inverse_of(lat[rows, :]), (32, LANES))

    for load in load_weights:
        load.wait()

    @pl.loop(1, ranks)
    def _(d):
        term_copy(d).wait()

    for t in range(tp_size):
        total = arrived[t]
        for s in range(1, sp_size):
            total = total + arrived[s * tp_size + t]
        vectors[:, t * piece_cols : (t + 1) * piece_cols] = total

    factor = (small[2:3, :] * (1.0 + vectors[2:3, :])).astype(BF16)
    factor_ctx = (small[2:3, :] * (1.0 + vectors[3:4, :])).astype(BF16)
    cblk[:context_rows, :] = ctx[...] * factor_ctx
    row16 = lax.broadcasted_iota(jnp.int32, (16, depth), 0)
    cblk[context_rows:, :] = jnp.where(
        row16 == 0, vectors[0:1, :], jnp.where(row16 == 1, vectors[1:2, :], 0.0)
    ).astype(BF16)
    block = jnp.dot(cblk[...], wqkv[...], preferred_element_type=F32)
    added = block[context_rows : context_rows + 1, :]
    ctx_place = pl.ds(aligned(sp, context_rows), context_rows)
    ctx_kv[ctx_place, :] = (
        block[:context_rows, width:] * inv_ctx
        + block[context_rows + 1 : context_rows + 2, width:]
    ).astype(BF16)

    def ctx_copy(d):
        return to_peer(
            ctx_kv.at[ctx_place], ctx_kv.at[ctx_place], ctx_send.at[d], ctx_recv.at[d],
            sp=(sp + d) % sp_size, tp=tp,
        )

    @pl.loop(1, sp_size)
    def _(d):
        ctx_copy(d).start()

    down = to_peer(
        kv.at[pl.ds(halo, below)], kv.at[pl.ds(halo + tokens, below)],
        halo_send.at[0], halo_recv.at[0], sp=jnp.maximum(sp - 1, 0),
    )
    up = to_peer(
        kv.at[pl.ds(tokens, halo)], kv.at[pl.ds(0, halo)],
        halo_send.at[1], halo_recv.at[1], sp=jnp.minimum(sp + 1, sp_size - 1),
    )

    @pl.loop(0, groups)
    def _(k):
        i = jnp.where(k == 0, 0, jnp.where(k == 1, groups - 1, k - 1))
        rows = pl.ds(aligned(i, group_tokens), group_tokens)
        xs[...] = lat[rows, :] * factor
        y = jnp.dot(xs[...], wqkv[...], preferred_element_type=F32)
        scale = jnp.concatenate([inv[rows, :]] * (3 * width // LANES), axis=1)
        y = y * scale + added
        q = y[:, :width] * (HEAD_DIM**-0.5 * LOG2E)
        turned = []
        for r in range(GROUP):
            turned.append(q[r * GRID_W + SHIFT : (r + 1) * GRID_W])
            turned.append(q[r * GRID_W : r * GRID_W + SHIFT])
        q_s[rows, :] = jnp.concatenate(turned, axis=0).astype(BF16)
        kv[pl.ds(aligned(i, group_tokens) + halo, group_tokens), :] = y[:, width:].astype(BF16)

        @pl.when((k == 0) & (sp > 0))
        def _():
            down.start()

        @pl.when((k == 1) & (sp < sp_size - 1))
        def _():
            up.start()

        @pl.when(k == 1)
        def _():
            @pl.loop(1, ranks)
            def _(d):
                gate_copy(d).start()

    @pl.loop(1, sp_size)
    def _(d):
        ctx_copy(d).wait()

    contract = (((1,), (1,)), ((), ()))
    stack_head = lax.broadcasted_iota(jnp.int32, (GROUP * BLOCK, width), 1) // HEAD_DIM
    blocks = GRID_W // BLOCK

    def attend(g):
        global_row = sp * grid_rows + g * GROUP
        top = global_row == 0
        bottom = global_row == sp_size * grid_rows - GROUP
        slots = (
            jnp.where(top, 5, jnp.where(bottom, 3, 0)), 1,
            jnp.where(top, 4, jnp.where(bottom, 5, 2)),
        )
        base = aligned(g, group_tokens)
        for b in range(blocks):
            kind = 1 if b == blocks - 1 else 0
            places = [
                pl.ds(base + (r * GRID_W + b * BLOCK), BLOCK) for r in range(GROUP)
            ]
            q = jnp.concatenate([q_s[place, :] for place in places], axis=0)
            stacked = jnp.concatenate(
                [jnp.where(stack_head == h, q, jnp.zeros_like(q)) for h in range(heads)], axis=0
            )
            strips = []
            for j in range(KEY_ROWS):
                if kind:
                    strips.append(pl.ds(base + (j * GRID_W + b * BLOCK), BLOCK))
                    strips.append(pl.ds(base + j * GRID_W, BLOCK))
                else:
                    strips.append(pl.ds(base + (j * GRID_W + b * BLOCK), STRIP))
            keys = jnp.concatenate([kv[s, :width] for s in strips], axis=0)
            values = jnp.concatenate([kv[s, width:] for s in strips], axis=0)
            near = lax.dot_general(stacked, keys, contract, preferred_element_type=F32)
            far = lax.dot_general(
                stacked, ctx_kv[:, :width], contract, preferred_element_type=F32
            )
            near = near + jnp.concatenate([table[kind, s] for s in slots], axis=1)
            peak = jnp.maximum(
                jnp.max(near, axis=1, keepdims=True), jnp.max(far, axis=1, keepdims=True)
            )
            near = jnp.exp2(near - peak)
            far = jnp.exp2(far - peak)
            total = jnp.sum(near, axis=1, keepdims=True) + jnp.sum(far, axis=1, keepdims=True)
            mixed = jnp.dot(
                near.astype(BF16), values, preferred_element_type=F32
            ) + jnp.dot(far.astype(BF16), ctx_kv[:, width:], preferred_element_type=F32)
            mixed = mixed * (1.0 / total)
            size = GROUP * BLOCK
            merged = mixed[:size]
            for h in range(1, heads):
                merged = jnp.where(stack_head == h, mixed[h * size : (h + 1) * size], merged)
            merged = merged.astype(BF16)
            for r, place in enumerate(places):
                stage[place, :] = merged[r * BLOCK : (r + 1) * BLOCK]

    def piece_copy(index):
        owner, p = index // pieces, index % pieces
        return to_peer(
            stage.at[pl.ds(aligned(index, piece), piece)],
            recv.at[tp, pl.ds(aligned(p, piece), piece)],
            piece_send.at[index], piece_recv.at[tp, p], tp=owner,
        )

    half = groups // 2
    upper = tp * 2 >= tp_size

    @pl.loop(0, groups)
    def _(k):
        second = k >= half
        j = jnp.where(second, k - half, k)
        low = upper != second
        g = jnp.where(low, (j + 1) % half, half + j)

        @pl.when((g == 0) & (sp > 0))
        def _():
            down.wait_send()
            up.wait_recv()

        @pl.when((g == groups - 1) & (sp < sp_size - 1))
        def _():
            up.wait_send()
            down.wait_recv()

        attend(g)
        for n in range(per_group):
            index = g * per_group + n

            @pl.when(index // pieces != tp)
            def _():
                piece_copy(index).start()

    load_wo.wait()

    @pl.loop(1, ranks)
    def _(d):
        gate_copy(d).wait()

    gates = []
    for t in range(tp_size):
        total = garrived[t]
        for s in range(1, sp_size):
            total = total + garrived[s * tp_size + t]
        gates.append(total)
    gate = jnp.concatenate(gates, axis=1)

    @pl.loop(0, pieces)
    def _(p):
        rows = pl.ds(aligned(p, piece), piece)
        own = pl.ds(aligned(tp * pieces + p, piece), piece)
        recv[tp, rows, :] = stage[own, :]

        @pl.loop(1, tp_size)
        def _(d):
            source = (tp + d) % tp_size
            to_peer(
                stage.at[own], recv.at[source, rows], piece_send.at[0],
                piece_recv.at[source, p], tp=source,
            ).wait_recv()

        mixed = jnp.concatenate([recv[t, rows, :] for t in range(tp_size)], axis=1)
        branch = jnp.dot(mixed, wo[...], preferred_element_type=F32)
        turned = []
        for r in range(piece_rows):
            turned.append(branch[(r + 1) * GRID_W - SHIFT : (r + 1) * GRID_W])
            turned.append(branch[r * GRID_W : (r + 1) * GRID_W - SHIFT])
        branch = jnp.concatenate(turned, axis=0)
        obuf[rows, :] = (lat[own, :].astype(F32) + gate * branch).astype(BF16)
        pltpu.make_async_copy(obuf.at[rows], out_hbm.at[rows], out_sem.at[p]).start()

    @pl.loop(0, pieces)
    def _(p):
        rows = pl.ds(aligned(p, piece), piece)
        pltpu.make_async_copy(obuf.at[rows], out_hbm.at[rows], out_sem.at[p]).wait()

    @pl.loop(0, groups * per_group)
    def _(index):
        @pl.when(index // pieces != tp)
        def _():
            piece_copy(index).wait_send()


def local(
    latent, condition, context_tokens, context_condition, shift_weight, scale_weight,
    gate_weight, norm_gain, query_weight, key_weight, value_weight, out_weight, offset_bias,
):
    sp_size, tp_size = lax.axis_size("sp"), lax.axis_size("tp")
    ranks = sp_size * tp_size
    tokens, depth = latent.shape
    context_rows = context_tokens.shape[0]
    input_rows, piece_cols = shift_weight.shape
    width = query_weight.shape[1]
    heads = width // HEAD_DIM
    groups = tokens // GRID_W // GROUP
    group_tokens = GROUP * GRID_W
    share = tokens // tp_size
    piece_rows = gcd(GROUP, share // GRID_W)
    pieces = share // (piece_rows * GRID_W)
    bias = jnp.transpose(offset_bias, (1, 0, 2))
    dma = pltpu.SemaphoreType.DMA
    vmem = pltpu.VMEM
    hbm = pl.BlockSpec(memory_space=pl.ANY)
    return pl.pallas_call(
        kernel,
        in_specs=[hbm] * 13,
        out_specs=hbm,
        out_shape=jax.ShapeDtypeStruct((share, depth), BF16),
        scratch_shapes=[
            vmem((depth,), BF16), vmem((depth,), BF16), vmem((depth,), BF16),
            vmem((8, depth), F32),
            vmem((3, input_rows, piece_cols), BF16),
            vmem(bias.shape, F32),
            vmem((bias.shape[0], heads, LANES), F32),
            vmem((2, 6, heads * GROUP * BLOCK, LANES), F32),
            vmem((context_rows, depth), BF16),
            vmem((context_rows + 16, depth), BF16),
            vmem((tokens, depth), BF16),
            vmem((group_tokens, depth), BF16),
            vmem((depth, 3 * width), BF16),
            vmem(out_weight.shape, BF16),
            vmem((4, piece_cols), F32),
            vmem((ranks, 4, piece_cols), F32),
            vmem((1, piece_cols), F32),
            vmem((ranks, 1, piece_cols), F32),
            vmem((4, depth), F32),
            vmem((tokens, LANES), F32),
            vmem((tokens, width), BF16),
            vmem((tokens + 2 * HALO * GRID_W, 2 * width), BF16),
            vmem((sp_size * context_rows, 2 * width), BF16),
            vmem((tokens, width), BF16),
            vmem((tp_size, share, width), BF16),
            vmem((share, depth), BF16),
            dma((12,)), dma((groups,)), dma((ranks,)), dma((ranks,)), dma((ranks,)),
            dma((ranks,)), dma((2,)), dma((2,)), dma((sp_size,)), dma((sp_size,)),
            dma((tp_size * pieces,)), dma((tp_size, pieces)), dma((pieces,)),
        ],
        compiler_params=pltpu.CompilerParams(
            vmem_limit_bytes=60 * 2**20, collective_id=0, has_side_effects=True
        ),
        cost_estimate=pl.CostEstimate(
            flops=6 * tokens * depth * width,
            bytes_accessed=2 * (tokens * depth + 3 * depth * width + share * depth),
            transcendentals=0,
        ),
    )(
        condition, context_condition, norm_gain, shift_weight, scale_weight, gate_weight, bias,
        context_tokens, latent, query_weight, key_weight, value_weight, out_weight,
    )


def solution(mesh):
    placed = (
        P(("grp", "sp"), None),
        P("grp"),
        P(("grp", "sp"), None),
        P(),
        P("sp", "tp"),
        P("sp", "tp"),
        P("sp", "tp"),
        P(),
        P(None, "tp"),
        P(None, "tp"),
        P(None, "tp"),
        P(),
        P("tp", None, None),
    )
    return jax.shard_map(
        local, mesh=mesh, in_specs=placed, out_specs=P(("grp", "sp", "tp"), None), check_vma=False
    )
```

```python
import functools

import jax
import jax.numpy as jnp
from jax import lax
from jax.experimental import pallas as pl
from jax.experimental.pallas import tpu as pltpu
from jax.sharding import PartitionSpec as P

HEAD_DIM = 64
GRID_W = 64
WIN_ROWS = 8
WIN_COLS = 16
HALO = WIN_ROWS // 2
BLOCK = 16
SHIFT = WIN_COLS // 2
STRIP = BLOCK + WIN_COLS
GROUP = 4
KEY_ROWS = GROUP + WIN_ROWS
LANES = 128
SEGMENTS = LANES // STRIP
TILES = KEY_ROWS // SEGMENTS
LOG2E = 1.4426950408889634
epsilon = 1e-06
masked_score = -1e30
F32 = jnp.float32
BF16 = jnp.bfloat16
MESH = pl.DeviceIdType.MESH


def to_peer(src, dst, send, recv, **place):
    return pltpu.make_async_remote_copy(
        src_ref=src, dst_ref=dst, send_sem=send, recv_sem=recv,
        device_id=place, device_id_type=MESH,
    )


def gcd(a, b):
    while b:
        a, b = b, a % b
    return a


def aligned(index, step):
    return pl.multiple_of(index * step, step)


def build_tables(bias_ref, braw, table, heads):
    offsets = bias_ref.shape[0]
    braw[...] = jnp.zeros_like(braw)
    for o in range(offsets):
        braw[o, :, : bias_ref.shape[2]] = bias_ref[o] * LOG2E
    lane_h = lax.broadcasted_iota(jnp.int32, (heads, LANES), 1) // STRIP
    first = HALO - 1
    combined = []
    for o in range(first - (GROUP - 1), first + (TILES - 1) * SEGMENTS + 1):
        row = braw[o]
        for j in range(1, SEGMENTS):
            row = jnp.where(lane_h == j, pltpu.roll(braw[o + j], STRIP * j, 1), row)
        combined.append(row)
    u = lax.broadcasted_iota(jnp.int32, (BLOCK, LANES), 0)
    lane = lax.broadcasted_iota(jnp.int32, (BLOCK, LANES), 1)
    v = lane % STRIP
    inner = (v >= u) & (v < u + WIN_COLS)
    edge = ((u < SHIFT) & (v < WIN_COLS)) | ((u >= SHIFT) & (v >= WIN_COLS))
    for t in range(TILES):
        for i in range(GROUP):
            j = t * SEGMENTS + lane // STRIP
            seen = (j >= i) & (j < i + WIN_ROWS)
            whole = t * SEGMENTS >= i and (t + 1) * SEGMENTS <= i + WIN_ROWS
            source = combined[t * SEGMENTS + GROUP - 1 - i]
            for h in range(heads):
                spread = jnp.broadcast_to(source[h : h + 1, :], (BLOCK, LANES))
                value = pltpu.roll(spread, LANES - (SHIFT - 1), 1, stride=1, stride_axis=0)
                place = slice((h * GROUP + i) * BLOCK, (h * GROUP + i + 1) * BLOCK)
                for kind, mask in enumerate((inner, edge)):
                    full = jnp.where(mask, value, masked_score)
                    table[kind, t, place, :] = (
                        full if whole else jnp.where(seen, full, masked_score)
                    )
                    if t != 1:
                        table[kind, 3 if t == 0 else 4, place, :] = full
    for kind in range(2):
        table[kind, 5] = jnp.full(table.shape[2:], masked_score, F32)


def kernel(
    cond_hbm, ctxcond_hbm, gain_hbm, shift_hbm, scale_hbm, gate_hbm, bias_hbm, ctx_hbm,
    lat_hbm, wq_hbm, wk_hbm, wv_hbm, wo_hbm,
    out_ref,
    cond, ctxcond, gain, small, modw, bias, braw, table, ctx, cblk, lat, xs, wqkv, wo,
    cterms, carrived, terms, arrived, gterms, garrived, vectors, inv, q_s, kv, ctx_kv,
    scores, probs, stage, recv, acc,
    load_sem, lat_sem, cterm_send, cterm_recv, term_send, term_recv, gate_send, gate_recv,
    halo_send, halo_recv, ctx_send, ctx_recv, piece_send, piece_recv,
):
    sp, tp = lax.axis_index("sp"), lax.axis_index("tp")
    sp_size, tp_size = lax.axis_size("sp"), lax.axis_size("tp")
    ranks = sp_size * tp_size
    me = sp * tp_size + tp
    tokens, depth = lat.shape
    width = wq_hbm.shape[1]
    heads = width // HEAD_DIM
    input_rows, piece_cols = modw.shape[1:]
    context_rows = ctx.shape[0]
    grid_rows = tokens // GRID_W
    groups = grid_rows // GROUP
    group_tokens = GROUP * GRID_W
    halo = HALO * GRID_W
    below = (HALO - 1) * GRID_W
    share = tokens // tp_size
    piece_rows = gcd(GROUP, share // GRID_W)
    piece = piece_rows * GRID_W
    pieces = share // piece
    per_group = GROUP // piece_rows
    big = xs.shape[0] - 16
    steps = tokens // big

    def peer(d):
        other = (me + d) % ranks
        return dict(sp=other // tp_size, tp=other % tp_size)

    barrier = pltpu.get_barrier_semaphore()

    early = [
        pltpu.make_async_copy(cond_hbm, cond, load_sem.at[0]),
        pltpu.make_async_copy(ctxcond_hbm, ctxcond, load_sem.at[1]),
        pltpu.make_async_copy(gain_hbm, gain, load_sem.at[2]),
        pltpu.make_async_copy(shift_hbm, modw.at[0], load_sem.at[3]),
        pltpu.make_async_copy(scale_hbm, modw.at[1], load_sem.at[4]),
        pltpu.make_async_copy(gate_hbm, modw.at[2], load_sem.at[5]),
    ]
    load_bias = pltpu.make_async_copy(bias_hbm, bias, load_sem.at[6])
    load_ctx = pltpu.make_async_copy(ctx_hbm, ctx, load_sem.at[7])
    load_weights = [
        pltpu.make_async_copy(w, wqkv.at[:, pl.ds(i * width, width)], load_sem.at[8 + i])
        for i, w in enumerate((wq_hbm, wk_hbm, wv_hbm))
    ]
    load_wo = pltpu.make_async_copy(wo_hbm, wo, load_sem.at[11])

    def load_lat(i):
        rows = pl.ds(aligned(i, group_tokens), group_tokens)
        return pltpu.make_async_copy(lat_hbm.at[rows], lat.at[rows], lat_sem.at[i])

    @pl.loop(1, ranks)
    def _(d):
        pl.semaphore_signal(barrier, inc=1, device_id=peer(d), device_id_type=MESH)

    for load in early:
        load.start()

    load_bias.start()
    load_ctx.start()

    @pl.loop(0, groups)
    def _(i):
        load_lat(i).start()

    for load in load_weights:
        load.start()
    load_wo.start()

    for load in early:
        load.wait()
    small[0:1, :] = cond[...].astype(F32).reshape(1, depth)
    small[1:2, :] = ctxcond[...].astype(F32).reshape(1, depth)
    small[2:3, :] = gain[...].astype(F32).reshape(1, depth)
    row8 = lax.broadcasted_iota(jnp.int32, (8, input_rows), 0)
    own_inputs = pl.ds(aligned(sp, input_rows), input_rows)
    value = jnp.where(row8 == 0, small[0:1, own_inputs], small[1:2, own_inputs])
    act = (value / (1.0 + jnp.exp(-value))).astype(BF16)
    for i in range(2):
        both = jnp.dot(act, modw[i], preferred_element_type=F32)
        terms[i : i + 1, :] = both[0:1]
        cterms[i : i + 1, :] = both[1:2]
    gterms[...] = jnp.dot(act, modw[2], preferred_element_type=F32)[:1]
    carrived[me] = cterms[...]
    arrived[me] = terms[...]
    garrived[me] = gterms[...]

    def cterm_copy(d):
        return to_peer(
            cterms, carrived.at[me], cterm_send.at[d], cterm_recv.at[d], **peer(d)
        )

    def term_copy(d):
        return to_peer(terms, arrived.at[me], term_send.at[d], term_recv.at[d], **peer(d))

    def gate_copy(d):
        return to_peer(gterms, garrived.at[me], gate_send.at[d], gate_recv.at[d], **peer(d))

    load_bias.wait()
    build_tables(bias, braw, table, heads)
    pl.semaphore_wait(barrier, ranks - 1)

    @pl.loop(1, ranks)
    def _(d):
        cterm_copy(d).start()

    @pl.loop(1, ranks)
    def _(d):
        term_copy(d).start()

    @pl.when(sp == 0)
    def _():
        kv[0:halo, :] = jnp.zeros((halo, 2 * width), BF16)

    @pl.when(sp == sp_size - 1)
    def _():
        kv[halo + tokens : halo + tokens + below, :] = jnp.zeros((below, 2 * width), BF16)

    kv[halo + tokens + below :, :] = jnp.zeros((halo - below, 2 * width), BF16)

    def inverse_of(ref, rows):
        total = None
        for c in range(depth // LANES):
            x = ref[rows, c * LANES : (c + 1) * LANES].astype(F32)
            total = x * x if total is None else total + x * x
        mean = jnp.sum(total, axis=1, keepdims=True) * (1.0 / depth)
        return lax.rsqrt(mean + epsilon)

    load_ctx.wait()
    inv_ctx = inverse_of(ctx, slice(None))

    @pl.loop(0, groups)
    def _(i):
        load_lat(i).wait()
        for r in range(0, group_tokens, 128):
            rows = pl.ds(aligned(i, group_tokens) + r, 128)
            inv[rows, :] = jnp.broadcast_to(inverse_of(lat, rows), (128, LANES))

    for load in load_weights:
        load.wait()

    def sum_terms(ref, rows):
        for t in range(tp_size):
            total = ref[t]
            for s in range(1, sp_size):
                total = total + ref[s * tp_size + t]
            vectors[rows, t * piece_cols : (t + 1) * piece_cols] = total

    @pl.loop(1, ranks)
    def _(d):
        cterm_copy(d).wait()

    sum_terms(carrived, slice(0, 2))
    row16 = lax.broadcasted_iota(jnp.int32, (16, depth), 0)
    factor_ctx = (small[2:3, :] * (1.0 + vectors[1:2, :])).astype(BF16)
    cblk[:context_rows, :] = ctx[...] * factor_ctx
    cblk[context_rows:, :] = jnp.where(row16 == 0, vectors[0:1, :], 0.0).astype(BF16)
    block = jnp.dot(cblk[...], wqkv[:, width:], preferred_element_type=F32)
    ctx_place = pl.ds(aligned(sp, context_rows), context_rows)
    ctx_kv[ctx_place, :] = (
        block[:context_rows] * inv_ctx + block[context_rows : context_rows + 1]
    ).astype(BF16)

    def ctx_copy(d):
        return to_peer(
            ctx_kv.at[ctx_place], ctx_kv.at[ctx_place], ctx_send.at[d], ctx_recv.at[d],
            sp=(sp + d) % sp_size, tp=tp,
        )

    @pl.loop(1, sp_size)
    def _(d):
        ctx_copy(d).start()

    down = to_peer(
        kv.at[pl.ds(halo, below)], kv.at[pl.ds(halo + tokens, below)],
        halo_send.at[0], halo_recv.at[0], sp=jnp.maximum(sp - 1, 0),
    )
    up = to_peer(
        kv.at[pl.ds(tokens, halo)], kv.at[pl.ds(0, halo)],
        halo_send.at[1], halo_recv.at[1], sp=jnp.minimum(sp + 1, sp_size - 1),
    )

    @pl.loop(1, ranks)
    def _(d):
        term_copy(d).wait()

    sum_terms(arrived, slice(2, 4))
    factor = (small[2:3, :] * (1.0 + vectors[3:4, :])).astype(BF16)
    xs[big:, :] = jnp.where(row16 == 0, vectors[2:3, :], 0.0).astype(BF16)

    @pl.loop(0, steps)
    def _(k):
        i = jnp.where(k == 0, 0, jnp.where(k == 1, steps - 1, k - 1))
        rows = pl.ds(aligned(i, big), big)
        xs[:big, :] = lat[rows, :] * factor
        y = jnp.dot(xs[...], wqkv[...], preferred_element_type=F32)
        scale = jnp.concatenate([inv[rows, :]] * (3 * width // LANES), axis=1)
        y = y[:big] * scale + y[big : big + 1]
        q = y[:, :width] * (HEAD_DIM**-0.5 * LOG2E)
        turned = []
        for r in range(big // GRID_W):
            turned.append(q[r * GRID_W + SHIFT : (r + 1) * GRID_W])
            turned.append(q[r * GRID_W : r * GRID_W + SHIFT])
        q_s[rows, :] = jnp.concatenate(turned, axis=0).astype(BF16)
        kv[pl.ds(aligned(i, big) + halo, big), :] = y[:, width:].astype(BF16)

        @pl.when((k == 0) & (sp > 0))
        def _():
            down.start()

        @pl.when((k == min(1, steps - 1)) & (sp < sp_size - 1))
        def _():
            up.start()

        @pl.when(k == min(1, steps - 1))
        def _():
            @pl.loop(1, ranks)
            def _(d):
                gate_copy(d).start()

    @pl.loop(1, sp_size)
    def _(d):
        ctx_copy(d).wait()

    contract = (((1,), (1,)), ((), ()))
    size = GROUP * BLOCK
    stack_head = lax.broadcasted_iota(jnp.int32, (size, width), 1) // HEAD_DIM
    first_head = lax.broadcasted_iota(jnp.int32, (size, LANES), 1) < HEAD_DIM
    blocks = GRID_W // BLOCK
    near_keys = KEY_ROWS * STRIP

    def attend(g):
        global_row = sp * grid_rows + g * GROUP
        top = global_row == 0
        bottom = global_row == sp_size * grid_rows - GROUP
        slots = (
            jnp.where(top, 5, jnp.where(bottom, 3, 0)), 1,
            jnp.where(top, 4, jnp.where(bottom, 5, 2)),
        )
        base = aligned(g, group_tokens)

        def strips(b):
            found = []
            for j in range(KEY_ROWS):
                if b == blocks - 1:
                    found.append(pl.ds(base + (j * GRID_W + b * BLOCK), BLOCK))
                    found.append(pl.ds(base + j * GRID_W, BLOCK))
                else:
                    found.append(pl.ds(base + (j * GRID_W + b * BLOCK), STRIP))
            return found

        def places(b):
            return [pl.ds(base + (r * GRID_W + b * BLOCK), BLOCK) for r in range(GROUP)]

        def score(b):
            kind = 1 if b == blocks - 1 else 0
            q = jnp.concatenate([q_s[place, :] for place in places(b)], axis=0)
            stacked = jnp.concatenate(
                [jnp.where(stack_head == h, q, jnp.zeros_like(q)) for h in range(heads)], axis=0
            )
            keys = jnp.concatenate(
                [kv[s, :width] for s in strips(b)] + [ctx_kv[:, :width]], axis=0
            )
            s = lax.dot_general(stacked, keys, contract, preferred_element_type=F32)
            for t in range(TILES):
                lanes = slice(t * LANES, (t + 1) * LANES)
                scores[b, :, lanes] = s[:, lanes] + table[kind, slots[t]]
            scores[b, :, near_keys:] = s[:, near_keys:]

        def soften(b):
            sums = []
            for h in range(heads):
                rows = slice(h * size, (h + 1) * size)
                s = scores[b, rows, :]
                p = jnp.exp2(s - jnp.max(s, axis=1, keepdims=True))
                sums.append(jnp.sum(p, axis=1, keepdims=True))
                probs[b, rows, :] = p.astype(BF16)
            return [1.0 / total for total in sums]

        def mix(b, inverses):
            values = jnp.concatenate(
                [kv[s, width:] for s in strips(b)] + [ctx_kv[:, width:]], axis=0
            )
            mixed = jnp.dot(probs[b], values, preferred_element_type=F32)
            parts = []
            for c in range(width // LANES):
                h, lanes = 2 * c, slice(c * LANES, (c + 1) * LANES)
                parts.append(
                    jnp.where(
                        first_head,
                        mixed[h * size : (h + 1) * size, lanes] * inverses[h],
                        mixed[(h + 1) * size : (h + 2) * size, lanes] * inverses[h + 1],
                    )
                )
            merged = jnp.concatenate(parts, axis=1).astype(BF16)
            for r, place in enumerate(places(b)):
                stage[place, :] = merged[r * BLOCK : (r + 1) * BLOCK]

        score(0)
        for b in range(blocks):
            if b + 1 < blocks:
                score(b + 1)
            mix(b, soften(b))

    def piece_copy(index):
        owner, p = index // pieces, index % pieces
        return to_peer(
            stage.at[pl.ds(aligned(index, piece), piece)],
            recv.at[tp, pl.ds(aligned(p, piece), piece)],
            piece_send.at[index], piece_recv.at[tp, p], tp=owner,
        )

    half = groups // 2
    upper = tp * 2 >= tp_size

    @pl.loop(0, groups)
    def _(k):
        second = k >= half
        j = jnp.where(second, k - half, k)
        low = upper != second
        g = jnp.where(low, (j + 1) % half, half + j)

        @pl.when((g == 0) & (sp > 0))
        def _():
            down.wait_send()
            up.wait_recv()

        @pl.when((g == groups - 1) & (sp < sp_size - 1))
        def _():
            up.wait_send()
            down.wait_recv()

        attend(g)
        for n in range(per_group):
            index = g * per_group + n

            @pl.when(index // pieces != tp)
            def _():
                piece_copy(index).start()

    load_wo.wait()

    @pl.loop(1, ranks)
    def _(d):
        gate_copy(d).wait()

    gates = []
    for t in range(tp_size):
        total = garrived[t]
        for s in range(1, sp_size):
            total = total + garrived[s * tp_size + t]
        gates.append(total)
    gate = jnp.concatenate(gates, axis=1)
    chips = tp_size // 2
    chip = tp // 2
    partner = tp + 1 - 2 * (tp % 2)

    def arrival(source, p):
        rows = pl.ds(aligned(p, piece), piece)
        return to_peer(
            stage.at[rows], recv.at[source, rows], piece_send.at[0],
            piece_recv.at[source, p], tp=source,
        )

    def product(c, rows):
        pair = jnp.concatenate([recv[2 * c, rows, :], recv[2 * c + 1, rows, :]], axis=1)
        return jnp.dot(
            pair, wo[pl.ds(aligned(c, 2 * width), 2 * width), :], preferred_element_type=F32
        )

    @pl.loop(0, pieces)
    def _(p):
        rows = pl.ds(aligned(p, piece), piece)
        recv[tp, rows, :] = stage[pl.ds(aligned(tp * pieces + p, piece), piece), :]
        arrival(partner, p).wait_recv()
        acc[rows, :] = product(chip, rows)

    @pl.loop(0, pieces)
    def _(k):
        p = jnp.where(tp == 0, (k + per_group) % pieces, k)
        rows = pl.ds(aligned(p, piece), piece)
        own = pl.ds(aligned(tp * pieces + p, piece), piece)
        branch = acc[rows, :]
        for d in range(1, chips):
            c = (chip + d) % chips
            arrival(2 * c, p).wait_recv()
            arrival(2 * c + 1, p).wait_recv()
            branch = branch + product(c, rows)
        turned = []
        for r in range(piece_rows):
            turned.append(branch[(r + 1) * GRID_W - SHIFT : (r + 1) * GRID_W])
            turned.append(branch[r * GRID_W : (r + 1) * GRID_W - SHIFT])
        branch = jnp.concatenate(turned, axis=0)
        out_ref[rows, :] = (lat[own, :].astype(F32) + gate * branch).astype(BF16)

    @pl.loop(0, groups * per_group)
    def _(index):
        @pl.when(index // pieces != tp)
        def _():
            piece_copy(index).wait_send()


def local(
    latent, condition, context_tokens, context_condition, shift_weight, scale_weight,
    gate_weight, norm_gain, query_weight, key_weight, value_weight, out_weight, offset_bias,
):
    sp_size, tp_size = lax.axis_size("sp"), lax.axis_size("tp")
    ranks = sp_size * tp_size
    tokens, depth = latent.shape
    context_rows = context_tokens.shape[0]
    input_rows, piece_cols = shift_weight.shape
    width = query_weight.shape[1]
    heads = width // HEAD_DIM
    groups = tokens // GRID_W // GROUP
    group_tokens = GROUP * GRID_W
    share = tokens // tp_size
    piece_rows = gcd(GROUP, share // GRID_W)
    pieces = share // (piece_rows * GRID_W)
    big = 2 * group_tokens if groups % 2 == 0 else group_tokens
    stacked = heads * GROUP * BLOCK
    keys = KEY_ROWS * STRIP + sp_size * context_rows
    bias = jnp.transpose(offset_bias, (1, 0, 2))
    dma = pltpu.SemaphoreType.DMA
    vmem = pltpu.VMEM
    hbm = pl.BlockSpec(memory_space=pl.ANY)
    return pl.pallas_call(
        kernel,
        in_specs=[hbm] * 13,
        out_specs=pl.BlockSpec(memory_space=pltpu.VMEM),
        out_shape=pltpu.VMEM((share, depth), BF16),
        scratch_shapes=[
            vmem((depth,), BF16), vmem((depth,), BF16), vmem((depth,), BF16),
            vmem((8, depth), F32),
            vmem((3, input_rows, piece_cols), BF16),
            vmem(bias.shape, F32),
            vmem((bias.shape[0], heads, LANES), F32),
            vmem((2, 6, heads * GROUP * BLOCK, LANES), F32),
            vmem((context_rows, depth), BF16),
            vmem((context_rows + 16, depth), BF16),
            vmem((tokens, depth), BF16),
            vmem((big + 16, depth), BF16),
            vmem((depth, 3 * width), BF16),
            vmem(out_weight.shape, BF16),
            vmem((2, piece_cols), F32),
            vmem((ranks, 2, piece_cols), F32),
            vmem((2, piece_cols), F32),
            vmem((ranks, 2, piece_cols), F32),
            vmem((1, piece_cols), F32),
            vmem((ranks, 1, piece_cols), F32),
            vmem((4, depth), F32),
            vmem((tokens, LANES), F32),
            vmem((tokens, width), BF16),
            vmem((tokens + 2 * HALO * GRID_W, 2 * width), BF16),
            vmem((sp_size * context_rows, 2 * width), BF16),
            vmem((GRID_W // BLOCK, stacked, keys), F32),
            vmem((GRID_W // BLOCK, stacked, keys), BF16),
            vmem((tokens, width), BF16),
            vmem((tp_size, share, width), BF16),
            vmem((share, depth), F32),
            dma((12,)), dma((groups,)), dma((ranks,)), dma((ranks,)), dma((ranks,)),
            dma((ranks,)), dma((ranks,)), dma((ranks,)), dma((2,)), dma((2,)),
            dma((sp_size,)), dma((sp_size,)),
            dma((tp_size * pieces,)), dma((tp_size, pieces)),
        ],
        compiler_params=pltpu.CompilerParams(
            vmem_limit_bytes=60 * 2**20, collective_id=0, has_side_effects=True
        ),
        cost_estimate=pl.CostEstimate(
            flops=6 * tokens * depth * width,
            bytes_accessed=2 * (tokens * depth + 3 * depth * width + share * depth),
            transcendentals=0,
        ),
    )(
        condition, context_condition, norm_gain, shift_weight, scale_weight, gate_weight, bias,
        context_tokens, latent, query_weight, key_weight, value_weight, out_weight,
    )


def solution(mesh):
    placed = (
        P(("grp", "sp"), None),
        P("grp"),
        P(("grp", "sp"), None),
        P(),
        P("sp", "tp"),
        P("sp", "tp"),
        P("sp", "tp"),
        P(),
        P(None, "tp"),
        P(None, "tp"),
        P(None, "tp"),
        P(),
        P("tp", None, None),
    )
    return jax.shard_map(
        local, mesh=mesh, in_specs=placed, out_specs=P(("grp", "sp", "tp"), None), check_vma=False
    )
```

```python
import functools

import jax
import jax.numpy as jnp
from jax import lax
from jax.experimental import pallas as pl
from jax.experimental.pallas import tpu as pltpu
from jax.sharding import PartitionSpec as P

HEAD_DIM = 64
GRID_W = 64
WIN_ROWS = 8
WIN_COLS = 16
HALO = WIN_ROWS // 2
BLOCK = 16
SHIFT = WIN_COLS // 2
STRIP = BLOCK + WIN_COLS
GROUP = 4
KEY_ROWS = GROUP + WIN_ROWS
LANES = 128
SEGMENTS = LANES // STRIP
TILES = KEY_ROWS // SEGMENTS
LOG2E = 1.4426950408889634
epsilon = 1e-06
masked_score = -1e30
F32 = jnp.float32
BF16 = jnp.bfloat16
MESH = pl.DeviceIdType.MESH


def to_peer(src, dst, send, recv, **place):
    return pltpu.make_async_remote_copy(
        src_ref=src, dst_ref=dst, send_sem=send, recv_sem=recv,
        device_id=place, device_id_type=MESH,
    )


def gcd(a, b):
    while b:
        a, b = b, a % b
    return a


def aligned(index, step):
    return pl.multiple_of(index * step, step)


def build_tables(bias_ref, braw, table, heads):
    offsets = bias_ref.shape[0]
    braw[...] = jnp.zeros_like(braw)
    for o in range(offsets):
        braw[o, :, : bias_ref.shape[2]] = bias_ref[o] * LOG2E
    lane_h = lax.broadcasted_iota(jnp.int32, (heads, LANES), 1) // STRIP
    first = HALO - 1
    combined = []
    for o in range(first - (GROUP - 1), first + (TILES - 1) * SEGMENTS + 1):
        row = braw[o]
        for j in range(1, SEGMENTS):
            row = jnp.where(lane_h == j, pltpu.roll(braw[o + j], STRIP * j, 1), row)
        combined.append(row)
    u = lax.broadcasted_iota(jnp.int32, (BLOCK, LANES), 0)
    lane = lax.broadcasted_iota(jnp.int32, (BLOCK, LANES), 1)
    v = lane % STRIP
    inner = (v >= u) & (v < u + WIN_COLS)
    edge = ((u < SHIFT) & (v < WIN_COLS)) | ((u >= SHIFT) & (v >= WIN_COLS))
    for t in range(TILES):
        for i in range(GROUP):
            j = t * SEGMENTS + lane // STRIP
            seen = (j >= i) & (j < i + WIN_ROWS)
            whole = t * SEGMENTS >= i and (t + 1) * SEGMENTS <= i + WIN_ROWS
            source = combined[t * SEGMENTS + GROUP - 1 - i]
            for h in range(heads):
                spread = jnp.broadcast_to(source[h : h + 1, :], (BLOCK, LANES))
                value = pltpu.roll(spread, LANES - (SHIFT - 1), 1, stride=1, stride_axis=0)
                place = slice((h * GROUP + i) * BLOCK, (h * GROUP + i + 1) * BLOCK)
                for kind, mask in enumerate((inner, edge)):
                    full = jnp.where(mask, value, masked_score)
                    table[kind, t, place, :] = (
                        full if whole else jnp.where(seen, full, masked_score)
                    )
                    if t != 1:
                        table[kind, 3 if t == 0 else 4, place, :] = full
    for kind in range(2):
        table[kind, 5] = jnp.full(table.shape[2:], masked_score, F32)


def kernel(
    cond_hbm, ctxcond_hbm, gain_hbm, shift_hbm, scale_hbm, gate_hbm, bias_hbm, ctx_hbm,
    lat_hbm, wq_hbm, wk_hbm, wv_hbm, wo_hbm,
    out_ref,
    cond, ctxcond, gain, small, modw, bias, braw, table, ctx, cblk, lat, xs, wqkv, wo,
    cterms, carrived, terms, arrived, gterms, garrived, vectors, added, inv, q_s, kv, ctx_kv,
    scores, probs, stage, recv, acc,
    load_sem, lat_sem, cterm_send, cterm_recv, term_send, term_recv, gate_send, gate_recv,
    halo_send, halo_recv, ctx_send, ctx_recv, piece_send, piece_recv,
):
    sp, tp = lax.axis_index("sp"), lax.axis_index("tp")
    sp_size, tp_size = lax.axis_size("sp"), lax.axis_size("tp")
    ranks = sp_size * tp_size
    me = sp * tp_size + tp
    tokens, depth = lat.shape
    width = wq_hbm.shape[1]
    heads = width // HEAD_DIM
    input_rows, piece_cols = modw.shape[1:]
    context_rows = ctx.shape[0]
    grid_rows = tokens // GRID_W
    groups = grid_rows // GROUP
    group_tokens = GROUP * GRID_W
    halo = HALO * GRID_W
    below = (HALO - 1) * GRID_W
    share = tokens // tp_size
    piece_rows = gcd(GROUP, share // GRID_W)
    piece = piece_rows * GRID_W
    pieces = share // piece
    per_group = GROUP // piece_rows

    def peer(d):
        other = (me + d) % ranks
        return dict(sp=other // tp_size, tp=other % tp_size)

    barrier = pltpu.get_barrier_semaphore()

    early = [
        pltpu.make_async_copy(cond_hbm, cond, load_sem.at[0]),
        pltpu.make_async_copy(ctxcond_hbm, ctxcond, load_sem.at[1]),
        pltpu.make_async_copy(gain_hbm, gain, load_sem.at[2]),
        pltpu.make_async_copy(shift_hbm, modw.at[0], load_sem.at[3]),
        pltpu.make_async_copy(scale_hbm, modw.at[1], load_sem.at[4]),
        pltpu.make_async_copy(gate_hbm, modw.at[2], load_sem.at[5]),
    ]
    load_bias = pltpu.make_async_copy(bias_hbm, bias, load_sem.at[6])
    load_ctx = pltpu.make_async_copy(ctx_hbm, ctx, load_sem.at[7])
    load_weights = [
        pltpu.make_async_copy(w, wqkv.at[:, pl.ds(i * width, width)], load_sem.at[8 + i])
        for i, w in enumerate((wq_hbm, wk_hbm, wv_hbm))
    ]
    load_wo = pltpu.make_async_copy(wo_hbm, wo, load_sem.at[11])

    def load_lat(i):
        rows = pl.ds(aligned(i, group_tokens), group_tokens)
        return pltpu.make_async_copy(lat_hbm.at[rows], lat.at[rows], lat_sem.at[i])

    @pl.loop(1, ranks)
    def _(d):
        pl.semaphore_signal(barrier, inc=1, device_id=peer(d), device_id_type=MESH)

    for load in early:
        load.start()

    load_bias.start()
    load_ctx.start()

    @pl.loop(0, groups)
    def _(i):
        load_lat(i).start()

    for load in load_weights:
        load.start()
    load_wo.start()

    for load in early:
        load.wait()
    small[0:1, :] = cond[...].astype(F32).reshape(1, depth)
    small[1:2, :] = ctxcond[...].astype(F32).reshape(1, depth)
    small[2:3, :] = gain[...].astype(F32).reshape(1, depth)
    row8 = lax.broadcasted_iota(jnp.int32, (8, input_rows), 0)
    own_inputs = pl.ds(aligned(sp, input_rows), input_rows)
    value = jnp.where(row8 == 0, small[0:1, own_inputs], small[1:2, own_inputs])
    act = (value / (1.0 + jnp.exp(-value))).astype(BF16)
    for i in range(2):
        both = jnp.dot(act, modw[i], preferred_element_type=F32)
        terms[i : i + 1, :] = both[0:1]
        cterms[i : i + 1, :] = both[1:2]
    gterms[...] = jnp.dot(act, modw[2], preferred_element_type=F32)[:1]
    carrived[me] = cterms[...]
    arrived[me] = terms[...]
    garrived[me] = gterms[...]

    def cterm_copy(d):
        return to_peer(
            cterms, carrived.at[me], cterm_send.at[d], cterm_recv.at[d], **peer(d)
        )

    def term_copy(d):
        return to_peer(terms, arrived.at[me], term_send.at[d], term_recv.at[d], **peer(d))

    def gate_copy(d):
        return to_peer(gterms, garrived.at[me], gate_send.at[d], gate_recv.at[d], **peer(d))

    load_bias.wait()
    build_tables(bias, braw, table, heads)
    pl.semaphore_wait(barrier, ranks - 1)

    @pl.loop(1, ranks)
    def _(d):
        cterm_copy(d).start()

    @pl.loop(1, ranks)
    def _(d):
        term_copy(d).start()

    @pl.when(sp == 0)
    def _():
        kv[0:halo, :] = jnp.zeros((halo, 2 * width), BF16)

    @pl.when(sp == sp_size - 1)
    def _():
        kv[halo + tokens : halo + tokens + below, :] = jnp.zeros((below, 2 * width), BF16)

    kv[halo + tokens + below :, :] = jnp.zeros((halo - below, 2 * width), BF16)

    def inverse_of(ref, rows):
        total = None
        for c in range(depth // LANES):
            x = ref[rows, c * LANES : (c + 1) * LANES].astype(F32)
            total = x * x if total is None else total + x * x
        mean = jnp.sum(total, axis=1, keepdims=True) * (1.0 / depth)
        return lax.rsqrt(mean + epsilon)

    load_ctx.wait()
    inv_ctx = inverse_of(ctx, slice(None))

    @pl.loop(0, groups)
    def _(i):
        load_lat(i).wait()
        for r in range(0, group_tokens, 128):
            rows = pl.ds(aligned(i, group_tokens) + r, 128)
            inv[rows, :] = jnp.broadcast_to(inverse_of(lat, rows), (128, LANES))

    for load in load_weights:
        load.wait()

    def sum_terms(ref, rows):
        for t in range(tp_size):
            total = ref[t]
            for s in range(1, sp_size):
                total = total + ref[s * tp_size + t]
            vectors[rows, t * piece_cols : (t + 1) * piece_cols] = total

    @pl.loop(1, ranks)
    def _(d):
        cterm_copy(d).wait()

    sum_terms(carrived, slice(0, 2))
    row16 = lax.broadcasted_iota(jnp.int32, (16, depth), 0)
    factor_ctx = (small[2:3, :] * (1.0 + vectors[1:2, :])).astype(BF16)
    cblk[:context_rows, :] = ctx[...] * factor_ctx
    cblk[context_rows:, :] = jnp.where(row16 == 0, vectors[0:1, :], 0.0).astype(BF16)
    block = jnp.dot(cblk[...], wqkv[:, width:], preferred_element_type=F32)
    ctx_place = pl.ds(aligned(sp, context_rows), context_rows)
    ctx_kv[ctx_place, :] = (
        block[:context_rows] * inv_ctx + block[context_rows : context_rows + 1]
    ).astype(BF16)

    def ctx_copy(d):
        return to_peer(
            ctx_kv.at[ctx_place], ctx_kv.at[ctx_place], ctx_send.at[d], ctx_recv.at[d],
            sp=(sp + d) % sp_size, tp=tp,
        )

    @pl.loop(1, sp_size)
    def _(d):
        ctx_copy(d).start()

    down = to_peer(
        kv.at[pl.ds(halo, below)], kv.at[pl.ds(halo + tokens, below)],
        halo_send.at[0], halo_recv.at[0], sp=jnp.maximum(sp - 1, 0),
    )
    up = to_peer(
        kv.at[pl.ds(tokens, halo)], kv.at[pl.ds(0, halo)],
        halo_send.at[1], halo_recv.at[1], sp=jnp.minimum(sp + 1, sp_size - 1),
    )

    @pl.loop(1, ranks)
    def _(d):
        term_copy(d).wait()

    sum_terms(arrived, slice(2, 4))
    factor = (small[2:3, :] * (1.0 + vectors[3:4, :])).astype(BF16)
    xs[group_tokens:, :] = jnp.where(row16 == 0, vectors[2:3, :], 0.0).astype(BF16)

    upper = tp * 2 >= tp_size

    def unit(k):
        if k == 0:
            return jnp.where(upper, groups - 1, 0)
        if k == groups - 1:
            return jnp.where(upper, groups - 2, 1)
        return jnp.where(upper, k - 1, k + 1)

    def project(i, first):
        rows = pl.ds(aligned(i, group_tokens), group_tokens)
        place = pl.ds(aligned(i, group_tokens) + halo, group_tokens)
        xs[:group_tokens, :] = lat[rows, :] * factor
        scale = jnp.concatenate([inv[rows, :]] * (width // LANES), axis=1)

        def part(n):
            columns = slice(n * width, (n + 1) * width)
            left = xs[...] if first else xs[:group_tokens, :]
            y = jnp.dot(left, wqkv[:, columns], preferred_element_type=F32)
            if first:
                added[0:1, columns] = y[group_tokens : group_tokens + 1]
            return y[:group_tokens] * scale + added[0:1, columns]

        q = part(0) * (HEAD_DIM**-0.5 * LOG2E)
        turned = []
        for r in range(GROUP):
            turned.append(q[r * GRID_W + SHIFT : (r + 1) * GRID_W])
            turned.append(q[r * GRID_W : r * GRID_W + SHIFT])
        q_s[rows, :] = jnp.concatenate(turned, axis=0).astype(BF16)
        kv[place, :width] = part(1).astype(BF16)
        kv[place, width:] = part(2).astype(BF16)

    project(unit(0), True)

    @pl.loop(1, groups - 1)
    def _(k):
        project(jnp.where(upper, k - 1, k + 1), False)

        @pl.when((k == 1) & (sp > 0))
        def _():
            down.start()

        @pl.when((k == groups - 2) & (sp < sp_size - 1))
        def _():
            up.start()

    @pl.loop(1, ranks)
    def _(d):
        gate_copy(d).start()

    contract = (((1,), (1,)), ((), ()))
    size = GROUP * BLOCK
    stack_head = lax.broadcasted_iota(jnp.int32, (size, width), 1) // HEAD_DIM
    first_head = lax.broadcasted_iota(jnp.int32, (size, LANES), 1) < HEAD_DIM
    blocks = GRID_W // BLOCK
    near_keys = KEY_ROWS * STRIP

    def strips(g, b):
        base = aligned(g, group_tokens)
        found = []
        for j in range(KEY_ROWS):
            if b == blocks - 1:
                found.append(pl.ds(base + (j * GRID_W + b * BLOCK), BLOCK))
                found.append(pl.ds(base + j * GRID_W, BLOCK))
            else:
                found.append(pl.ds(base + (j * GRID_W + b * BLOCK), STRIP))
        return found

    def places(g, b):
        base = aligned(g, group_tokens)
        return [pl.ds(base + (r * GRID_W + b * BLOCK), BLOCK) for r in range(GROUP)]

    def stacked(g, b):
        q = jnp.concatenate([q_s[place, :] for place in places(g, b)], axis=0)
        return jnp.concatenate(
            [jnp.where(stack_head == h, q, jnp.zeros_like(q)) for h in range(heads)], axis=0
        )

    def score_near(g, b):
        global_row = sp * grid_rows + g * GROUP
        top = global_row == 0
        bottom = global_row == sp_size * grid_rows - GROUP
        slots = (
            jnp.where(top, 5, jnp.where(bottom, 3, 0)), 1,
            jnp.where(top, 4, jnp.where(bottom, 5, 2)),
        )
        kind = 1 if b == blocks - 1 else 0
        keys = jnp.concatenate([kv[s, :width] for s in strips(g, b)], axis=0)
        s = lax.dot_general(stacked(g, b), keys, contract, preferred_element_type=F32)
        for t in range(TILES):
            lanes = slice(t * LANES, (t + 1) * LANES)
            scores[b, :, lanes] = s[:, lanes] + table[kind, slots[t]]

    def score_far(g, b):
        scores[b, :, near_keys:] = lax.dot_general(
            stacked(g, b), ctx_kv[:, :width], contract, preferred_element_type=F32
        )

    def soften(b):
        sums = []
        for h in range(heads):
            rows = slice(h * size, (h + 1) * size)
            s = scores[b, rows, :]
            p = jnp.exp2(s - jnp.max(s, axis=1, keepdims=True))
            sums.append(jnp.sum(p, axis=1, keepdims=True))
            probs[b, rows, :] = p.astype(BF16)
        return [1.0 / total for total in sums]

    def mix(g, b, inverses):
        values = jnp.concatenate(
            [kv[s, width:] for s in strips(g, b)] + [ctx_kv[:, width:]], axis=0
        )
        mixed = jnp.dot(probs[b], values, preferred_element_type=F32)
        parts = []
        for c in range(width // LANES):
            h, lanes = 2 * c, slice(c * LANES, (c + 1) * LANES)
            parts.append(
                jnp.where(
                    first_head,
                    mixed[h * size : (h + 1) * size, lanes] * inverses[h],
                    mixed[(h + 1) * size : (h + 2) * size, lanes] * inverses[h + 1],
                )
            )
        merged = jnp.concatenate(parts, axis=1).astype(BF16)
        for r, place in enumerate(places(g, b)):
            stage[place, :] = merged[r * BLOCK : (r + 1) * BLOCK]

    def piece_copy(index):
        owner, p = index // pieces, index % pieces
        return to_peer(
            stage.at[pl.ds(aligned(index, piece), piece)],
            recv.at[tp, pl.ds(aligned(p, piece), piece)],
            piece_send.at[index], piece_recv.at[tp, p], tp=owner,
        )

    half = groups // 2
    inner = half - 1

    def group_of(own, j):
        return jnp.where(upper != own, (j + 1) % half, half + j)

    def send_pieces(g):
        for n in range(per_group):
            index = g * per_group + n

            @pl.when(index // pieces != tp)
            def _():
                piece_copy(index).start()

    for b in range(blocks):
        score_near(group_of(False, 0), b)

    @pl.loop(1, sp_size)
    def _(d):
        ctx_copy(d).wait()

    @pl.loop(0, inner)
    def _(k):
        g, following = group_of(False, k), group_of(False, jnp.minimum(k + 1, inner - 1))
        score_far(g, 0)
        for b in range(blocks):
            if b + 1 < blocks:
                score_far(g, b + 1)
            inverses = soften(b)
            score_near(following, b)
            mix(g, b, inverses)
        send_pieces(g)

    project(unit(groups - 1), False)

    @pl.loop(0, groups - inner)
    def _(k):
        edge = (k == 1) | (k == groups - inner - 1)
        own = k != 1
        j = jnp.where(edge, inner, jnp.where(k > 1, k - 1, k))
        g = group_of(own, j)

        @pl.when((g == 0) & (sp > 0))
        def _():
            down.wait_send()
            up.wait_recv()

        @pl.when((g == groups - 1) & (sp < sp_size - 1))
        def _():
            up.wait_send()
            down.wait_recv()

        score_near(g, 0)
        score_far(g, 0)
        for b in range(blocks):
            if b + 1 < blocks:
                score_near(g, b + 1)
                score_far(g, b + 1)
            mix(g, b, soften(b))
        send_pieces(g)

    load_wo.wait()

    @pl.loop(1, ranks)
    def _(d):
        gate_copy(d).wait()

    gates = []
    for t in range(tp_size):
        total = garrived[t]
        for s in range(1, sp_size):
            total = total + garrived[s * tp_size + t]
        gates.append(total)
    gate = jnp.concatenate(gates, axis=1)
    chips = tp_size // 2
    chip = tp // 2
    partner = tp + 1 - 2 * (tp % 2)

    def arrival(source, p):
        rows = pl.ds(aligned(p, piece), piece)
        return to_peer(
            stage.at[rows], recv.at[source, rows], piece_send.at[0],
            piece_recv.at[source, p], tp=source,
        )

    def product(c, rows):
        pair = jnp.concatenate([recv[2 * c, rows, :], recv[2 * c + 1, rows, :]], axis=1)
        return jnp.dot(
            pair, wo[pl.ds(aligned(c, 2 * width), 2 * width), :], preferred_element_type=F32
        )

    @pl.loop(0, pieces)
    def _(p):
        rows = pl.ds(aligned(p, piece), piece)
        recv[tp, rows, :] = stage[pl.ds(aligned(tp * pieces + p, piece), piece), :]
        arrival(partner, p).wait_recv()
        acc[rows, :] = product(chip, rows)

    @pl.loop(0, groups * per_group)
    def _(index):
        @pl.when(index // pieces != tp)
        def _():
            piece_copy(index).wait_send()

    @pl.loop(0, pieces)
    def _(k):
        p = jnp.where(tp == 0, (k + per_group) % pieces, k)
        rows = pl.ds(aligned(p, piece), piece)
        own = pl.ds(aligned(tp * pieces + p, piece), piece)
        branch = acc[rows, :]
        for d in range(1, chips):
            c = (chip + d) % chips
            arrival(2 * c, p).wait_recv()
            arrival(2 * c + 1, p).wait_recv()
            branch = branch + product(c, rows)
        turned = []
        for r in range(piece_rows):
            turned.append(branch[(r + 1) * GRID_W - SHIFT : (r + 1) * GRID_W])
            turned.append(branch[r * GRID_W : (r + 1) * GRID_W - SHIFT])
        branch = jnp.concatenate(turned, axis=0)
        out_ref[rows, :] = (lat[own, :].astype(F32) + gate * branch).astype(BF16)


def local(
    latent, condition, context_tokens, context_condition, shift_weight, scale_weight,
    gate_weight, norm_gain, query_weight, key_weight, value_weight, out_weight, offset_bias,
):
    sp_size, tp_size = lax.axis_size("sp"), lax.axis_size("tp")
    ranks = sp_size * tp_size
    tokens, depth = latent.shape
    context_rows = context_tokens.shape[0]
    input_rows, piece_cols = shift_weight.shape
    width = query_weight.shape[1]
    heads = width // HEAD_DIM
    groups = tokens // GRID_W // GROUP
    group_tokens = GROUP * GRID_W
    share = tokens // tp_size
    piece_rows = gcd(GROUP, share // GRID_W)
    pieces = share // (piece_rows * GRID_W)
    stacked = heads * GROUP * BLOCK
    keys = KEY_ROWS * STRIP + sp_size * context_rows
    bias = jnp.transpose(offset_bias, (1, 0, 2))
    dma = pltpu.SemaphoreType.DMA
    vmem = pltpu.VMEM
    hbm = pl.BlockSpec(memory_space=pl.ANY)
    return pl.pallas_call(
        kernel,
        in_specs=[hbm] * 13,
        out_specs=pl.BlockSpec(memory_space=pltpu.VMEM),
        out_shape=pltpu.VMEM((share, depth), BF16),
        scratch_shapes=[
            vmem((depth,), BF16), vmem((depth,), BF16), vmem((depth,), BF16),
            vmem((8, depth), F32),
            vmem((3, input_rows, piece_cols), BF16),
            vmem(bias.shape, F32),
            vmem((bias.shape[0], heads, LANES), F32),
            vmem((2, 6, heads * GROUP * BLOCK, LANES), F32),
            vmem((context_rows, depth), BF16),
            vmem((context_rows + 16, depth), BF16),
            vmem((tokens, depth), BF16),
            vmem((group_tokens + 16, depth), BF16),
            vmem((depth, 3 * width), BF16),
            vmem(out_weight.shape, BF16),
            vmem((2, piece_cols), F32),
            vmem((ranks, 2, piece_cols), F32),
            vmem((2, piece_cols), F32),
            vmem((ranks, 2, piece_cols), F32),
            vmem((1, piece_cols), F32),
            vmem((ranks, 1, piece_cols), F32),
            vmem((4, depth), F32),
            vmem((1, 3 * width), F32),
            vmem((tokens, LANES), F32),
            vmem((tokens, width), BF16),
            vmem((tokens + 2 * HALO * GRID_W, 2 * width), BF16),
            vmem((sp_size * context_rows, 2 * width), BF16),
            vmem((GRID_W // BLOCK, stacked, keys), F32),
            vmem((GRID_W // BLOCK, stacked, keys), BF16),
            vmem((tokens, width), BF16),
            vmem((tp_size, share, width), BF16),
            vmem((share, depth), F32),
            dma((12,)), dma((groups,)), dma((ranks,)), dma((ranks,)), dma((ranks,)),
            dma((ranks,)), dma((ranks,)), dma((ranks,)), dma((2,)), dma((2,)),
            dma((sp_size,)), dma((sp_size,)),
            dma((tp_size * pieces,)), dma((tp_size, pieces)),
        ],
        compiler_params=pltpu.CompilerParams(
            vmem_limit_bytes=60 * 2**20, collective_id=0, has_side_effects=True
        ),
        cost_estimate=pl.CostEstimate(
            flops=6 * tokens * depth * width,
            bytes_accessed=2 * (tokens * depth + 3 * depth * width + share * depth),
            transcendentals=0,
        ),
    )(
        condition, context_condition, norm_gain, shift_weight, scale_weight, gate_weight, bias,
        context_tokens, latent, query_weight, key_weight, value_weight, out_weight,
    )


def solution(mesh):
    placed = (
        P(("grp", "sp"), None),
        P("grp"),
        P(("grp", "sp"), None),
        P(),
        P("sp", "tp"),
        P("sp", "tp"),
        P("sp", "tp"),
        P(),
        P(None, "tp"),
        P(None, "tp"),
        P(None, "tp"),
        P(),
        P("tp", None, None),
    )
    return jax.shard_map(
        local, mesh=mesh, in_specs=placed, out_specs=P(("grp", "sp", "tp"), None), check_vma=False
    )
```

```python
import functools

import jax
import jax.numpy as jnp
from jax import lax
from jax.experimental import pallas as pl
from jax.experimental.pallas import tpu as pltpu
from jax.sharding import PartitionSpec as P

HEAD_DIM = 64
GRID_W = 64
WIN_ROWS = 8
WIN_COLS = 16
HALO = WIN_ROWS // 2
BLOCK = 16
SHIFT = WIN_COLS // 2
STRIP = BLOCK + WIN_COLS
GROUP = 4
KEY_ROWS = GROUP + WIN_ROWS
LANES = 128
SEGMENTS = LANES // STRIP
TILES = KEY_ROWS // SEGMENTS
LOG2E = 1.4426950408889634
epsilon = 1e-06
masked_score = -1e30
F32 = jnp.float32
BF16 = jnp.bfloat16
MESH = pl.DeviceIdType.MESH


def to_peer(src, dst, send, recv, **place):
    return pltpu.make_async_remote_copy(
        src_ref=src, dst_ref=dst, send_sem=send, recv_sem=recv,
        device_id=place, device_id_type=MESH,
    )


def gcd(a, b):
    while b:
        a, b = b, a % b
    return a


def aligned(index, step):
    return pl.multiple_of(index * step, step)


def build_tables(bias_ref, braw, table, heads):
    offsets = bias_ref.shape[0]
    braw[...] = jnp.zeros_like(braw)
    for o in range(offsets):
        braw[o, :, : bias_ref.shape[2]] = bias_ref[o] * LOG2E
    lane_h = lax.broadcasted_iota(jnp.int32, (heads, LANES), 1) // STRIP
    first = HALO - 1
    combined = []
    for o in range(first - (GROUP - 1), first + (TILES - 1) * SEGMENTS + 1):
        row = braw[o]
        for j in range(1, SEGMENTS):
            row = jnp.where(lane_h == j, pltpu.roll(braw[o + j], STRIP * j, 1), row)
        combined.append(row)
    u = lax.broadcasted_iota(jnp.int32, (BLOCK, LANES), 0)
    lane = lax.broadcasted_iota(jnp.int32, (BLOCK, LANES), 1)
    v = lane % STRIP
    inner = (v >= u) & (v < u + WIN_COLS)
    edge = ((u < SHIFT) & (v < WIN_COLS)) | ((u >= SHIFT) & (v >= WIN_COLS))
    for t in range(TILES):
        for i in range(GROUP):
            j = t * SEGMENTS + lane // STRIP
            seen = (j >= i) & (j < i + WIN_ROWS)
            whole = t * SEGMENTS >= i and (t + 1) * SEGMENTS <= i + WIN_ROWS
            source = combined[t * SEGMENTS + GROUP - 1 - i]
            for h in range(heads):
                spread = jnp.broadcast_to(source[h : h + 1, :], (BLOCK, LANES))
                value = pltpu.roll(spread, LANES - (SHIFT - 1), 1, stride=1, stride_axis=0)
                place = slice((h * GROUP + i) * BLOCK, (h * GROUP + i + 1) * BLOCK)
                for kind, mask in enumerate((inner, edge)):
                    full = jnp.where(mask, value, masked_score)
                    table[kind, t, place, :] = (
                        full if whole else jnp.where(seen, full, masked_score)
                    )
                    if t != 1:
                        table[kind, 3 if t == 0 else 4, place, :] = full
    for kind in range(2):
        table[kind, 5] = jnp.full(table.shape[2:], masked_score, F32)


def kernel(
    cond_hbm, ctxcond_hbm, gain_hbm, shift_hbm, scale_hbm, gate_hbm, bias_hbm, ctx_hbm,
    lat_hbm, wq_hbm, wk_hbm, wv_hbm, wo_hbm,
    out_ref,
    cond, ctxcond, gain, small, modw, bias, braw, table, ctx, cblk, lat, xs, wqkv, wo,
    cterms, carrived, terms, arrived, gterms, garrived, vectors, added, inv, q_s, kv, ctx_kv,
    scores, probs, partial, stats, stage, recv, acc,
    load_sem, lat_sem, cterm_send, cterm_recv, term_send, term_recv, gate_send, gate_recv,
    halo_send, halo_recv, ctx_send, ctx_recv, piece_send, piece_recv,
):
    sp, tp = lax.axis_index("sp"), lax.axis_index("tp")
    sp_size, tp_size = lax.axis_size("sp"), lax.axis_size("tp")
    ranks = sp_size * tp_size
    me = sp * tp_size + tp
    tokens, depth = lat.shape
    width = wq_hbm.shape[1]
    heads = width // HEAD_DIM
    input_rows, piece_cols = modw.shape[1:]
    context_rows = ctx.shape[0]
    grid_rows = tokens // GRID_W
    groups = grid_rows // GROUP
    group_tokens = GROUP * GRID_W
    halo = HALO * GRID_W
    below = (HALO - 1) * GRID_W
    share = tokens // tp_size
    piece_rows = gcd(GROUP, share // GRID_W)
    piece = piece_rows * GRID_W
    pieces = share // piece
    per_group = GROUP // piece_rows

    def peer(d):
        other = (me + d) % ranks
        return dict(sp=other // tp_size, tp=other % tp_size)

    barrier = pltpu.get_barrier_semaphore()

    early = [
        pltpu.make_async_copy(cond_hbm, cond, load_sem.at[0]),
        pltpu.make_async_copy(ctxcond_hbm, ctxcond, load_sem.at[1]),
        pltpu.make_async_copy(gain_hbm, gain, load_sem.at[2]),
        pltpu.make_async_copy(shift_hbm, modw.at[0], load_sem.at[3]),
        pltpu.make_async_copy(scale_hbm, modw.at[1], load_sem.at[4]),
        pltpu.make_async_copy(gate_hbm, modw.at[2], load_sem.at[5]),
    ]
    load_bias = pltpu.make_async_copy(bias_hbm, bias, load_sem.at[6])
    load_ctx = pltpu.make_async_copy(ctx_hbm, ctx, load_sem.at[7])
    load_weights = [
        pltpu.make_async_copy(w, wqkv.at[:, pl.ds(i * width, width)], load_sem.at[8 + i])
        for i, w in enumerate((wq_hbm, wk_hbm, wv_hbm))
    ]
    load_wo = pltpu.make_async_copy(wo_hbm, wo, load_sem.at[11])

    def load_lat(i):
        rows = pl.ds(aligned(i, group_tokens), group_tokens)
        return pltpu.make_async_copy(lat_hbm.at[rows], lat.at[rows], lat_sem.at[i])

    @pl.loop(1, ranks)
    def _(d):
        pl.semaphore_signal(barrier, inc=1, device_id=peer(d), device_id_type=MESH)

    for load in early:
        load.start()

    load_bias.start()
    load_ctx.start()

    @pl.loop(0, groups)
    def _(i):
        load_lat(i).start()

    for load in load_weights:
        load.start()
    load_wo.start()

    for load in early:
        load.wait()
    small[0:1, :] = cond[...].astype(F32).reshape(1, depth)
    small[1:2, :] = ctxcond[...].astype(F32).reshape(1, depth)
    small[2:3, :] = gain[...].astype(F32).reshape(1, depth)
    row8 = lax.broadcasted_iota(jnp.int32, (8, input_rows), 0)
    own_inputs = pl.ds(aligned(sp, input_rows), input_rows)
    value = jnp.where(row8 == 0, small[0:1, own_inputs], small[1:2, own_inputs])
    act = (value / (1.0 + jnp.exp(-value))).astype(BF16)
    for i in range(2):
        both = jnp.dot(act, modw[i], preferred_element_type=F32)
        terms[i : i + 1, :] = both[0:1]
        cterms[i : i + 1, :] = both[1:2]
    gterms[...] = jnp.dot(act, modw[2], preferred_element_type=F32)[:1]
    carrived[me] = cterms[...]
    arrived[me] = terms[...]
    garrived[me] = gterms[...]

    def wait_all(slots, send, recv_sem):
        all_but_one = slots.at[pl.ds(0, ranks - 1)]
        to_peer(all_but_one, all_but_one, send, recv_sem, **peer(1)).wait()

    def cterm_copy(d):
        return to_peer(
            cterms, carrived.at[me], cterm_send, cterm_recv, **peer(d)
        )

    def term_copy(d):
        return to_peer(terms, arrived.at[me], term_send, term_recv, **peer(d))

    def gate_copy(d):
        return to_peer(gterms, garrived.at[me], gate_send, gate_recv, **peer(d))

    load_bias.wait()
    build_tables(bias, braw, table, heads)
    pl.semaphore_wait(barrier, ranks - 1)

    @pl.loop(1, ranks)
    def _(d):
        cterm_copy(d).start()

    @pl.loop(1, ranks)
    def _(d):
        term_copy(d).start()

    @pl.when(sp == 0)
    def _():
        kv[0:halo, :] = jnp.zeros((halo, 2 * width), BF16)

    @pl.when(sp == sp_size - 1)
    def _():
        kv[halo + tokens : halo + tokens + below, :] = jnp.zeros((below, 2 * width), BF16)

    kv[halo + tokens + below :, :] = jnp.zeros((halo - below, 2 * width), BF16)

    def inverse_of(ref, rows):
        total = None
        for c in range(depth // LANES):
            x = ref[rows, c * LANES : (c + 1) * LANES].astype(F32)
            total = x * x if total is None else total + x * x
        mean = jnp.sum(total, axis=1, keepdims=True) * (1.0 / depth)
        return lax.rsqrt(mean + epsilon)

    load_ctx.wait()
    inv_ctx = inverse_of(ctx, slice(None))

    @pl.loop(0, groups)
    def _(i):
        load_lat(i).wait()
        for r in range(0, group_tokens, 128):
            rows = pl.ds(aligned(i, group_tokens) + r, 128)
            inv[rows, :] = jnp.broadcast_to(inverse_of(lat, rows), (128, LANES))

    for load in load_weights:
        load.wait()

    def sum_terms(ref, rows):
        for t in range(tp_size):
            total = ref[t]
            for s in range(1, sp_size):
                total = total + ref[s * tp_size + t]
            vectors[rows, t * piece_cols : (t + 1) * piece_cols] = total

    wait_all(carrived, cterm_send, cterm_recv)

    sum_terms(carrived, slice(0, 2))
    row16 = lax.broadcasted_iota(jnp.int32, (16, depth), 0)
    factor_ctx = (small[2:3, :] * (1.0 + vectors[1:2, :])).astype(BF16)
    cblk[:context_rows, :] = ctx[...] * factor_ctx
    cblk[context_rows:, :] = jnp.where(row16 == 0, vectors[0:1, :], 0.0).astype(BF16)
    block = jnp.dot(cblk[...], wqkv[:, width:], preferred_element_type=F32)
    ctx_place = pl.ds(aligned(sp, context_rows), context_rows)
    ctx_kv[ctx_place, :] = (
        block[:context_rows] * inv_ctx + block[context_rows : context_rows + 1]
    ).astype(BF16)

    def ctx_copy(d):
        return to_peer(
            ctx_kv.at[ctx_place], ctx_kv.at[ctx_place], ctx_send, ctx_recv,
            sp=(sp + d) % sp_size, tp=tp,
        )

    @pl.loop(1, sp_size)
    def _(d):
        ctx_copy(d).start()

    down = to_peer(
        kv.at[pl.ds(halo, below)], kv.at[pl.ds(halo + tokens, below)],
        halo_send.at[0], halo_recv.at[0], sp=jnp.maximum(sp - 1, 0),
    )
    up = to_peer(
        kv.at[pl.ds(tokens, halo)], kv.at[pl.ds(0, halo)],
        halo_send.at[1], halo_recv.at[1], sp=jnp.minimum(sp + 1, sp_size - 1),
    )

    wait_all(arrived, term_send, term_recv)

    sum_terms(arrived, slice(2, 4))
    factor = (small[2:3, :] * (1.0 + vectors[3:4, :])).astype(BF16)
    xs[group_tokens:, :] = jnp.where(row16 == 0, vectors[2:3, :], 0.0).astype(BF16)

    upper = tp * 2 >= tp_size

    def unit(k):
        if k == 0:
            return jnp.where(upper, groups - 1, 0)
        if k == groups - 1:
            return jnp.where(upper, groups - 2, 1)
        return jnp.where(upper, k - 1, k + 1)

    def project(i, first):
        rows = pl.ds(aligned(i, group_tokens), group_tokens)
        place = pl.ds(aligned(i, group_tokens) + halo, group_tokens)
        xs[:group_tokens, :] = lat[rows, :] * factor
        scale = jnp.concatenate([inv[rows, :]] * (width // LANES), axis=1)

        def part(n):
            columns = slice(n * width, (n + 1) * width)
            left = xs[...] if first else xs[:group_tokens, :]
            y = jnp.dot(left, wqkv[:, columns], preferred_element_type=F32)
            if first:
                added[0:1, columns] = y[group_tokens : group_tokens + 1]
            return y[:group_tokens] * scale + added[0:1, columns]

        q = part(0) * (HEAD_DIM**-0.5 * LOG2E)
        turned = []
        for r in range(GROUP):
            turned.append(q[r * GRID_W + SHIFT : (r + 1) * GRID_W])
            turned.append(q[r * GRID_W : r * GRID_W + SHIFT])
        q_s[rows, :] = jnp.concatenate(turned, axis=0).astype(BF16)
        kv[place, :width] = part(1).astype(BF16)
        kv[place, width:] = part(2).astype(BF16)

    project(unit(0), True)

    @pl.loop(1, groups - 1)
    def _(k):
        project(jnp.where(upper, k - 1, k + 1), False)

        @pl.when((k == 1) & (sp > 0))
        def _():
            down.start()

        @pl.when((k == groups - 2) & (sp < sp_size - 1))
        def _():
            up.start()

    @pl.loop(1, ranks)
    def _(d):
        gate_copy(d).start()

    contract = (((1,), (1,)), ((), ()))
    size = GROUP * BLOCK
    stack_head = lax.broadcasted_iota(jnp.int32, (size, width), 1) // HEAD_DIM
    first_head = lax.broadcasted_iota(jnp.int32, (size, LANES), 1) < HEAD_DIM
    blocks = GRID_W // BLOCK
    near_keys = KEY_ROWS * STRIP

    def strips(g, b):
        base = aligned(g, group_tokens)
        found = []
        for j in range(KEY_ROWS):
            if b == blocks - 1:
                found.append(pl.ds(base + (j * GRID_W + b * BLOCK), BLOCK))
                found.append(pl.ds(base + j * GRID_W, BLOCK))
            else:
                found.append(pl.ds(base + (j * GRID_W + b * BLOCK), STRIP))
        return found

    def places(g, b):
        base = aligned(g, group_tokens)
        return [pl.ds(base + (r * GRID_W + b * BLOCK), BLOCK) for r in range(GROUP)]

    def stacked(g, b):
        q = jnp.concatenate([q_s[place, :] for place in places(g, b)], axis=0)
        return jnp.concatenate(
            [jnp.where(stack_head == h, q, jnp.zeros_like(q)) for h in range(heads)], axis=0
        )

    def score_near(g, b):
        global_row = sp * grid_rows + g * GROUP
        top = global_row == 0
        bottom = global_row == sp_size * grid_rows - GROUP
        slots = (
            jnp.where(top, 5, jnp.where(bottom, 3, 0)), 1,
            jnp.where(top, 4, jnp.where(bottom, 5, 2)),
        )
        kind = 1 if b == blocks - 1 else 0
        keys = jnp.concatenate([kv[s, :width] for s in strips(g, b)], axis=0)
        s = lax.dot_general(stacked(g, b), keys, contract, preferred_element_type=F32)
        for t in range(TILES):
            lanes = slice(t * LANES, (t + 1) * LANES)
            scores[b, :, lanes] = s[:, lanes] + table[kind, slots[t]]

    def score_far(g, b):
        scores[b, :, near_keys:] = lax.dot_general(
            stacked(g, b), ctx_kv[:, :width], contract, preferred_element_type=F32
        )

    def soften(b):
        sums = []
        for h in range(heads):
            rows = slice(h * size, (h + 1) * size)
            s = scores[b, rows, :]
            p = jnp.exp2(s - jnp.max(s, axis=1, keepdims=True))
            sums.append(jnp.sum(p, axis=1, keepdims=True))
            probs[b, rows, :] = p.astype(BF16)
        return [1.0 / total for total in sums]

    def merge(column, row=None):
        parts = []
        for c in range(width // LANES):
            low, high = 2 * c, 2 * c + 1
            if row is not None:
                lanes = slice(c * LANES, (c + 1) * LANES)
                first = row[low * size : (low + 1) * size, lanes]
                second = row[high * size : (high + 1) * size, lanes]
                if column is not None:
                    first, second = first * column[low], second * column[high]
            else:
                first, second = column[low], column[high]
            parts.append(jnp.where(first_head, first, second))
        return jnp.concatenate(parts, axis=1)

    def place_merged(g, b, merged):
        merged = merged.astype(BF16)
        for r, place in enumerate(places(g, b)):
            stage[place, :] = merged[r * BLOCK : (r + 1) * BLOCK]

    def mix(g, b, inverses):
        values = jnp.concatenate(
            [kv[s, width:] for s in strips(g, b)] + [ctx_kv[:, width:]], axis=0
        )
        mixed = jnp.dot(probs[b], values, preferred_element_type=F32)
        place_merged(g, b, merge(inverses, mixed))

    def head_rows(h):
        return slice(h * size, (h + 1) * size)

    def attend_near(g, b, slot):
        for h in range(heads):
            s = scores[b, head_rows(h), :near_keys]
            peak = jnp.max(s, axis=1, keepdims=True)
            p = jnp.exp2(s - peak)
            spread = (size, LANES)
            stats[slot, b, 0, head_rows(h), :] = jnp.broadcast_to(peak, spread)
            stats[slot, b, 1, head_rows(h), :] = jnp.broadcast_to(
                jnp.sum(p, axis=1, keepdims=True), spread
            )
            probs[b, head_rows(h), :near_keys] = p.astype(BF16)
        values = jnp.concatenate([kv[s, width:] for s in strips(g, b)], axis=0)
        mixed = jnp.dot(probs[b, :, :near_keys], values, preferred_element_type=F32)
        partial[slot, b] = merge(None, mixed)

    def attend_far(g, b, slot):
        keeps, inverses = [], []
        for h in range(heads):
            old = stats[slot, b, 0, head_rows(h), :]
            s = scores[b, head_rows(h), near_keys:]
            peak = jnp.maximum(old, jnp.max(s, axis=1, keepdims=True))
            p = jnp.exp2(s - jnp.concatenate([peak] * (s.shape[1] // LANES), axis=1))
            keep = jnp.exp2(old - peak)
            total = stats[slot, b, 1, head_rows(h), :] * keep
            total = total + jnp.sum(p, axis=1, keepdims=True)
            inverse = 1.0 / total
            inverses.append(inverse)
            keeps.append(keep * inverse)
            probs[b, head_rows(h), near_keys:] = p.astype(BF16)
        mixed = jnp.dot(
            probs[b, :, near_keys:], ctx_kv[:, width:], preferred_element_type=F32
        )
        place_merged(g, b, partial[slot, b] * merge(keeps) + merge(inverses, mixed))

    def piece_copy(index):
        owner, p = index // pieces, index % pieces
        return to_peer(
            stage.at[pl.ds(aligned(index, piece), piece)],
            recv.at[tp, pl.ds(aligned(p, piece), piece)],
            piece_send, piece_recv.at[tp, p], tp=owner,
        )

    half = groups // 2
    inner = half - 1

    def group_of(own, j):
        return jnp.where(upper != own, (j + 1) % half, half + j)

    def send_pieces(g):
        for n in range(per_group):
            index = g * per_group + n

            @pl.when(index // pieces != tp)
            def _():
                piece_copy(index).start()

    @pl.loop(0, inner)
    def _(k):
        g = group_of(False, k)
        score_near(g, 0)
        for b in range(blocks):
            if b + 1 < blocks:
                score_near(g, b + 1)
            attend_near(g, b, k)

    others = ctx_kv.at[pl.ds(0, (sp_size - 1) * context_rows)]
    to_peer(others, others, ctx_send, ctx_recv, sp=(sp + 1) % sp_size).wait()

    @pl.loop(0, inner)
    def _(k):
        g = group_of(False, k)
        for b in range(blocks):
            score_far(g, b)
        for b in range(blocks):
            attend_far(g, b, k)
        send_pieces(g)

    project(unit(groups - 1), False)

    @pl.loop(0, groups - inner)
    def _(k):
        edge = (k == 2) | (k == groups - inner - 1)
        own = k != 2
        j = jnp.where(edge, inner, jnp.where(k > 2, k - 1, k))
        g = group_of(own, j)

        @pl.when((g == 0) & (sp > 0))
        def _():
            down.wait_send()
            up.wait_recv()

        @pl.when((g == groups - 1) & (sp < sp_size - 1))
        def _():
            up.wait_send()
            down.wait_recv()

        score_near(g, 0)
        score_far(g, 0)
        for b in range(blocks):
            if b + 1 < blocks:
                score_near(g, b + 1)
                score_far(g, b + 1)
            mix(g, b, soften(b))
        send_pieces(g)

    load_wo.wait()

    wait_all(garrived, gate_send, gate_recv)

    gates = []
    for t in range(tp_size):
        total = garrived[t]
        for s in range(1, sp_size):
            total = total + garrived[s * tp_size + t]
        gates.append(total)
    gate = jnp.concatenate(gates, axis=1)
    chips = tp_size // 2
    chip = tp // 2
    partner = tp + 1 - 2 * (tp % 2)

    def arrival(source, p):
        rows = pl.ds(aligned(p, piece), piece)
        return to_peer(
            stage.at[rows], recv.at[source, rows], piece_send,
            piece_recv.at[source, p], tp=source,
        )

    def product(c, rows):
        pair = jnp.concatenate([recv[2 * c, rows, :], recv[2 * c + 1, rows, :]], axis=1)
        return jnp.dot(
            pair, wo[pl.ds(aligned(c, 2 * width), 2 * width), :], preferred_element_type=F32
        )

    @pl.loop(0, pieces)
    def _(p):
        rows = pl.ds(aligned(p, piece), piece)
        recv[tp, rows, :] = stage[pl.ds(aligned(tp * pieces + p, piece), piece), :]
        arrival(partner, p).wait_recv()
        acc[rows, :] = product(chip, rows)

    @pl.loop(0, pieces)
    def _(k):
        p = jnp.where(tp == 0, (k + per_group) % pieces, k)
        rows = pl.ds(aligned(p, piece), piece)
        own = pl.ds(aligned(tp * pieces + p, piece), piece)
        branch = acc[rows, :]
        for d in range(1, chips):
            c = (chip + d) % chips
            arrival(2 * c, p).wait_recv()
            arrival(2 * c + 1, p).wait_recv()
            branch = branch + product(c, rows)
        turned = []
        for r in range(piece_rows):
            turned.append(branch[(r + 1) * GRID_W - SHIFT : (r + 1) * GRID_W])
            turned.append(branch[r * GRID_W : (r + 1) * GRID_W - SHIFT])
        branch = jnp.concatenate(turned, axis=0)
        out_ref[rows, :] = (lat[own, :].astype(F32) + gate * branch).astype(BF16)

    sent = stage.at[pl.ds(0, tokens - share)]
    to_peer(sent, sent, piece_send, piece_recv.at[0, 0], tp=partner).wait_send()


def local(
    latent, condition, context_tokens, context_condition, shift_weight, scale_weight,
    gate_weight, norm_gain, query_weight, key_weight, value_weight, out_weight, offset_bias,
):
    sp_size, tp_size = lax.axis_size("sp"), lax.axis_size("tp")
    ranks = sp_size * tp_size
    tokens, depth = latent.shape
    context_rows = context_tokens.shape[0]
    input_rows, piece_cols = shift_weight.shape
    width = query_weight.shape[1]
    heads = width // HEAD_DIM
    groups = tokens // GRID_W // GROUP
    group_tokens = GROUP * GRID_W
    share = tokens // tp_size
    piece_rows = gcd(GROUP, share // GRID_W)
    pieces = share // (piece_rows * GRID_W)
    stacked = heads * GROUP * BLOCK
    keys = KEY_ROWS * STRIP + sp_size * context_rows
    bias = jnp.transpose(offset_bias, (1, 0, 2))
    dma = pltpu.SemaphoreType.DMA
    vmem = pltpu.VMEM
    hbm = pl.BlockSpec(memory_space=pl.ANY)
    return pl.pallas_call(
        kernel,
        in_specs=[hbm] * 13,
        out_specs=pl.BlockSpec(memory_space=pltpu.VMEM),
        out_shape=pltpu.VMEM((share, depth), BF16),
        scratch_shapes=[
            vmem((depth,), BF16), vmem((depth,), BF16), vmem((depth,), BF16),
            vmem((8, depth), F32),
            vmem((3, input_rows, piece_cols), BF16),
            vmem(bias.shape, F32),
            vmem((bias.shape[0], heads, LANES), F32),
            vmem((2, 6, heads * GROUP * BLOCK, LANES), F32),
            vmem((context_rows, depth), BF16),
            vmem((context_rows + 16, depth), BF16),
            vmem((tokens, depth), BF16),
            vmem((group_tokens + 16, depth), BF16),
            vmem((depth, 3 * width), BF16),
            vmem(out_weight.shape, BF16),
            vmem((2, piece_cols), F32),
            vmem((ranks, 2, piece_cols), F32),
            vmem((2, piece_cols), F32),
            vmem((ranks, 2, piece_cols), F32),
            vmem((1, piece_cols), F32),
            vmem((ranks, 1, piece_cols), F32),
            vmem((4, depth), F32),
            vmem((1, 3 * width), F32),
            vmem((tokens, LANES), F32),
            vmem((tokens, width), BF16),
            vmem((tokens + 2 * HALO * GRID_W, 2 * width), BF16),
            vmem((sp_size * context_rows, 2 * width), BF16),
            vmem((GRID_W // BLOCK, stacked, keys), F32),
            vmem((GRID_W // BLOCK, stacked, keys), BF16),
            vmem((groups // 2 - 1, GRID_W // BLOCK, GROUP * BLOCK, width), F32),
            vmem((groups // 2 - 1, GRID_W // BLOCK, 2, stacked, LANES), F32),
            vmem((tokens, width), BF16),
            vmem((tp_size, share, width), BF16),
            vmem((share, depth), F32),
            dma((12,)), dma((groups,)), dma, dma, dma, dma, dma, dma, dma((2,)), dma((2,)),
            dma, dma, dma, dma((tp_size, pieces)),
        ],
        compiler_params=pltpu.CompilerParams(
            vmem_limit_bytes=60 * 2**20, collective_id=0, has_side_effects=True
        ),
        cost_estimate=pl.CostEstimate(
            flops=6 * tokens * depth * width,
            bytes_accessed=2 * (tokens * depth + 3 * depth * width + share * depth),
            transcendentals=0,
        ),
    )(
        condition, context_condition, norm_gain, shift_weight, scale_weight, gate_weight, bias,
        context_tokens, latent, query_weight, key_weight, value_weight, out_weight,
    )


def solution(mesh):
    placed = (
        P(("grp", "sp"), None),
        P("grp"),
        P(("grp", "sp"), None),
        P(),
        P("sp", "tp"),
        P("sp", "tp"),
        P("sp", "tp"),
        P(),
        P(None, "tp"),
        P(None, "tp"),
        P(None, "tp"),
        P(),
        P("tp", None, None),
    )
    return jax.shard_map(
        local, mesh=mesh, in_specs=placed, out_specs=P(("grp", "sp", "tp"), None), check_vma=False
    )
```

```python
import functools

import jax
import jax.numpy as jnp
from jax import lax
from jax.experimental import pallas as pl
from jax.experimental.pallas import tpu as pltpu
from jax.sharding import PartitionSpec as P

HEAD_DIM = 64
GRID_W = 64
WIN_ROWS = 8
WIN_COLS = 16
HALO = WIN_ROWS // 2
BLOCK = 16
SHIFT = WIN_COLS // 2
STRIP = BLOCK + WIN_COLS
GROUP = 4
KEY_ROWS = GROUP + WIN_ROWS
LANES = 128
SEGMENTS = LANES // STRIP
TILES = KEY_ROWS // SEGMENTS
LOG2E = 1.4426950408889634
epsilon = 1e-06
masked_score = -1e30
F32 = jnp.float32
BF16 = jnp.bfloat16
MESH = pl.DeviceIdType.MESH


def to_peer(src, dst, send, recv, **place):
    return pltpu.make_async_remote_copy(
        src_ref=src, dst_ref=dst, send_sem=send, recv_sem=recv,
        device_id=place, device_id_type=MESH,
    )


def gcd(a, b):
    while b:
        a, b = b, a % b
    return a


def aligned(index, step):
    return pl.multiple_of(index * step, step)


def build_tables(bias_ref, braw, table, heads):
    offsets = bias_ref.shape[0]
    braw[...] = jnp.zeros_like(braw)
    for o in range(offsets):
        braw[o, :, : bias_ref.shape[2]] = bias_ref[o] * LOG2E
    lane_h = lax.broadcasted_iota(jnp.int32, (heads, LANES), 1) // STRIP
    first = HALO - 1
    combined = []
    for o in range(first - (GROUP - 1), first + (TILES - 1) * SEGMENTS + 1):
        row = braw[o]
        for j in range(1, SEGMENTS):
            row = jnp.where(lane_h == j, pltpu.roll(braw[o + j], STRIP * j, 1), row)
        combined.append(row)
    u = lax.broadcasted_iota(jnp.int32, (BLOCK, LANES), 0)
    lane = lax.broadcasted_iota(jnp.int32, (BLOCK, LANES), 1)
    v = lane % STRIP
    inner = (v >= u) & (v < u + WIN_COLS)
    edge = ((u < SHIFT) & (v < WIN_COLS)) | ((u >= SHIFT) & (v >= WIN_COLS))
    for t in range(TILES):
        for i in range(GROUP):
            j = t * SEGMENTS + lane // STRIP
            seen = (j >= i) & (j < i + WIN_ROWS)
            whole = t * SEGMENTS >= i and (t + 1) * SEGMENTS <= i + WIN_ROWS
            source = combined[t * SEGMENTS + GROUP - 1 - i]
            for h in range(heads):
                spread = jnp.broadcast_to(source[h : h + 1, :], (BLOCK, LANES))
                value = pltpu.roll(spread, LANES - (SHIFT - 1), 1, stride=1, stride_axis=0)
                place = slice((h * GROUP + i) * BLOCK, (h * GROUP + i + 1) * BLOCK)
                for kind, mask in enumerate((inner, edge)):
                    full = jnp.where(mask, value, masked_score)
                    table[kind, t, place, :] = (
                        full if whole else jnp.where(seen, full, masked_score)
                    )
                    if t != 1:
                        table[kind, 3 if t == 0 else 4, place, :] = full
    for kind in range(2):
        table[kind, 5] = jnp.full(table.shape[2:], masked_score, F32)


def kernel(
    cond_hbm, ctxcond_hbm, gain_hbm, shift_hbm, scale_hbm, gate_hbm, bias_hbm, ctx_hbm,
    lat_hbm, wq_hbm, wk_hbm, wv_hbm, wo_hbm,
    out_ref,
    cond, ctxcond, gain, small, modw, bias, braw, table, ctx, cblk, lat, xs, wqkv, wo,
    cterms, carrived, terms, arrived, gterms, garrived, vectors, added, inv, q_s, kv, ctx_kv,
    scores, probs, partial, stats, stage, recv, acc,
    load_sem, lat_sem, cterm_send, cterm_recv, term_send, term_recv, gate_send, gate_recv,
    halo_send, halo_recv, ctx_send, ctx_recv, piece_send, piece_recv,
):
    sp, tp = lax.axis_index("sp"), lax.axis_index("tp")
    sp_size, tp_size = lax.axis_size("sp"), lax.axis_size("tp")
    ranks = sp_size * tp_size
    me = sp * tp_size + tp
    tokens, depth = lat.shape
    width = wq_hbm.shape[1]
    heads = width // HEAD_DIM
    input_rows, piece_cols = modw.shape[1:]
    context_rows = ctx.shape[0]
    grid_rows = tokens // GRID_W
    groups = grid_rows // GROUP
    group_tokens = GROUP * GRID_W
    halo = HALO * GRID_W
    below = (HALO - 1) * GRID_W
    share = tokens // tp_size
    piece_rows = gcd(GROUP, share // GRID_W)
    piece = piece_rows * GRID_W
    pieces = share // piece
    per_group = GROUP // piece_rows

    def peer(d):
        other = (me + d) % ranks
        return dict(sp=other // tp_size, tp=other % tp_size)

    barrier = pltpu.get_barrier_semaphore()

    early = [
        pltpu.make_async_copy(cond_hbm, cond, load_sem.at[0]),
        pltpu.make_async_copy(ctxcond_hbm, ctxcond, load_sem.at[1]),
        pltpu.make_async_copy(gain_hbm, gain, load_sem.at[2]),
        pltpu.make_async_copy(shift_hbm, modw.at[0], load_sem.at[3]),
        pltpu.make_async_copy(scale_hbm, modw.at[1], load_sem.at[4]),
        pltpu.make_async_copy(gate_hbm, modw.at[2], load_sem.at[5]),
    ]
    load_bias = pltpu.make_async_copy(bias_hbm, bias, load_sem.at[6])
    load_ctx = pltpu.make_async_copy(ctx_hbm, ctx, load_sem.at[7])
    load_weights = [
        pltpu.make_async_copy(w, wqkv.at[:, pl.ds(i * width, width)], load_sem.at[8 + i])
        for i, w in enumerate((wq_hbm, wk_hbm, wv_hbm))
    ]
    load_wo = pltpu.make_async_copy(wo_hbm, wo, load_sem.at[11])

    def load_lat(i):
        rows = pl.ds(aligned(i, group_tokens), group_tokens)
        return pltpu.make_async_copy(lat_hbm.at[rows], lat.at[rows], lat_sem.at[i])

    @pl.loop(1, ranks)
    def _(d):
        pl.semaphore_signal(barrier, inc=1, device_id=peer(d), device_id_type=MESH)

    for load in early:
        load.start()

    load_bias.start()
    load_ctx.start()

    @pl.loop(0, groups)
    def _(i):
        load_lat(i).start()

    for load in load_weights:
        load.start()
    load_wo.start()

    for load in early:
        load.wait()
    small[0:1, :] = cond[...].astype(F32).reshape(1, depth)
    small[1:2, :] = ctxcond[...].astype(F32).reshape(1, depth)
    small[2:3, :] = gain[...].astype(F32).reshape(1, depth)
    row8 = lax.broadcasted_iota(jnp.int32, (8, input_rows), 0)
    own_inputs = pl.ds(aligned(sp, input_rows), input_rows)
    value = jnp.where(row8 == 0, small[0:1, own_inputs], small[1:2, own_inputs])
    act = (value / (1.0 + jnp.exp(-value))).astype(BF16)
    products = []
    for i in range(2):
        both = jnp.dot(act, modw[i], preferred_element_type=F32)
        products.append(both)
    cterms[...] = jnp.concatenate([both[1:2] for both in products], axis=0).astype(BF16)
    terms[...] = jnp.concatenate([both[0:1] for both in products], axis=0).astype(BF16)
    gterms[...] = jnp.dot(act, modw[2], preferred_element_type=F32)[:1]
    carrived[me] = cterms[...]
    arrived[me] = terms[...]
    garrived[me] = gterms[...]

    def wait_all(slots, send, recv_sem):
        all_but_one = slots.at[pl.ds(0, ranks - 1)]
        to_peer(all_but_one, all_but_one, send, recv_sem, **peer(1)).wait()

    def cterm_copy(d):
        return to_peer(
            cterms, carrived.at[me], cterm_send, cterm_recv, **peer(d)
        )

    def term_copy(d):
        return to_peer(terms, arrived.at[me], term_send, term_recv, **peer(d))

    def gate_copy(d):
        return to_peer(gterms, garrived.at[me], gate_send, gate_recv, **peer(d))

    load_bias.wait()
    build_tables(bias, braw, table, heads)
    pl.semaphore_wait(barrier, ranks - 1)

    @pl.loop(1, ranks)
    def _(d):
        cterm_copy(d).start()

    @pl.loop(1, ranks)
    def _(d):
        term_copy(d).start()

    @pl.when(sp == 0)
    def _():
        kv[0:halo, :] = jnp.zeros((halo, 2 * width), BF16)

    @pl.when(sp == sp_size - 1)
    def _():
        kv[halo + tokens : halo + tokens + below, :] = jnp.zeros((below, 2 * width), BF16)

    kv[halo + tokens + below :, :] = jnp.zeros((halo - below, 2 * width), BF16)

    def inverse_of(ref, rows):
        total = None
        for c in range(depth // LANES):
            x = ref[rows, c * LANES : (c + 1) * LANES].astype(F32)
            total = x * x if total is None else total + x * x
        mean = jnp.sum(total, axis=1, keepdims=True) * (1.0 / depth)
        return lax.rsqrt(mean + epsilon)

    load_ctx.wait()
    inv_ctx = inverse_of(ctx, slice(None))

    @pl.loop(0, groups)
    def _(i):
        load_lat(i).wait()
        for r in range(0, group_tokens, 128):
            rows = pl.ds(aligned(i, group_tokens) + r, 128)
            inv[rows, :] = jnp.broadcast_to(inverse_of(lat, rows), (128, LANES))

    for load in load_weights:
        load.wait()

    def sum_terms(ref, rows):
        for t in range(tp_size):
            total = ref[t].astype(F32)
            for s in range(1, sp_size):
                total = total + ref[s * tp_size + t].astype(F32)
            vectors[rows, t * piece_cols : (t + 1) * piece_cols] = total

    wait_all(carrived, cterm_send, cterm_recv)

    sum_terms(carrived, slice(0, 2))
    row16 = lax.broadcasted_iota(jnp.int32, (16, depth), 0)
    factor_ctx = (small[2:3, :] * (1.0 + vectors[1:2, :])).astype(BF16)
    cblk[:context_rows, :] = ctx[...] * factor_ctx
    cblk[context_rows:, :] = jnp.where(row16 == 0, vectors[0:1, :], 0.0).astype(BF16)
    block = jnp.dot(cblk[...], wqkv[:, width:], preferred_element_type=F32)
    ctx_place = pl.ds(aligned(sp, context_rows), context_rows)
    ctx_kv[ctx_place, :] = (
        block[:context_rows] * inv_ctx + block[context_rows : context_rows + 1]
    ).astype(BF16)

    def ctx_copy(d):
        return to_peer(
            ctx_kv.at[ctx_place], ctx_kv.at[ctx_place], ctx_send, ctx_recv,
            sp=(sp + d) % sp_size, tp=tp,
        )

    @pl.loop(1, sp_size)
    def _(d):
        ctx_copy(d).start()

    down = to_peer(
        kv.at[pl.ds(halo, below)], kv.at[pl.ds(halo + tokens, below)],
        halo_send.at[0], halo_recv.at[0], sp=jnp.maximum(sp - 1, 0),
    )
    up = to_peer(
        kv.at[pl.ds(tokens, halo)], kv.at[pl.ds(0, halo)],
        halo_send.at[1], halo_recv.at[1], sp=jnp.minimum(sp + 1, sp_size - 1),
    )

    wait_all(arrived, term_send, term_recv)

    sum_terms(arrived, slice(2, 4))
    factor = (small[2:3, :] * (1.0 + vectors[3:4, :])).astype(BF16)
    xs[group_tokens:, :] = jnp.where(row16 == 0, vectors[2:3, :], 0.0).astype(BF16)

    upper = tp * 2 >= tp_size

    def unit(k):
        if k == 0:
            return jnp.where(upper, groups - 1, 0)
        if k == groups - 1:
            return jnp.where(upper, groups - 2, 1)
        return jnp.where(upper, k - 1, k + 1)

    def project(i, first):
        rows = pl.ds(aligned(i, group_tokens), group_tokens)
        place = pl.ds(aligned(i, group_tokens) + halo, group_tokens)
        xs[:group_tokens, :] = lat[rows, :] * factor
        scale = jnp.concatenate([inv[rows, :]] * (width // LANES), axis=1)

        def part(n):
            columns = slice(n * width, (n + 1) * width)
            left = xs[...] if first else xs[:group_tokens, :]
            y = jnp.dot(left, wqkv[:, columns], preferred_element_type=F32)
            if first:
                added[0:1, columns] = y[group_tokens : group_tokens + 1]
            return y[:group_tokens] * scale + added[0:1, columns]

        q = part(0) * (HEAD_DIM**-0.5 * LOG2E)
        turned = []
        for r in range(GROUP):
            turned.append(q[r * GRID_W + SHIFT : (r + 1) * GRID_W])
            turned.append(q[r * GRID_W : r * GRID_W + SHIFT])
        q_s[rows, :] = jnp.concatenate(turned, axis=0).astype(BF16)
        kv[place, :width] = part(1).astype(BF16)
        kv[place, width:] = part(2).astype(BF16)

    project(unit(0), True)

    @pl.loop(1, groups - 1)
    def _(k):
        project(jnp.where(upper, k - 1, k + 1), False)

        @pl.when((k == 1) & (sp > 0))
        def _():
            down.start()

        @pl.when((k == groups - 2) & (sp < sp_size - 1))
        def _():
            up.start()

    @pl.loop(1, ranks)
    def _(d):
        gate_copy(d).start()

    contract = (((1,), (1,)), ((), ()))
    size = GROUP * BLOCK
    stack_head = lax.broadcasted_iota(jnp.int32, (size, width), 1) // HEAD_DIM
    first_head = lax.broadcasted_iota(jnp.int32, (size, LANES), 1) < HEAD_DIM
    blocks = GRID_W // BLOCK
    near_keys = KEY_ROWS * STRIP

    def strips(g, b):
        base = aligned(g, group_tokens)
        found = []
        for j in range(KEY_ROWS):
            if b == blocks - 1:
                found.append(pl.ds(base + (j * GRID_W + b * BLOCK), BLOCK))
                found.append(pl.ds(base + j * GRID_W, BLOCK))
            else:
                found.append(pl.ds(base + (j * GRID_W + b * BLOCK), STRIP))
        return found

    def places(g, b):
        base = aligned(g, group_tokens)
        return [pl.ds(base + (r * GRID_W + b * BLOCK), BLOCK) for r in range(GROUP)]

    def stacked(g, b):
        q = jnp.concatenate([q_s[place, :] for place in places(g, b)], axis=0)
        return jnp.concatenate(
            [jnp.where(stack_head == h, q, jnp.zeros_like(q)) for h in range(heads)], axis=0
        )

    def score_near(g, b):
        global_row = sp * grid_rows + g * GROUP
        top = global_row == 0
        bottom = global_row == sp_size * grid_rows - GROUP
        slots = (
            jnp.where(top, 5, jnp.where(bottom, 3, 0)), 1,
            jnp.where(top, 4, jnp.where(bottom, 5, 2)),
        )
        kind = 1 if b == blocks - 1 else 0
        keys = jnp.concatenate([kv[s, :width] for s in strips(g, b)], axis=0)
        s = lax.dot_general(stacked(g, b), keys, contract, preferred_element_type=F32)
        for t in range(TILES):
            lanes = slice(t * LANES, (t + 1) * LANES)
            scores[b, :, lanes] = s[:, lanes] + table[kind, slots[t]]

    def score_far(g, b):
        scores[b, :, near_keys:] = lax.dot_general(
            stacked(g, b), ctx_kv[:, :width], contract, preferred_element_type=F32
        )

    def soften(b):
        sums = []
        for h in range(heads):
            rows = slice(h * size, (h + 1) * size)
            s = scores[b, rows, :]
            p = jnp.exp2(s - jnp.max(s, axis=1, keepdims=True))
            sums.append(jnp.sum(p, axis=1, keepdims=True))
            probs[b, rows, :] = p.astype(BF16)
        return [1.0 / total for total in sums]

    def merge(column, row=None):
        parts = []
        for c in range(width // LANES):
            low, high = 2 * c, 2 * c + 1
            if row is not None:
                lanes = slice(c * LANES, (c + 1) * LANES)
                first = row[low * size : (low + 1) * size, lanes]
                second = row[high * size : (high + 1) * size, lanes]
                if column is not None:
                    first, second = first * column[low], second * column[high]
            else:
                first, second = column[low], column[high]
            parts.append(jnp.where(first_head, first, second))
        return jnp.concatenate(parts, axis=1)

    def place_merged(g, b, merged):
        merged = merged.astype(BF16)
        for r, place in enumerate(places(g, b)):
            stage[place, :] = merged[r * BLOCK : (r + 1) * BLOCK]

    def mix(g, b, inverses):
        values = jnp.concatenate(
            [kv[s, width:] for s in strips(g, b)] + [ctx_kv[:, width:]], axis=0
        )
        mixed = jnp.dot(probs[b], values, preferred_element_type=F32)
        place_merged(g, b, merge(inverses, mixed))

    def head_rows(h):
        return slice(h * size, (h + 1) * size)

    def attend_near(g, b, slot):
        for h in range(heads):
            s = scores[b, head_rows(h), :near_keys]
            peak = jnp.max(s, axis=1, keepdims=True)
            p = jnp.exp2(s - peak)
            spread = (size, LANES)
            stats[slot, b, 0, head_rows(h), :] = jnp.broadcast_to(peak, spread)
            stats[slot, b, 1, head_rows(h), :] = jnp.broadcast_to(
                jnp.sum(p, axis=1, keepdims=True), spread
            )
            probs[b, head_rows(h), :near_keys] = p.astype(BF16)
        values = jnp.concatenate([kv[s, width:] for s in strips(g, b)], axis=0)
        mixed = jnp.dot(probs[b, :, :near_keys], values, preferred_element_type=F32)
        partial[slot, b] = merge(None, mixed)

    def attend_far(g, b, slot):
        keeps, inverses = [], []
        for h in range(heads):
            old = stats[slot, b, 0, head_rows(h), :]
            s = scores[b, head_rows(h), near_keys:]
            peak = jnp.maximum(old, jnp.max(s, axis=1, keepdims=True))
            p = jnp.exp2(s - jnp.concatenate([peak] * (s.shape[1] // LANES), axis=1))
            keep = jnp.exp2(old - peak)
            total = stats[slot, b, 1, head_rows(h), :] * keep
            total = total + jnp.sum(p, axis=1, keepdims=True)
            inverse = 1.0 / total
            inverses.append(inverse)
            keeps.append(keep * inverse)
            probs[b, head_rows(h), near_keys:] = p.astype(BF16)
        mixed = jnp.dot(
            probs[b, :, near_keys:], ctx_kv[:, width:], preferred_element_type=F32
        )
        place_merged(g, b, partial[slot, b] * merge(keeps) + merge(inverses, mixed))

    def piece_copy(index):
        owner, p = index // pieces, index % pieces
        return to_peer(
            stage.at[pl.ds(aligned(index, piece), piece)],
            recv.at[tp, pl.ds(aligned(p, piece), piece)],
            piece_send, piece_recv.at[tp, p], tp=owner,
        )

    half = groups // 2
    inner = half - 1

    def group_of(own, j):
        return jnp.where(upper != own, (j + 1) % half, half + j)

    def send_pieces(g):
        for n in range(per_group):
            index = g * per_group + n

            @pl.when(index // pieces != tp)
            def _():
                piece_copy(index).start()

    @pl.loop(0, inner)
    def _(k):
        g = group_of(False, k)
        score_near(g, 0)
        for b in range(blocks):
            if b + 1 < blocks:
                score_near(g, b + 1)
            attend_near(g, b, k)

    others = ctx_kv.at[pl.ds(0, (sp_size - 1) * context_rows)]
    to_peer(others, others, ctx_send, ctx_recv, sp=(sp + 1) % sp_size).wait()

    @pl.loop(0, inner)
    def _(k):
        g = group_of(False, k)
        for b in range(blocks):
            score_far(g, b)
        for b in range(blocks):
            attend_far(g, b, k)
        send_pieces(g)

    project(unit(groups - 1), False)

    @pl.loop(0, groups - inner)
    def _(k):
        edge = (k == 2) | (k == groups - inner - 1)
        own = k != 2
        j = jnp.where(edge, inner, jnp.where(k > 2, k - 1, k))
        g = group_of(own, j)

        @pl.when((g == 0) & (sp > 0))
        def _():
            down.wait_send()
            up.wait_recv()

        @pl.when((g == groups - 1) & (sp < sp_size - 1))
        def _():
            up.wait_send()
            down.wait_recv()

        score_near(g, 0)
        score_far(g, 0)
        for b in range(blocks):
            if b + 1 < blocks:
                score_near(g, b + 1)
                score_far(g, b + 1)
            mix(g, b, soften(b))
        send_pieces(g)

    load_wo.wait()

    wait_all(garrived, gate_send, gate_recv)

    gates = []
    for t in range(tp_size):
        total = garrived[t]
        for s in range(1, sp_size):
            total = total + garrived[s * tp_size + t]
        gates.append(total)
    gate = jnp.concatenate(gates, axis=1)
    chips = tp_size // 2
    chip = tp // 2
    partner = tp + 1 - 2 * (tp % 2)

    def arrival(source, p):
        rows = pl.ds(aligned(p, piece), piece)
        return to_peer(
            stage.at[rows], recv.at[source, rows], piece_send,
            piece_recv.at[source, p], tp=source,
        )

    def product(c, rows):
        pair = jnp.concatenate([recv[2 * c, rows, :], recv[2 * c + 1, rows, :]], axis=1)
        return jnp.dot(
            pair, wo[pl.ds(aligned(c, 2 * width), 2 * width), :], preferred_element_type=F32
        )

    @pl.loop(0, pieces)
    def _(p):
        rows = pl.ds(aligned(p, piece), piece)
        recv[tp, rows, :] = stage[pl.ds(aligned(tp * pieces + p, piece), piece), :]
        arrival(partner, p).wait_recv()
        acc[rows, :] = product(chip, rows)

    @pl.loop(0, pieces)
    def _(k):
        p = jnp.where(tp == 0, (k + per_group) % pieces, k)
        rows = pl.ds(aligned(p, piece), piece)
        own = pl.ds(aligned(tp * pieces + p, piece), piece)
        branch = acc[rows, :]
        for d in range(1, chips):
            c = (chip + d) % chips
            arrival(2 * c, p).wait_recv()
            arrival(2 * c + 1, p).wait_recv()
            branch = branch + product(c, rows)
        turned = []
        for r in range(piece_rows):
            turned.append(branch[(r + 1) * GRID_W - SHIFT : (r + 1) * GRID_W])
            turned.append(branch[r * GRID_W : (r + 1) * GRID_W - SHIFT])
        branch = jnp.concatenate(turned, axis=0)
        out_ref[rows, :] = (lat[own, :].astype(F32) + gate * branch).astype(BF16)

    sent = stage.at[pl.ds(0, tokens - share)]
    to_peer(sent, sent, piece_send, piece_recv.at[0, 0], tp=partner).wait_send()


def local(
    latent, condition, context_tokens, context_condition, shift_weight, scale_weight,
    gate_weight, norm_gain, query_weight, key_weight, value_weight, out_weight, offset_bias,
):
    sp_size, tp_size = lax.axis_size("sp"), lax.axis_size("tp")
    ranks = sp_size * tp_size
    tokens, depth = latent.shape
    context_rows = context_tokens.shape[0]
    input_rows, piece_cols = shift_weight.shape
    width = query_weight.shape[1]
    heads = width // HEAD_DIM
    groups = tokens // GRID_W // GROUP
    group_tokens = GROUP * GRID_W
    share = tokens // tp_size
    piece_rows = gcd(GROUP, share // GRID_W)
    pieces = share // (piece_rows * GRID_W)
    stacked = heads * GROUP * BLOCK
    keys = KEY_ROWS * STRIP + sp_size * context_rows
    bias = jnp.transpose(offset_bias, (1, 0, 2))
    dma = pltpu.SemaphoreType.DMA
    vmem = pltpu.VMEM
    hbm = pl.BlockSpec(memory_space=pl.ANY)
    return pl.pallas_call(
        kernel,
        in_specs=[hbm] * 13,
        out_specs=pl.BlockSpec(memory_space=pltpu.VMEM),
        out_shape=pltpu.VMEM((share, depth), BF16),
        scratch_shapes=[
            vmem((depth,), BF16), vmem((depth,), BF16), vmem((depth,), BF16),
            vmem((8, depth), F32),
            vmem((3, input_rows, piece_cols), BF16),
            vmem(bias.shape, F32),
            vmem((bias.shape[0], heads, LANES), F32),
            vmem((2, 6, heads * GROUP * BLOCK, LANES), F32),
            vmem((context_rows, depth), BF16),
            vmem((context_rows + 16, depth), BF16),
            vmem((tokens, depth), BF16),
            vmem((group_tokens + 16, depth), BF16),
            vmem((depth, 3 * width), BF16),
            vmem(out_weight.shape, BF16),
            vmem((2, piece_cols), BF16),
            vmem((ranks, 2, piece_cols), BF16),
            vmem((2, piece_cols), BF16),
            vmem((ranks, 2, piece_cols), BF16),
            vmem((1, piece_cols), F32),
            vmem((ranks, 1, piece_cols), F32),
            vmem((4, depth), F32),
            vmem((1, 3 * width), F32),
            vmem((tokens, LANES), F32),
            vmem((tokens, width), BF16),
            vmem((tokens + 2 * HALO * GRID_W, 2 * width), BF16),
            vmem((sp_size * context_rows, 2 * width), BF16),
            vmem((GRID_W // BLOCK, stacked, keys), F32),
            vmem((GRID_W // BLOCK, stacked, keys), BF16),
            vmem((groups // 2 - 1, GRID_W // BLOCK, GROUP * BLOCK, width), F32),
            vmem((groups // 2 - 1, GRID_W // BLOCK, 2, stacked, LANES), F32),
            vmem((tokens, width), BF16),
            vmem((tp_size, share, width), BF16),
            vmem((share, depth), F32),
            dma((12,)), dma((groups,)), dma, dma, dma, dma, dma, dma, dma((2,)), dma((2,)),
            dma, dma, dma, dma((tp_size, pieces)),
        ],
        compiler_params=pltpu.CompilerParams(
            vmem_limit_bytes=60 * 2**20, collective_id=0, has_side_effects=True
        ),
        cost_estimate=pl.CostEstimate(
            flops=6 * tokens * depth * width,
            bytes_accessed=2 * (tokens * depth + 3 * depth * width + share * depth),
            transcendentals=0,
        ),
    )(
        condition, context_condition, norm_gain, shift_weight, scale_weight, gate_weight, bias,
        context_tokens, latent, query_weight, key_weight, value_weight, out_weight,
    )


def solution(mesh):
    placed = (
        P(("grp", "sp"), None),
        P("grp"),
        P(("grp", "sp"), None),
        P(),
        P("sp", "tp"),
        P("sp", "tp"),
        P("sp", "tp"),
        P(),
        P(None, "tp"),
        P(None, "tp"),
        P(None, "tp"),
        P(),
        P("tp", None, None),
    )
    return jax.shard_map(
        local, mesh=mesh, in_specs=placed, out_specs=P(("grp", "sp", "tp"), None), check_vma=False
    )
```

```python
import functools

import jax
import jax.numpy as jnp
from jax import lax
from jax.experimental import pallas as pl
from jax.experimental.pallas import tpu as pltpu
from jax.sharding import PartitionSpec as P

HEAD_DIM = 64
GRID_W = 64
WIN_ROWS = 8
WIN_COLS = 16
HALO = WIN_ROWS // 2
BLOCK = 16
SHIFT = WIN_COLS // 2
STRIP = BLOCK + WIN_COLS
GROUP = 4
KEY_ROWS = GROUP + WIN_ROWS
LANES = 128
SEGMENTS = LANES // STRIP
TILES = KEY_ROWS // SEGMENTS
LOG2E = 1.4426950408889634
epsilon = 1e-06
masked_score = -1e30
F32 = jnp.float32
BF16 = jnp.bfloat16
MESH = pl.DeviceIdType.MESH


def to_peer(src, dst, send, recv, **place):
    return pltpu.make_async_remote_copy(
        src_ref=src, dst_ref=dst, send_sem=send, recv_sem=recv,
        device_id=place, device_id_type=MESH,
    )


def gcd(a, b):
    while b:
        a, b = b, a % b
    return a


def aligned(index, step):
    return pl.multiple_of(index * step, step)


def build_tables(bias_ref, braw, table, heads):
    offsets = bias_ref.shape[0]
    braw[...] = jnp.zeros_like(braw)
    for o in range(offsets):
        braw[o, :, : bias_ref.shape[2]] = bias_ref[o] * LOG2E
    lane_h = lax.broadcasted_iota(jnp.int32, (heads, LANES), 1) // STRIP
    first = HALO - 1
    combined = []
    for o in range(first - (GROUP - 1), first + (TILES - 1) * SEGMENTS + 1):
        row = braw[o]
        for j in range(1, SEGMENTS):
            row = jnp.where(lane_h == j, pltpu.roll(braw[o + j], STRIP * j, 1), row)
        combined.append(row)
    u = lax.broadcasted_iota(jnp.int32, (BLOCK, LANES), 0)
    lane = lax.broadcasted_iota(jnp.int32, (BLOCK, LANES), 1)
    v = lane % STRIP
    inner = (v >= u) & (v < u + WIN_COLS)
    edge = ((u < SHIFT) & (v < WIN_COLS)) | ((u >= SHIFT) & (v >= WIN_COLS))
    for t in range(TILES):
        for i in range(GROUP):
            j = t * SEGMENTS + lane // STRIP
            seen = (j >= i) & (j < i + WIN_ROWS)
            whole = t * SEGMENTS >= i and (t + 1) * SEGMENTS <= i + WIN_ROWS
            source = combined[t * SEGMENTS + GROUP - 1 - i]
            for h in range(heads):
                spread = jnp.broadcast_to(source[h : h + 1, :], (BLOCK, LANES))
                value = pltpu.roll(spread, LANES - (SHIFT - 1), 1, stride=1, stride_axis=0)
                place = slice((h * GROUP + i) * BLOCK, (h * GROUP + i + 1) * BLOCK)
                for kind, mask in enumerate((inner, edge)):
                    full = jnp.where(mask, value, masked_score)
                    table[kind, t, place, :] = (
                        full if whole else jnp.where(seen, full, masked_score)
                    )
                    if t != 1:
                        table[kind, 3 if t == 0 else 4, place, :] = full
    for kind in range(2):
        table[kind, 5] = jnp.full(table.shape[2:], masked_score, F32)


def kernel(
    cond_hbm, ctxcond_hbm, gain_hbm, shift_hbm, scale_hbm, gate_hbm, bias_hbm, ctx_hbm,
    lat_hbm, wq_hbm, wk_hbm, wv_hbm, wo_hbm,
    out_ref,
    cond, ctxcond, gain, small, modw, bias, braw, table, ctx, cblk, lat, xs, wqkv, wo,
    cterms, carrived, terms, arrived, gterms, garrived, vectors, added, inv, q_s, kv, ctx_kv,
    scores, probs, partial, stats, stage, recv, acc,
    load_sem, lat_sem, cterm_send, cterm_recv, term_send, term_recv, gate_send, gate_recv,
    halo_send, halo_recv, ctx_send, ctx_recv, piece_send, piece_recv,
):
    sp, tp = lax.axis_index("sp"), lax.axis_index("tp")
    sp_size, tp_size = lax.axis_size("sp"), lax.axis_size("tp")
    ranks = sp_size * tp_size
    me = sp * tp_size + tp
    tokens, depth = lat.shape
    width = wq_hbm.shape[1]
    heads = width // HEAD_DIM
    input_rows, piece_cols = modw.shape[1:]
    context_rows = ctx.shape[0]
    grid_rows = tokens // GRID_W
    groups = grid_rows // GROUP
    group_tokens = GROUP * GRID_W
    halo = HALO * GRID_W
    below = (HALO - 1) * GRID_W
    share = tokens // tp_size
    piece_rows = gcd(GROUP, share // GRID_W)
    piece = piece_rows * GRID_W
    pieces = share // piece
    per_group = GROUP // piece_rows

    def peer(d):
        other = (me + d) % ranks
        return dict(sp=other // tp_size, tp=other % tp_size)

    barrier = pltpu.get_barrier_semaphore()

    early = [
        pltpu.make_async_copy(cond_hbm, cond, load_sem.at[0]),
        pltpu.make_async_copy(ctxcond_hbm, ctxcond, load_sem.at[1]),
        pltpu.make_async_copy(gain_hbm, gain, load_sem.at[2]),
        pltpu.make_async_copy(shift_hbm, modw.at[0], load_sem.at[3]),
        pltpu.make_async_copy(scale_hbm, modw.at[1], load_sem.at[4]),
        pltpu.make_async_copy(gate_hbm, modw.at[2], load_sem.at[5]),
    ]
    load_bias = pltpu.make_async_copy(bias_hbm, bias, load_sem.at[6])
    load_ctx = pltpu.make_async_copy(ctx_hbm, ctx, load_sem.at[7])
    load_weights = [
        pltpu.make_async_copy(w, wqkv.at[:, pl.ds(i * width, width)], load_sem.at[8 + i])
        for i, w in enumerate((wq_hbm, wk_hbm, wv_hbm))
    ]
    load_wo = pltpu.make_async_copy(wo_hbm, wo, load_sem.at[11])

    def load_lat(i):
        rows = pl.ds(aligned(i, group_tokens), group_tokens)
        return pltpu.make_async_copy(lat_hbm.at[rows], lat.at[rows], lat_sem.at[i])

    @pl.loop(1, ranks)
    def _(d):
        pl.semaphore_signal(barrier, inc=1, device_id=peer(d), device_id_type=MESH)

    for load in early:
        load.start()

    load_bias.start()
    load_ctx.start()

    @pl.loop(0, groups)
    def _(i):
        load_lat(i).start()

    for load in load_weights:
        load.start()
    load_wo.start()

    for load in early:
        load.wait()
    small[0:1, :] = cond[...].astype(F32).reshape(1, depth)
    small[1:2, :] = ctxcond[...].astype(F32).reshape(1, depth)
    small[2:3, :] = gain[...].astype(F32).reshape(1, depth)
    row8 = lax.broadcasted_iota(jnp.int32, (8, input_rows), 0)
    own_inputs = pl.ds(aligned(sp, input_rows), input_rows)
    value = jnp.where(row8 == 0, small[0:1, own_inputs], small[1:2, own_inputs])
    act = (value / (1.0 + jnp.exp(-value))).astype(BF16)
    products = []
    for i in range(2):
        both = jnp.dot(act, modw[i], preferred_element_type=F32)
        products.append(both)
    cterms[...] = jnp.concatenate([both[1:2] for both in products], axis=0).astype(BF16)
    terms[...] = jnp.concatenate([both[0:1] for both in products], axis=0).astype(BF16)
    gterms[...] = jnp.dot(act, modw[2], preferred_element_type=F32)[:1]
    carrived[me] = cterms[...]
    arrived[me] = terms[...]
    garrived[me] = gterms[...]

    def wait_all(slots, send, recv_sem):
        all_but_one = slots.at[pl.ds(0, ranks - 1)]
        to_peer(all_but_one, all_but_one, send, recv_sem, **peer(1)).wait()

    def cterm_copy(d):
        return to_peer(
            cterms, carrived.at[me], cterm_send, cterm_recv, **peer(d)
        )

    def term_copy(d):
        return to_peer(terms, arrived.at[me], term_send, term_recv, **peer(d))

    def gate_copy(d):
        return to_peer(gterms, garrived.at[me], gate_send, gate_recv, **peer(d))

    load_bias.wait()
    build_tables(bias, braw, table, heads)
    pl.semaphore_wait(barrier, ranks - 1)

    @pl.loop(1, ranks)
    def _(d):
        cterm_copy(d).start()

    @pl.loop(1, ranks)
    def _(d):
        term_copy(d).start()

    @pl.when(sp == 0)
    def _():
        kv[0:halo, :] = jnp.zeros((halo, 2 * width), BF16)

    @pl.when(sp == sp_size - 1)
    def _():
        kv[halo + tokens : halo + tokens + below, :] = jnp.zeros((below, 2 * width), BF16)

    kv[halo + tokens + below :, :] = jnp.zeros((halo - below, 2 * width), BF16)

    def inverse_of(ref, rows):
        total = None
        for c in range(depth // LANES):
            x = ref[rows, c * LANES : (c + 1) * LANES].astype(F32)
            total = x * x if total is None else total + x * x
        mean = jnp.sum(total, axis=1, keepdims=True) * (1.0 / depth)
        return lax.rsqrt(mean + epsilon)

    load_ctx.wait()
    inv_ctx = inverse_of(ctx, slice(None))

    @pl.loop(0, groups)
    def _(i):
        load_lat(i).wait()
        for r in range(0, group_tokens, 128):
            rows = pl.ds(aligned(i, group_tokens) + r, 128)
            inv[rows, :] = jnp.broadcast_to(inverse_of(lat, rows), (128, LANES))

    for load in load_weights:
        load.wait()

    def sum_terms(ref, rows):
        for t in range(tp_size):
            total = ref[t].astype(F32)
            for s in range(1, sp_size):
                total = total + ref[s * tp_size + t].astype(F32)
            vectors[rows, t * piece_cols : (t + 1) * piece_cols] = total

    wait_all(carrived, cterm_send, cterm_recv)

    sum_terms(carrived, slice(0, 2))
    row16 = lax.broadcasted_iota(jnp.int32, (16, depth), 0)
    factor_ctx = (small[2:3, :] * (1.0 + vectors[1:2, :])).astype(BF16)
    cblk[:context_rows, :] = ctx[...] * factor_ctx
    cblk[context_rows:, :] = jnp.where(row16 == 0, vectors[0:1, :], 0.0).astype(BF16)
    block = jnp.dot(cblk[...], wqkv[:, width:], preferred_element_type=F32)
    ctx_place = pl.ds(aligned(sp, context_rows), context_rows)
    ctx_kv[ctx_place, :] = (
        block[:context_rows] * inv_ctx + block[context_rows : context_rows + 1]
    ).astype(BF16)

    def ctx_copy(d):
        return to_peer(
            ctx_kv.at[ctx_place], ctx_kv.at[ctx_place], ctx_send, ctx_recv,
            sp=(sp + d) % sp_size, tp=tp,
        )

    @pl.loop(1, sp_size)
    def _(d):
        ctx_copy(d).start()

    down = to_peer(
        kv.at[pl.ds(halo, below)], kv.at[pl.ds(halo + tokens, below)],
        halo_send.at[0], halo_recv.at[0], sp=jnp.maximum(sp - 1, 0),
    )
    up = to_peer(
        kv.at[pl.ds(tokens, halo)], kv.at[pl.ds(0, halo)],
        halo_send.at[1], halo_recv.at[1], sp=jnp.minimum(sp + 1, sp_size - 1),
    )

    wait_all(arrived, term_send, term_recv)

    sum_terms(arrived, slice(2, 4))
    factor = (small[2:3, :] * (1.0 + vectors[3:4, :])).astype(BF16)
    xs[group_tokens : group_tokens + 16, :] = jnp.where(row16 == 0, vectors[2:3, :], 0.0).astype(BF16)

    upper = tp * 2 >= tp_size

    def unit(k):
        if k == 0:
            return jnp.where(upper, groups - 1, 0)
        if k == groups - 1:
            return jnp.where(upper, groups - 2, 1)
        return jnp.where(upper, k - 1, k + 1)

    def project(i, first, span=1):
        step = span * group_tokens
        rows = pl.ds(aligned(i, group_tokens), step)
        place = pl.ds(aligned(i, group_tokens) + halo, step)
        xs[:step, :] = lat[rows, :] * factor
        scale = jnp.concatenate([inv[rows, :]] * (width // LANES), axis=1)

        def part(n):
            columns = slice(n * width, (n + 1) * width)
            y = jnp.dot(
                xs[: step + 16 if first else step, :], wqkv[:, columns],
                preferred_element_type=F32,
            )
            if first:
                added[0:1, columns] = y[step : step + 1]
            return y[:step] * scale + added[0:1, columns]

        q = part(0) * (HEAD_DIM**-0.5 * LOG2E)
        turned = []
        for r in range(span * GROUP):
            turned.append(q[r * GRID_W + SHIFT : (r + 1) * GRID_W])
            turned.append(q[r * GRID_W : r * GRID_W + SHIFT])
        q_s[rows, :] = jnp.concatenate(turned, axis=0).astype(BF16)
        kv[place, :width] = part(1).astype(BF16)
        kv[place, width:] = part(2).astype(BF16)

    project(unit(0), True)

    steps = (groups - 2) // 2

    @pl.loop(0, steps)
    def _(k):
        project(jnp.where(upper, 2 * k, 2 * k + 2), False, 2)

        @pl.when((k == steps - 1) & (sp > 0))
        def _():
            down.start()

        @pl.when((k == steps - 1) & (sp < sp_size - 1))
        def _():
            up.start()

    @pl.loop(1, ranks)
    def _(d):
        gate_copy(d).start()

    contract = (((1,), (1,)), ((), ()))
    size = GROUP * BLOCK
    stack_head = lax.broadcasted_iota(jnp.int32, (size, width), 1) // HEAD_DIM
    first_head = lax.broadcasted_iota(jnp.int32, (size, LANES), 1) < HEAD_DIM
    blocks = GRID_W // BLOCK
    near_keys = KEY_ROWS * STRIP

    def strips(g, b):
        base = aligned(g, group_tokens)
        found = []
        for j in range(KEY_ROWS):
            if b == blocks - 1:
                found.append(pl.ds(base + (j * GRID_W + b * BLOCK), BLOCK))
                found.append(pl.ds(base + j * GRID_W, BLOCK))
            else:
                found.append(pl.ds(base + (j * GRID_W + b * BLOCK), STRIP))
        return found

    def places(g, b):
        base = aligned(g, group_tokens)
        return [pl.ds(base + (r * GRID_W + b * BLOCK), BLOCK) for r in range(GROUP)]

    def stacked(g, b):
        q = jnp.concatenate([q_s[place, :] for place in places(g, b)], axis=0)
        return jnp.concatenate(
            [jnp.where(stack_head == h, q, jnp.zeros_like(q)) for h in range(heads)], axis=0
        )

    def score_near(g, b):
        global_row = sp * grid_rows + g * GROUP
        top = global_row == 0
        bottom = global_row == sp_size * grid_rows - GROUP
        slots = (
            jnp.where(top, 5, jnp.where(bottom, 3, 0)), 1,
            jnp.where(top, 4, jnp.where(bottom, 5, 2)),
        )
        kind = 1 if b == blocks - 1 else 0
        keys = jnp.concatenate([kv[s, :width] for s in strips(g, b)], axis=0)
        s = lax.dot_general(stacked(g, b), keys, contract, preferred_element_type=F32)
        for t in range(TILES):
            lanes = slice(t * LANES, (t + 1) * LANES)
            scores[b, :, lanes] = s[:, lanes] + table[kind, slots[t]]

    def score_far(g, b):
        scores[b, :, near_keys:] = lax.dot_general(
            stacked(g, b), ctx_kv[:, :width], contract, preferred_element_type=F32
        )

    def soften(b):
        sums = []
        for h in range(heads):
            rows = slice(h * size, (h + 1) * size)
            s = scores[b, rows, :]
            p = jnp.exp2(s - jnp.max(s, axis=1, keepdims=True))
            sums.append(jnp.sum(p, axis=1, keepdims=True))
            probs[b, rows, :] = p.astype(BF16)
        return [1.0 / total for total in sums]

    def merge(column, row=None):
        parts = []
        for c in range(width // LANES):
            low, high = 2 * c, 2 * c + 1
            if row is not None:
                lanes = slice(c * LANES, (c + 1) * LANES)
                first = row[low * size : (low + 1) * size, lanes]
                second = row[high * size : (high + 1) * size, lanes]
                if column is not None:
                    first, second = first * column[low], second * column[high]
            else:
                first, second = column[low], column[high]
            parts.append(jnp.where(first_head, first, second))
        return jnp.concatenate(parts, axis=1)

    def place_merged(g, b, merged):
        merged = merged.astype(BF16)
        for r, place in enumerate(places(g, b)):
            stage[place, :] = merged[r * BLOCK : (r + 1) * BLOCK]

    def mix(g, b, inverses):
        values = jnp.concatenate(
            [kv[s, width:] for s in strips(g, b)] + [ctx_kv[:, width:]], axis=0
        )
        mixed = jnp.dot(probs[b], values, preferred_element_type=F32)
        place_merged(g, b, merge(inverses, mixed))

    def head_rows(h):
        return slice(h * size, (h + 1) * size)

    def attend_near(g, b, slot):
        for h in range(heads):
            s = scores[b, head_rows(h), :near_keys]
            peak = jnp.max(s, axis=1, keepdims=True)
            p = jnp.exp2(s - peak)
            spread = (size, LANES)
            stats[slot, b, 0, head_rows(h), :] = jnp.broadcast_to(peak, spread)
            stats[slot, b, 1, head_rows(h), :] = jnp.broadcast_to(
                jnp.sum(p, axis=1, keepdims=True), spread
            )
            probs[b, head_rows(h), :near_keys] = p.astype(BF16)
        values = jnp.concatenate([kv[s, width:] for s in strips(g, b)], axis=0)
        mixed = jnp.dot(probs[b, :, :near_keys], values, preferred_element_type=F32)
        partial[slot, b] = merge(None, mixed)

    def attend_far(g, b, slot):
        keeps, inverses = [], []
        for h in range(heads):
            old = stats[slot, b, 0, head_rows(h), :]
            s = scores[b, head_rows(h), near_keys:]
            peak = jnp.maximum(old, jnp.max(s, axis=1, keepdims=True))
            p = jnp.exp2(s - jnp.concatenate([peak] * (s.shape[1] // LANES), axis=1))
            keep = jnp.exp2(old - peak)
            total = stats[slot, b, 1, head_rows(h), :] * keep
            total = total + jnp.sum(p, axis=1, keepdims=True)
            inverse = 1.0 / total
            inverses.append(inverse)
            keeps.append(keep * inverse)
            probs[b, head_rows(h), near_keys:] = p.astype(BF16)
        mixed = jnp.dot(
            probs[b, :, near_keys:], ctx_kv[:, width:], preferred_element_type=F32
        )
        place_merged(g, b, partial[slot, b] * merge(keeps) + merge(inverses, mixed))

    def piece_copy(index):
        owner, p = index // pieces, index % pieces
        return to_peer(
            stage.at[pl.ds(aligned(index, piece), piece)],
            recv.at[tp, pl.ds(aligned(p, piece), piece)],
            piece_send, piece_recv.at[tp, p], tp=owner,
        )

    half = groups // 2
    inner = half - 1

    def group_of(own, j):
        early = jnp.where(j == 0, 0, jnp.where(j == 1, inner, j - 1))
        low = (jnp.where(sp == 0, early, j) + 1) % half
        return jnp.where(upper != own, low, half + j)

    def send_pieces(g):
        for n in range(per_group):
            index = g * per_group + n

            @pl.when(index // pieces != tp)
            def _():
                piece_copy(index).start()

    @pl.loop(0, inner)
    def _(k):
        g = group_of(False, k)
        score_near(g, 0)
        for b in range(blocks):
            if b + 1 < blocks:
                score_near(g, b + 1)
            attend_near(g, b, k)

    others = ctx_kv.at[pl.ds(0, (sp_size - 1) * context_rows)]
    to_peer(others, others, ctx_send, ctx_recv, sp=(sp + 1) % sp_size).wait()

    @pl.loop(0, inner)
    def _(k):
        g = group_of(False, k)
        for b in range(blocks):
            score_far(g, b)
        for b in range(blocks):
            attend_far(g, b, k)
        send_pieces(g)

    project(unit(groups - 1), False)

    no_halo = jnp.where(upper, sp == 0, sp == sp_size - 1)
    turn = jnp.where(no_halo, 0, jnp.where(sp == 0, groups - inner - 1, inner))

    @pl.loop(0, groups - inner)
    def _(k):
        own = k != turn
        g = group_of(own, jnp.where(own, k - jnp.where(k > turn, 1, 0), inner))

        @pl.when((g == 0) & (sp > 0))
        def _():
            down.wait_send()
            up.wait_recv()

        @pl.when((g == groups - 1) & (sp < sp_size - 1))
        def _():
            up.wait_send()
            down.wait_recv()

        score_near(g, 0)
        score_far(g, 0)
        for b in range(blocks):
            if b + 1 < blocks:
                score_near(g, b + 1)
                score_far(g, b + 1)
            mix(g, b, soften(b))
        send_pieces(g)

    load_wo.wait()

    wait_all(garrived, gate_send, gate_recv)

    gates = []
    for t in range(tp_size):
        total = garrived[t]
        for s in range(1, sp_size):
            total = total + garrived[s * tp_size + t]
        gates.append(total)
    gate = jnp.concatenate(gates, axis=1)
    chips = tp_size // 2
    chip = tp // 2
    partner = tp + 1 - 2 * (tp % 2)

    def arrival(source, p):
        rows = pl.ds(aligned(p, piece), piece)
        return to_peer(
            stage.at[rows], recv.at[source, rows], piece_send,
            piece_recv.at[source, p], tp=source,
        )

    def product(c, rows):
        pair = jnp.concatenate([recv[2 * c, rows, :], recv[2 * c + 1, rows, :]], axis=1)
        return jnp.dot(
            pair, wo[pl.ds(aligned(c, 2 * width), 2 * width), :], preferred_element_type=F32
        )

    def landing(k):
        return jnp.where(tp == 0, (k + per_group) % pieces, k)

    @pl.loop(0, pieces)
    def _(k):
        p = landing(k)
        rows = pl.ds(aligned(p, piece), piece)
        recv[tp, rows, :] = stage[pl.ds(aligned(tp * pieces + p, piece), piece), :]
        arrival(partner, p).wait_recv()
        acc[rows, :] = product(chip, rows)

    @pl.loop(0, pieces)
    def _(k):
        p = landing(k)
        rows = pl.ds(aligned(p, piece), piece)
        own = pl.ds(aligned(tp * pieces + p, piece), piece)
        branch = acc[rows, :]
        for d in range(1, chips):
            c = (chip + d) % chips
            arrival(2 * c, p).wait_recv()
            arrival(2 * c + 1, p).wait_recv()
            branch = branch + product(c, rows)
        turned = []
        for r in range(piece_rows):
            turned.append(branch[(r + 1) * GRID_W - SHIFT : (r + 1) * GRID_W])
            turned.append(branch[r * GRID_W : (r + 1) * GRID_W - SHIFT])
        branch = jnp.concatenate(turned, axis=0)
        out_ref[rows, :] = (lat[own, :].astype(F32) + gate * branch).astype(BF16)

    sent = stage.at[pl.ds(0, tokens - share)]
    to_peer(sent, sent, piece_send, piece_recv.at[0, 0], tp=partner).wait_send()


def local(
    latent, condition, context_tokens, context_condition, shift_weight, scale_weight,
    gate_weight, norm_gain, query_weight, key_weight, value_weight, out_weight, offset_bias,
):
    sp_size, tp_size = lax.axis_size("sp"), lax.axis_size("tp")
    ranks = sp_size * tp_size
    tokens, depth = latent.shape
    context_rows = context_tokens.shape[0]
    input_rows, piece_cols = shift_weight.shape
    width = query_weight.shape[1]
    heads = width // HEAD_DIM
    groups = tokens // GRID_W // GROUP
    group_tokens = GROUP * GRID_W
    share = tokens // tp_size
    piece_rows = gcd(GROUP, share // GRID_W)
    pieces = share // (piece_rows * GRID_W)
    stacked = heads * GROUP * BLOCK
    keys = KEY_ROWS * STRIP + sp_size * context_rows
    bias = jnp.transpose(offset_bias, (1, 0, 2))
    dma = pltpu.SemaphoreType.DMA
    vmem = pltpu.VMEM
    hbm = pl.BlockSpec(memory_space=pl.ANY)
    return pl.pallas_call(
        kernel,
        in_specs=[hbm] * 13,
        out_specs=pl.BlockSpec(memory_space=pltpu.VMEM),
        out_shape=pltpu.VMEM((share, depth), BF16),
        scratch_shapes=[
            vmem((depth,), BF16), vmem((depth,), BF16), vmem((depth,), BF16),
            vmem((8, depth), F32),
            vmem((3, input_rows, piece_cols), BF16),
            vmem(bias.shape, F32),
            vmem((bias.shape[0], heads, LANES), F32),
            vmem((2, 6, heads * GROUP * BLOCK, LANES), F32),
            vmem((context_rows, depth), BF16),
            vmem((context_rows + 16, depth), BF16),
            vmem((tokens, depth), BF16),
            vmem((2 * group_tokens, depth), BF16),
            vmem((depth, 3 * width), BF16),
            vmem(out_weight.shape, BF16),
            vmem((2, piece_cols), BF16),
            vmem((ranks, 2, piece_cols), BF16),
            vmem((2, piece_cols), BF16),
            vmem((ranks, 2, piece_cols), BF16),
            vmem((1, piece_cols), F32),
            vmem((ranks, 1, piece_cols), F32),
            vmem((4, depth), F32),
            vmem((1, 3 * width), F32),
            vmem((tokens, LANES), F32),
            vmem((tokens, width), BF16),
            vmem((tokens + 2 * HALO * GRID_W, 2 * width), BF16),
            vmem((sp_size * context_rows, 2 * width), BF16),
            vmem((GRID_W // BLOCK, stacked, keys), F32),
            vmem((GRID_W // BLOCK, stacked, keys), BF16),
            vmem((groups // 2 - 1, GRID_W // BLOCK, GROUP * BLOCK, width), F32),
            vmem((groups // 2 - 1, GRID_W // BLOCK, 2, stacked, LANES), F32),
            vmem((tokens, width), BF16),
            vmem((tp_size, share, width), BF16),
            vmem((share, depth), F32),
            dma((12,)), dma((groups,)), dma, dma, dma, dma, dma, dma, dma((2,)), dma((2,)),
            dma, dma, dma, dma((tp_size, pieces)),
        ],
        compiler_params=pltpu.CompilerParams(
            vmem_limit_bytes=60 * 2**20, collective_id=0, has_side_effects=True
        ),
        cost_estimate=pl.CostEstimate(
            flops=6 * tokens * depth * width,
            bytes_accessed=2 * (tokens * depth + 3 * depth * width + share * depth),
            transcendentals=0,
        ),
    )(
        condition, context_condition, norm_gain, shift_weight, scale_weight, gate_weight, bias,
        context_tokens, latent, query_weight, key_weight, value_weight, out_weight,
    )


def solution(mesh):
    placed = (
        P(("grp", "sp"), None),
        P("grp"),
        P(("grp", "sp"), None),
        P(),
        P("sp", "tp"),
        P("sp", "tp"),
        P("sp", "tp"),
        P(),
        P(None, "tp"),
        P(None, "tp"),
        P(None, "tp"),
        P(),
        P("tp", None, None),
    )
    return jax.shard_map(
        local, mesh=mesh, in_specs=placed, out_specs=P(("grp", "sp", "tp"), None), check_vma=False
    )
```

```python
import functools

import jax
import jax.numpy as jnp
from jax import lax
from jax.experimental import pallas as pl
from jax.experimental.pallas import tpu as pltpu
from jax.sharding import PartitionSpec as P

HEAD_DIM = 64
GRID_W = 64
WIN_ROWS = 8
WIN_COLS = 16
HALO = WIN_ROWS // 2
BLOCK = 16
SHIFT = WIN_COLS // 2
STRIP = BLOCK + WIN_COLS
GROUP = 4
KEY_ROWS = GROUP + WIN_ROWS
LANES = 128
SEGMENTS = LANES // STRIP
TILES = KEY_ROWS // SEGMENTS
LOG2E = 1.4426950408889634
epsilon = 1e-06
masked_score = -1e30
F32 = jnp.float32
BF16 = jnp.bfloat16
MESH = pl.DeviceIdType.MESH


def to_peer(src, dst, send, recv, **place):
    return pltpu.make_async_remote_copy(
        src_ref=src, dst_ref=dst, send_sem=send, recv_sem=recv,
        device_id=place, device_id_type=MESH,
    )


def gcd(a, b):
    while b:
        a, b = b, a % b
    return a


def aligned(index, step):
    return pl.multiple_of(index * step, step)


def build_tables(bias_ref, braw, table, heads):
    offsets = bias_ref.shape[0]
    braw[...] = jnp.zeros_like(braw)
    for o in range(offsets):
        braw[o, :, : bias_ref.shape[2]] = bias_ref[o] * LOG2E
    lane_h = lax.broadcasted_iota(jnp.int32, (heads, LANES), 1) // STRIP
    first = HALO - 1
    combined = []
    for o in range(first - (GROUP - 1), first + (TILES - 1) * SEGMENTS + 1):
        row = braw[o]
        for j in range(1, SEGMENTS):
            row = jnp.where(lane_h == j, pltpu.roll(braw[o + j], STRIP * j, 1), row)
        combined.append(row)
    u = lax.broadcasted_iota(jnp.int32, (BLOCK, LANES), 0)
    lane = lax.broadcasted_iota(jnp.int32, (BLOCK, LANES), 1)
    v = lane % STRIP
    inner = (v >= u) & (v < u + WIN_COLS)
    edge = ((u < SHIFT) & (v < WIN_COLS)) | ((u >= SHIFT) & (v >= WIN_COLS))
    for t in range(TILES):
        for i in range(GROUP):
            j = t * SEGMENTS + lane // STRIP
            seen = (j >= i) & (j < i + WIN_ROWS)
            whole = t * SEGMENTS >= i and (t + 1) * SEGMENTS <= i + WIN_ROWS
            source = combined[t * SEGMENTS + GROUP - 1 - i]
            for h in range(heads):
                spread = jnp.broadcast_to(source[h : h + 1, :], (BLOCK, LANES))
                value = pltpu.roll(spread, LANES - (SHIFT - 1), 1, stride=1, stride_axis=0)
                place = slice((h * GROUP + i) * BLOCK, (h * GROUP + i + 1) * BLOCK)
                for kind, mask in enumerate((inner, edge)):
                    full = jnp.where(mask, value, masked_score)
                    table[kind, t, place, :] = (
                        full if whole else jnp.where(seen, full, masked_score)
                    )
                    if t != 1:
                        table[kind, 3 if t == 0 else 4, place, :] = full
    for kind in range(2):
        table[kind, 5] = jnp.full(table.shape[2:], masked_score, F32)


def kernel(
    cond_hbm, ctxcond_hbm, gain_hbm, shift_hbm, scale_hbm, gate_hbm, bias_hbm, ctx_hbm,
    lat_hbm, wq_hbm, wk_hbm, wv_hbm, wo_hbm,
    out_ref,
    cond, ctxcond, gain, small, modw, bias, braw, table, ctx, cblk, lat, xs, wqkv, wo,
    cterms, carrived, terms, arrived, gterms, garrived, vectors, added, inv, q_s, kv, ctx_kv,
    scores, probs, partial, stats, stage, recv, acc,
    load_sem, lat_sem, cterm_send, cterm_recv, term_send, term_recv, gate_send, gate_recv,
    halo_send, halo_recv, ctx_send, ctx_recv, piece_send, piece_recv,
):
    sp, tp = lax.axis_index("sp"), lax.axis_index("tp")
    sp_size, tp_size = lax.axis_size("sp"), lax.axis_size("tp")
    ranks = sp_size * tp_size
    me = sp * tp_size + tp
    tokens, depth = lat.shape
    width = wq_hbm.shape[1]
    heads = width // HEAD_DIM
    input_rows, piece_cols = modw.shape[1:]
    context_rows = ctx.shape[0]
    grid_rows = tokens // GRID_W
    groups = grid_rows // GROUP
    group_tokens = GROUP * GRID_W
    halo = HALO * GRID_W
    below = (HALO - 1) * GRID_W
    share = tokens // tp_size
    piece_rows = gcd(GROUP, share // GRID_W)
    piece = piece_rows * GRID_W
    pieces = share // piece
    per_group = GROUP // piece_rows

    def peer(d):
        other = (me + d) % ranks
        return dict(sp=other // tp_size, tp=other % tp_size)

    barrier = pltpu.get_barrier_semaphore()

    early = [
        pltpu.make_async_copy(cond_hbm, cond, load_sem.at[0]),
        pltpu.make_async_copy(ctxcond_hbm, ctxcond, load_sem.at[1]),
        pltpu.make_async_copy(gain_hbm, gain, load_sem.at[2]),
        pltpu.make_async_copy(shift_hbm, modw.at[0], load_sem.at[3]),
        pltpu.make_async_copy(scale_hbm, modw.at[1], load_sem.at[4]),
        pltpu.make_async_copy(gate_hbm, modw.at[2], load_sem.at[5]),
    ]
    load_bias = pltpu.make_async_copy(bias_hbm, bias, load_sem.at[6])
    load_ctx = pltpu.make_async_copy(ctx_hbm, ctx, load_sem.at[7])
    load_weights = [
        pltpu.make_async_copy(w, wqkv.at[:, pl.ds(i * width, width)], load_sem.at[8 + i])
        for i, w in enumerate((wq_hbm, wk_hbm, wv_hbm))
    ]
    load_wo = pltpu.make_async_copy(wo_hbm, wo, load_sem.at[11])

    def load_lat(i):
        rows = pl.ds(aligned(i, group_tokens), group_tokens)
        return pltpu.make_async_copy(lat_hbm.at[rows], lat.at[rows], lat_sem.at[i])

    @pl.loop(1, ranks)
    def _(d):
        pl.semaphore_signal(barrier, inc=1, device_id=peer(d), device_id_type=MESH)

    for load in early:
        load.start()

    load_bias.start()
    load_ctx.start()

    @pl.loop(0, groups)
    def _(i):
        load_lat(i).start()

    for load in load_weights:
        load.start()
    load_wo.start()

    for load in early:
        load.wait()
    small[0:1, :] = cond[...].astype(F32).reshape(1, depth)
    small[1:2, :] = ctxcond[...].astype(F32).reshape(1, depth)
    small[2:3, :] = gain[...].astype(F32).reshape(1, depth)
    row8 = lax.broadcasted_iota(jnp.int32, (8, input_rows), 0)
    own_inputs = pl.ds(aligned(sp, input_rows), input_rows)
    value = jnp.where(row8 == 0, small[0:1, own_inputs], small[1:2, own_inputs])
    act = (value / (1.0 + jnp.exp(-value))).astype(BF16)
    products = []
    for i in range(2):
        both = jnp.dot(act, modw[i], preferred_element_type=F32)
        products.append(both)
    cterms[...] = jnp.concatenate([both[1:2] for both in products], axis=0).astype(BF16)
    terms[...] = jnp.concatenate([both[0:1] for both in products], axis=0).astype(BF16)
    gterms[...] = jnp.dot(act, modw[2], preferred_element_type=F32)[:1]
    carrived[me] = cterms[...]
    arrived[me] = terms[...]
    garrived[me] = gterms[...]

    def wait_all(slots, send, recv_sem):
        all_but_one = slots.at[pl.ds(0, ranks - 1)]
        to_peer(all_but_one, all_but_one, send, recv_sem, **peer(1)).wait()

    def cterm_copy(d):
        return to_peer(
            cterms, carrived.at[me], cterm_send, cterm_recv, **peer(d)
        )

    def term_copy(d):
        return to_peer(terms, arrived.at[me], term_send, term_recv, **peer(d))

    def gate_copy(d):
        return to_peer(gterms, garrived.at[me], gate_send, gate_recv, **peer(d))

    load_bias.wait()
    build_tables(bias, braw, table, heads)
    pl.semaphore_wait(barrier, ranks - 1)

    @pl.loop(1, ranks)
    def _(d):
        cterm_copy(d).start()

    @pl.loop(1, ranks)
    def _(d):
        term_copy(d).start()

    @pl.when(sp == 0)
    def _():
        kv[0:halo, :] = jnp.zeros((halo, 2 * width), BF16)

    @pl.when(sp == sp_size - 1)
    def _():
        kv[halo + tokens : halo + tokens + below, :] = jnp.zeros((below, 2 * width), BF16)

    kv[halo + tokens + below :, :] = jnp.zeros((halo - below, 2 * width), BF16)

    def inverse_of(ref, rows):
        total = None
        for c in range(depth // LANES):
            x = ref[rows, c * LANES : (c + 1) * LANES].astype(F32)
            total = x * x if total is None else total + x * x
        mean = jnp.sum(total, axis=1, keepdims=True) * (1.0 / depth)
        return lax.rsqrt(mean + epsilon)

    load_ctx.wait()
    inv_ctx = inverse_of(ctx, slice(None))

    @pl.loop(0, groups)
    def _(i):
        load_lat(i).wait()
        for r in range(0, group_tokens, 128):
            rows = pl.ds(aligned(i, group_tokens) + r, 128)
            inv[rows, :] = jnp.broadcast_to(inverse_of(lat, rows), (128, LANES))

    for load in load_weights:
        load.wait()

    def sum_terms(ref, rows):
        for t in range(tp_size):
            total = ref[t].astype(F32)
            for s in range(1, sp_size):
                total = total + ref[s * tp_size + t].astype(F32)
            vectors[rows, t * piece_cols : (t + 1) * piece_cols] = total

    wait_all(carrived, cterm_send, cterm_recv)

    sum_terms(carrived, slice(0, 2))
    row16 = lax.broadcasted_iota(jnp.int32, (16, depth), 0)
    factor_ctx = (small[2:3, :] * (1.0 + vectors[1:2, :])).astype(BF16)
    cblk[:context_rows, :] = ctx[...] * factor_ctx
    cblk[context_rows:, :] = jnp.where(row16 == 0, vectors[0:1, :], 0.0).astype(BF16)
    block = jnp.dot(cblk[...], wqkv[:, width:], preferred_element_type=F32)
    ctx_place = pl.ds(aligned(sp, context_rows), context_rows)
    ctx_kv[ctx_place, :] = (
        block[:context_rows] * inv_ctx + block[context_rows : context_rows + 1]
    ).astype(BF16)

    def ctx_copy(d):
        return to_peer(
            ctx_kv.at[ctx_place], ctx_kv.at[ctx_place], ctx_send, ctx_recv,
            sp=(sp + d) % sp_size, tp=tp,
        )

    @pl.loop(1, sp_size)
    def _(d):
        ctx_copy(d).start()

    down = to_peer(
        kv.at[pl.ds(halo, below)], kv.at[pl.ds(halo + tokens, below)],
        halo_send.at[0], halo_recv.at[0], sp=jnp.maximum(sp - 1, 0),
    )
    up = to_peer(
        kv.at[pl.ds(tokens, halo)], kv.at[pl.ds(0, halo)],
        halo_send.at[1], halo_recv.at[1], sp=jnp.minimum(sp + 1, sp_size - 1),
    )

    wait_all(arrived, term_send, term_recv)

    sum_terms(arrived, slice(2, 4))
    factor = (small[2:3, :] * (1.0 + vectors[3:4, :])).astype(BF16)
    xs[group_tokens : group_tokens + 16, :] = jnp.where(row16 == 0, vectors[2:3, :], 0.0).astype(BF16)

    upper = tp * 2 >= tp_size

    def unit(k):
        if k == 0:
            return jnp.where(upper, groups - 1, 0)
        if k == groups - 1:
            return jnp.where(upper, groups - 2, 1)
        return jnp.where(upper, k - 1, k + 1)

    def project(i, first, span=1):
        step = span * group_tokens
        rows = pl.ds(aligned(i, group_tokens), step)
        place = pl.ds(aligned(i, group_tokens) + halo, step)
        xs[:step, :] = lat[rows, :] * factor
        scale = jnp.concatenate([inv[rows, :]] * (width // LANES), axis=1)

        def part(n):
            columns = slice(n * width, (n + 1) * width)
            y = jnp.dot(
                xs[: step + 16 if first else step, :], wqkv[:, columns],
                preferred_element_type=F32,
            )
            if first:
                added[0:1, columns] = y[step : step + 1]
            return y[:step] * scale + added[0:1, columns]

        q = part(0) * (HEAD_DIM**-0.5 * LOG2E)
        turned = []
        for r in range(span * GROUP):
            turned.append(q[r * GRID_W + SHIFT : (r + 1) * GRID_W])
            turned.append(q[r * GRID_W : r * GRID_W + SHIFT])
        q_s[rows, :] = jnp.concatenate(turned, axis=0).astype(BF16)
        kv[place, :width] = part(1).astype(BF16)
        kv[place, width:] = part(2).astype(BF16)

    project(unit(0), True)

    steps = (groups - 2) // 2

    @pl.loop(0, steps)
    def _(k):
        project(jnp.where(upper, 2 * k, 2 * k + 2), False, 2)

        @pl.when((k == steps - 1) & (sp > 0))
        def _():
            down.start()

        @pl.when((k == steps - 1) & (sp < sp_size - 1))
        def _():
            up.start()

    @pl.loop(1, ranks)
    def _(d):
        gate_copy(d).start()

    contract = (((1,), (1,)), ((), ()))
    size = GROUP * BLOCK
    stack_head = lax.broadcasted_iota(jnp.int32, (size, width), 1) // HEAD_DIM
    first_head = lax.broadcasted_iota(jnp.int32, (size, LANES), 1) < HEAD_DIM
    blocks = GRID_W // BLOCK
    near_keys = KEY_ROWS * STRIP

    def strips(g, b):
        base = aligned(g, group_tokens)
        found = []
        for j in range(KEY_ROWS):
            if b == blocks - 1:
                found.append(pl.ds(base + (j * GRID_W + b * BLOCK), BLOCK))
                found.append(pl.ds(base + j * GRID_W, BLOCK))
            else:
                found.append(pl.ds(base + (j * GRID_W + b * BLOCK), STRIP))
        return found

    def places(g, b):
        base = aligned(g, group_tokens)
        return [pl.ds(base + (r * GRID_W + b * BLOCK), BLOCK) for r in range(GROUP)]

    def stacked(g, b):
        q = jnp.concatenate([q_s[place, :] for place in places(g, b)], axis=0)
        return jnp.concatenate(
            [jnp.where(stack_head == h, q, jnp.zeros_like(q)) for h in range(heads)], axis=0
        )

    def score_near(g, b):
        global_row = sp * grid_rows + g * GROUP
        top = global_row == 0
        bottom = global_row == sp_size * grid_rows - GROUP
        slots = (
            jnp.where(top, 5, jnp.where(bottom, 3, 0)), 1,
            jnp.where(top, 4, jnp.where(bottom, 5, 2)),
        )
        kind = 1 if b == blocks - 1 else 0
        keys = jnp.concatenate([kv[s, :width] for s in strips(g, b)], axis=0)
        s = lax.dot_general(stacked(g, b), keys, contract, preferred_element_type=F32)
        for t in range(TILES):
            lanes = slice(t * LANES, (t + 1) * LANES)
            scores[b, :, lanes] = s[:, lanes] + table[kind, slots[t]]

    def score_far(g, b):
        scores[b, :, near_keys:] = lax.dot_general(
            stacked(g, b), ctx_kv[:, :width], contract, preferred_element_type=F32
        )

    def soften(b):
        sums = []
        for h in range(heads):
            rows = slice(h * size, (h + 1) * size)
            s = scores[b, rows, :]
            p = jnp.exp2(s - jnp.max(s, axis=1, keepdims=True))
            sums.append(jnp.sum(p, axis=1, keepdims=True))
            probs[b, rows, :] = p.astype(BF16)
        return [1.0 / total for total in sums]

    def merge(column, row=None):
        parts = []
        for c in range(width // LANES):
            low, high = 2 * c, 2 * c + 1
            if row is not None:
                lanes = slice(c * LANES, (c + 1) * LANES)
                first = row[low * size : (low + 1) * size, lanes]
                second = row[high * size : (high + 1) * size, lanes]
                if column is not None:
                    first, second = first * column[low], second * column[high]
            else:
                first, second = column[low], column[high]
            parts.append(jnp.where(first_head, first, second))
        return jnp.concatenate(parts, axis=1)

    def place_merged(g, b, merged):
        merged = merged.astype(BF16)
        for r, place in enumerate(places(g, b)):
            stage[place, :] = merged[r * BLOCK : (r + 1) * BLOCK]

    def mix(g, b, inverses):
        values = jnp.concatenate(
            [kv[s, width:] for s in strips(g, b)] + [ctx_kv[:, width:]], axis=0
        )
        mixed = jnp.dot(probs[b], values, preferred_element_type=F32)
        place_merged(g, b, merge(inverses, mixed))

    def head_rows(h):
        return slice(h * size, (h + 1) * size)

    def attend_near(g, b, slot):
        for h in range(heads):
            s = scores[b, head_rows(h), :near_keys]
            peak = jnp.max(s, axis=1, keepdims=True)
            p = jnp.exp2(s - peak)
            spread = (size, LANES)
            stats[slot, b, 0, head_rows(h), :] = jnp.broadcast_to(peak, spread)
            stats[slot, b, 1, head_rows(h), :] = jnp.broadcast_to(
                jnp.sum(p, axis=1, keepdims=True), spread
            )
            probs[b, head_rows(h), :near_keys] = p.astype(BF16)
        values = jnp.concatenate([kv[s, width:] for s in strips(g, b)], axis=0)
        mixed = jnp.dot(probs[b, :, :near_keys], values, preferred_element_type=F32)
        partial[slot, b] = merge(None, mixed)

    def attend_far(g, b, slot):
        keeps, inverses = [], []
        for h in range(heads):
            old = stats[slot, b, 0, head_rows(h), :]
            s = scores[b, head_rows(h), near_keys:]
            peak = jnp.maximum(old, jnp.max(s, axis=1, keepdims=True))
            p = jnp.exp2(s - jnp.concatenate([peak] * (s.shape[1] // LANES), axis=1))
            keep = jnp.exp2(old - peak)
            total = stats[slot, b, 1, head_rows(h), :] * keep
            total = total + jnp.sum(p, axis=1, keepdims=True)
            inverse = 1.0 / total
            inverses.append(inverse)
            keeps.append(keep * inverse)
            probs[b, head_rows(h), near_keys:] = p.astype(BF16)
        mixed = jnp.dot(
            probs[b, :, near_keys:], ctx_kv[:, width:], preferred_element_type=F32
        )
        place_merged(g, b, partial[slot, b] * merge(keeps) + merge(inverses, mixed))

    def piece_copy(index):
        owner, p = index // pieces, index % pieces
        return to_peer(
            stage.at[pl.ds(aligned(index, piece), piece)],
            recv.at[tp, pl.ds(aligned(p, piece), piece)],
            piece_send, piece_recv.at[tp, p], tp=owner,
        )

    half = groups // 2
    inner = half - 1

    def group_of(own, j):
        early = jnp.where(j == 0, 0, jnp.where(j == 1, inner, j - 1))
        low = (jnp.where(sp == 0, early, j) + 1) % half
        return jnp.where(upper != own, low, half + j)

    def send_pieces(g):
        for n in range(per_group):
            index = g * per_group + n

            @pl.when(index // pieces != tp)
            def _():
                piece_copy(index).start()

    @pl.loop(0, inner)
    def _(k):
        g = group_of(False, k)
        for b in range(blocks):
            score_near(g, b)
        for b in range(blocks):
            attend_near(g, b, k)

    others = ctx_kv.at[pl.ds(0, (sp_size - 1) * context_rows)]
    to_peer(others, others, ctx_send, ctx_recv, sp=(sp + 1) % sp_size).wait()

    @pl.loop(0, inner)
    def _(k):
        g = group_of(False, k)
        for b in range(blocks):
            score_far(g, b)
        for b in range(blocks):
            attend_far(g, b, k)
        send_pieces(g)

    project(unit(groups - 1), False)

    no_halo = jnp.where(upper, sp == 0, sp == sp_size - 1)
    turn = jnp.where(no_halo, 0, jnp.where(sp == 0, groups - inner - 1, inner))

    @pl.loop(0, groups - inner)
    def _(k):
        own = k != turn
        g = group_of(own, jnp.where(own, k - jnp.where(k > turn, 1, 0), inner))

        @pl.when((g == 0) & (sp > 0))
        def _():
            down.wait_send()
            up.wait_recv()

        @pl.when((g == groups - 1) & (sp < sp_size - 1))
        def _():
            up.wait_send()
            down.wait_recv()

        for b in range(blocks):
            score_near(g, b)
            score_far(g, b)
        for b in range(blocks):
            mix(g, b, soften(b))
        send_pieces(g)

    load_wo.wait()

    wait_all(garrived, gate_send, gate_recv)

    gates = []
    for t in range(tp_size):
        total = garrived[t]
        for s in range(1, sp_size):
            total = total + garrived[s * tp_size + t]
        gates.append(total)
    gate = jnp.concatenate(gates, axis=1)
    chips = tp_size // 2
    chip = tp // 2
    partner = tp + 1 - 2 * (tp % 2)

    def arrival(source, p):
        rows = pl.ds(aligned(p, piece), piece)
        return to_peer(
            stage.at[rows], recv.at[source, rows], piece_send,
            piece_recv.at[source, p], tp=source,
        )

    def product(c, rows):
        pair = jnp.concatenate([recv[2 * c, rows, :], recv[2 * c + 1, rows, :]], axis=1)
        return jnp.dot(
            pair, wo[pl.ds(aligned(c, 2 * width), 2 * width), :], preferred_element_type=F32
        )

    def landing(k):
        return jnp.where(tp == 0, (k + per_group) % pieces, k)

    @pl.loop(0, pieces)
    def _(k):
        p = landing(k)
        rows = pl.ds(aligned(p, piece), piece)
        recv[tp, rows, :] = stage[pl.ds(aligned(tp * pieces + p, piece), piece), :]
        arrival(partner, p).wait_recv()
        acc[rows, :] = product(chip, rows)

    @pl.loop(0, pieces)
    def _(k):
        p = landing(k)
        rows = pl.ds(aligned(p, piece), piece)
        own = pl.ds(aligned(tp * pieces + p, piece), piece)
        branch = acc[rows, :]
        for d in range(1, chips):
            c = (chip + d) % chips
            arrival(2 * c, p).wait_recv()
            arrival(2 * c + 1, p).wait_recv()
            branch = branch + product(c, rows)
        turned = []
        for r in range(piece_rows):
            turned.append(branch[(r + 1) * GRID_W - SHIFT : (r + 1) * GRID_W])
            turned.append(branch[r * GRID_W : (r + 1) * GRID_W - SHIFT])
        branch = jnp.concatenate(turned, axis=0)
        out_ref[rows, :] = (lat[own, :].astype(F32) + gate * branch).astype(BF16)

    sent = stage.at[pl.ds(0, tokens - share)]
    to_peer(sent, sent, piece_send, piece_recv.at[0, 0], tp=partner).wait_send()


def local(
    latent, condition, context_tokens, context_condition, shift_weight, scale_weight,
    gate_weight, norm_gain, query_weight, key_weight, value_weight, out_weight, offset_bias,
):
    sp_size, tp_size = lax.axis_size("sp"), lax.axis_size("tp")
    ranks = sp_size * tp_size
    tokens, depth = latent.shape
    context_rows = context_tokens.shape[0]
    input_rows, piece_cols = shift_weight.shape
    width = query_weight.shape[1]
    heads = width // HEAD_DIM
    groups = tokens // GRID_W // GROUP
    group_tokens = GROUP * GRID_W
    share = tokens // tp_size
    piece_rows = gcd(GROUP, share // GRID_W)
    pieces = share // (piece_rows * GRID_W)
    stacked = heads * GROUP * BLOCK
    keys = KEY_ROWS * STRIP + sp_size * context_rows
    bias = jnp.transpose(offset_bias, (1, 0, 2))
    dma = pltpu.SemaphoreType.DMA
    vmem = pltpu.VMEM
    hbm = pl.BlockSpec(memory_space=pl.ANY)
    return pl.pallas_call(
        kernel,
        in_specs=[hbm] * 13,
        out_specs=pl.BlockSpec(memory_space=pltpu.VMEM),
        out_shape=pltpu.VMEM((share, depth), BF16),
        scratch_shapes=[
            vmem((depth,), BF16), vmem((depth,), BF16), vmem((depth,), BF16),
            vmem((8, depth), F32),
            vmem((3, input_rows, piece_cols), BF16),
            vmem(bias.shape, F32),
            vmem((bias.shape[0], heads, LANES), F32),
            vmem((2, 6, heads * GROUP * BLOCK, LANES), F32),
            vmem((context_rows, depth), BF16),
            vmem((context_rows + 16, depth), BF16),
            vmem((tokens, depth), BF16),
            vmem((2 * group_tokens, depth), BF16),
            vmem((depth, 3 * width), BF16),
            vmem(out_weight.shape, BF16),
            vmem((2, piece_cols), BF16),
            vmem((ranks, 2, piece_cols), BF16),
            vmem((2, piece_cols), BF16),
            vmem((ranks, 2, piece_cols), BF16),
            vmem((1, piece_cols), F32),
            vmem((ranks, 1, piece_cols), F32),
            vmem((4, depth), F32),
            vmem((1, 3 * width), F32),
            vmem((tokens, LANES), F32),
            vmem((tokens, width), BF16),
            vmem((tokens + 2 * HALO * GRID_W, 2 * width), BF16),
            vmem((sp_size * context_rows, 2 * width), BF16),
            vmem((GRID_W // BLOCK, stacked, keys), F32),
            vmem((GRID_W // BLOCK, stacked, keys), BF16),
            vmem((groups // 2 - 1, GRID_W // BLOCK, GROUP * BLOCK, width), F32),
            vmem((groups // 2 - 1, GRID_W // BLOCK, 2, stacked, LANES), F32),
            vmem((tokens, width), BF16),
            vmem((tp_size, share, width), BF16),
            vmem((share, depth), F32),
            dma((12,)), dma((groups,)), dma, dma, dma, dma, dma, dma, dma((2,)), dma((2,)),
            dma, dma, dma, dma((tp_size, pieces)),
        ],
        compiler_params=pltpu.CompilerParams(
            vmem_limit_bytes=60 * 2**20, collective_id=0, has_side_effects=True
        ),
        cost_estimate=pl.CostEstimate(
            flops=6 * tokens * depth * width,
            bytes_accessed=2 * (tokens * depth + 3 * depth * width + share * depth),
            transcendentals=0,
        ),
    )(
        condition, context_condition, norm_gain, shift_weight, scale_weight, gate_weight, bias,
        context_tokens, latent, query_weight, key_weight, value_weight, out_weight,
    )


def solution(mesh):
    placed = (
        P(("grp", "sp"), None),
        P("grp"),
        P(("grp", "sp"), None),
        P(),
        P("sp", "tp"),
        P("sp", "tp"),
        P("sp", "tp"),
        P(),
        P(None, "tp"),
        P(None, "tp"),
        P(None, "tp"),
        P(),
        P("tp", None, None),
    )
    return jax.shard_map(
        local, mesh=mesh, in_specs=placed, out_specs=P(("grp", "sp", "tp"), None), check_vma=False
    )
```

```python
import functools

import jax
import jax.numpy as jnp
from jax import lax
from jax.experimental import pallas as pl
from jax.experimental.pallas import tpu as pltpu
from jax.sharding import PartitionSpec as P

HEAD_DIM = 64
GRID_W = 64
WIN_ROWS = 8
WIN_COLS = 16
HALO = WIN_ROWS // 2
BLOCK = 16
SHIFT = WIN_COLS // 2
STRIP = BLOCK + WIN_COLS
GROUP = 4
KEY_ROWS = GROUP + WIN_ROWS
LANES = 128
SEGMENTS = LANES // STRIP
TILES = KEY_ROWS // SEGMENTS
LOG2E = 1.4426950408889634
epsilon = 1e-06
masked_score = -1e30
F32 = jnp.float32
BF16 = jnp.bfloat16
MESH = pl.DeviceIdType.MESH


def to_peer(src, dst, send, recv, **place):
    return pltpu.make_async_remote_copy(
        src_ref=src, dst_ref=dst, send_sem=send, recv_sem=recv,
        device_id=place, device_id_type=MESH,
    )


def gcd(a, b):
    while b:
        a, b = b, a % b
    return a


def aligned(index, step):
    return pl.multiple_of(index * step, step)


def build_tables(bias_ref, braw, table, heads):
    offsets = bias_ref.shape[0]
    braw[...] = jnp.zeros_like(braw)
    for o in range(offsets):
        braw[o, :, : bias_ref.shape[2]] = bias_ref[o] * LOG2E
    lane_h = lax.broadcasted_iota(jnp.int32, (heads, LANES), 1) // STRIP
    first = HALO - 1
    combined = []
    for o in range(first - (GROUP - 1), first + (TILES - 1) * SEGMENTS + 1):
        row = braw[o]
        for j in range(1, SEGMENTS):
            row = jnp.where(lane_h == j, pltpu.roll(braw[o + j], STRIP * j, 1), row)
        combined.append(row)
    u = lax.broadcasted_iota(jnp.int32, (BLOCK, LANES), 0)
    lane = lax.broadcasted_iota(jnp.int32, (BLOCK, LANES), 1)
    v = lane % STRIP
    inner = (v >= u) & (v < u + WIN_COLS)
    edge = ((u < SHIFT) & (v < WIN_COLS)) | ((u >= SHIFT) & (v >= WIN_COLS))
    for t in range(TILES):
        for i in range(GROUP):
            j = t * SEGMENTS + lane // STRIP
            seen = (j >= i) & (j < i + WIN_ROWS)
            whole = t * SEGMENTS >= i and (t + 1) * SEGMENTS <= i + WIN_ROWS
            source = combined[t * SEGMENTS + GROUP - 1 - i]
            for h in range(heads):
                spread = jnp.broadcast_to(source[h : h + 1, :], (BLOCK, LANES))
                value = pltpu.roll(spread, LANES - (SHIFT - 1), 1, stride=1, stride_axis=0)
                place = slice((h * GROUP + i) * BLOCK, (h * GROUP + i + 1) * BLOCK)
                for kind, mask in enumerate((inner, edge)):
                    full = jnp.where(mask, value, masked_score)
                    table[kind, t, place, :] = (
                        full if whole else jnp.where(seen, full, masked_score)
                    )
                    if t != 1:
                        table[kind, 3 if t == 0 else 4, place, :] = full
    for kind in range(2):
        table[kind, 5] = jnp.full(table.shape[2:], masked_score, F32)


def kernel(
    cond_hbm, ctxcond_hbm, gain_hbm, shift_hbm, scale_hbm, gate_hbm, bias_hbm, ctx_hbm,
    lat_hbm, wq_hbm, wk_hbm, wv_hbm, wo_hbm,
    out_ref,
    cond, ctxcond, gain, small, modw, bias, braw, table, ctx, cblk, lat, xs, wqkv, wo,
    cterms, carrived, terms, arrived, gterms, garrived, vectors, added, inv, q_s, kv, ctx_kv,
    scores, probs, partial, stats, stage, recv, acc,
    load_sem, lat_sem, cterm_send, cterm_recv, term_send, term_recv, gate_send, gate_recv,
    halo_send, halo_recv, ctx_send, ctx_recv, piece_send, piece_recv,
):
    sp, tp = lax.axis_index("sp"), lax.axis_index("tp")
    sp_size, tp_size = lax.axis_size("sp"), lax.axis_size("tp")
    ranks = sp_size * tp_size
    me = sp * tp_size + tp
    tokens, depth = lat.shape
    width = wq_hbm.shape[1]
    heads = width // HEAD_DIM
    input_rows, piece_cols = modw.shape[1:]
    context_rows = ctx.shape[0]
    grid_rows = tokens // GRID_W
    groups = grid_rows // GROUP
    group_tokens = GROUP * GRID_W
    halo = HALO * GRID_W
    below = (HALO - 1) * GRID_W
    share = tokens // tp_size
    piece_rows = gcd(GROUP, share // GRID_W)
    piece = piece_rows * GRID_W
    pieces = share // piece
    per_group = GROUP // piece_rows

    def peer(d):
        other = (me + d) % ranks
        return dict(sp=other // tp_size, tp=other % tp_size)

    barrier = pltpu.get_barrier_semaphore()

    early = [
        pltpu.make_async_copy(cond_hbm, cond, load_sem.at[0]),
        pltpu.make_async_copy(ctxcond_hbm, ctxcond, load_sem.at[1]),
        pltpu.make_async_copy(gain_hbm, gain, load_sem.at[2]),
        pltpu.make_async_copy(shift_hbm, modw.at[0], load_sem.at[3]),
        pltpu.make_async_copy(scale_hbm, modw.at[1], load_sem.at[3]),
        pltpu.make_async_copy(gate_hbm, modw.at[2], load_sem.at[3]),
    ]
    load_bias = pltpu.make_async_copy(bias_hbm, bias, load_sem.at[4])
    load_ctx = pltpu.make_async_copy(ctx_hbm, ctx, load_sem.at[5])
    load_weights = [
        pltpu.make_async_copy(w, wqkv.at[:, pl.ds(i * width, width)], load_sem.at[6])
        for i, w in enumerate((wq_hbm, wk_hbm, wv_hbm))
    ]
    load_wo = pltpu.make_async_copy(wo_hbm, wo, load_sem.at[7])

    def load_lat(i):
        rows = pl.ds(aligned(i, group_tokens), group_tokens)
        return pltpu.make_async_copy(lat_hbm.at[rows], lat.at[rows], lat_sem.at[i])

    @pl.loop(1, ranks)
    def _(d):
        pl.semaphore_signal(barrier, inc=1, device_id=peer(d), device_id_type=MESH)

    for load in early:
        load.start()

    load_bias.start()
    load_ctx.start()

    @pl.loop(0, groups)
    def _(i):
        load_lat(i).start()

    for load in load_weights:
        load.start()
    load_wo.start()

    for load in early[:3]:
        load.wait()
    pltpu.make_async_copy(modw, modw, load_sem.at[3]).wait()
    small[0:1, :] = cond[...].astype(F32).reshape(1, depth)
    small[1:2, :] = ctxcond[...].astype(F32).reshape(1, depth)
    small[2:3, :] = gain[...].astype(F32).reshape(1, depth)
    row8 = lax.broadcasted_iota(jnp.int32, (8, input_rows), 0)
    own_inputs = pl.ds(aligned(sp, input_rows), input_rows)
    value = jnp.where(row8 == 0, small[0:1, own_inputs], small[1:2, own_inputs])
    act = (value / (1.0 + jnp.exp(-value))).astype(BF16)
    products = []
    for i in range(2):
        both = jnp.dot(act, modw[i], preferred_element_type=F32)
        products.append(both)
    cterms[...] = jnp.concatenate([both[1:2] for both in products], axis=0).astype(BF16)
    terms[...] = jnp.concatenate([both[0:1] for both in products], axis=0).astype(BF16)
    gterms[...] = jnp.dot(act, modw[2], preferred_element_type=F32)[:1]
    carrived[me] = cterms[...]
    arrived[me] = terms[...]
    garrived[me] = gterms[...]

    def wait_all(slots, send, recv_sem):
        all_but_one = slots.at[pl.ds(0, ranks - 1)]
        to_peer(all_but_one, all_but_one, send, recv_sem, **peer(1)).wait()

    def cterm_copy(d):
        return to_peer(
            cterms, carrived.at[me], cterm_send, cterm_recv, **peer(d)
        )

    def term_copy(d):
        return to_peer(terms, arrived.at[me], term_send, term_recv, **peer(d))

    def gate_copy(d):
        return to_peer(gterms, garrived.at[me], gate_send, gate_recv, **peer(d))

    load_bias.wait()
    build_tables(bias, braw, table, heads)
    pl.semaphore_wait(barrier, ranks - 1)

    @pl.loop(1, ranks)
    def _(d):
        cterm_copy(d).start()

    @pl.loop(1, ranks)
    def _(d):
        term_copy(d).start()

    @pl.when(sp == 0)
    def _():
        kv[0:halo, :] = jnp.zeros((halo, 2 * width), BF16)

    @pl.when(sp == sp_size - 1)
    def _():
        kv[halo + tokens : halo + tokens + below, :] = jnp.zeros((below, 2 * width), BF16)

    kv[halo + tokens + below :, :] = jnp.zeros((halo - below, 2 * width), BF16)

    def inverse_of(ref, rows):
        total = None
        for c in range(depth // LANES):
            x = ref[rows, c * LANES : (c + 1) * LANES].astype(F32)
            total = x * x if total is None else total + x * x
        mean = jnp.sum(total, axis=1, keepdims=True) * (1.0 / depth)
        return lax.rsqrt(mean + epsilon)

    load_ctx.wait()
    inv_ctx = inverse_of(ctx, slice(None))

    @pl.loop(0, groups)
    def _(i):
        load_lat(i).wait()
        for r in range(0, group_tokens, 128):
            rows = pl.ds(aligned(i, group_tokens) + r, 128)
            inv[rows, :] = jnp.broadcast_to(inverse_of(lat, rows), (128, LANES))

    pltpu.make_async_copy(wqkv, wqkv, load_sem.at[6]).wait()

    def sum_terms(ref, rows):
        for t in range(tp_size):
            total = ref[t].astype(F32)
            for s in range(1, sp_size):
                total = total + ref[s * tp_size + t].astype(F32)
            vectors[rows, t * piece_cols : (t + 1) * piece_cols] = total

    wait_all(carrived, cterm_send, cterm_recv)

    sum_terms(carrived, slice(0, 2))
    row16 = lax.broadcasted_iota(jnp.int32, (16, depth), 0)
    factor_ctx = (small[2:3, :] * (1.0 + vectors[1:2, :])).astype(BF16)
    cblk[:context_rows, :] = ctx[...] * factor_ctx
    cblk[context_rows:, :] = jnp.where(row16 == 0, vectors[0:1, :], 0.0).astype(BF16)
    block = jnp.dot(cblk[...], wqkv[:, width:], preferred_element_type=F32)
    ctx_place = pl.ds(aligned(sp, context_rows), context_rows)
    ctx_kv[ctx_place, :] = (
        block[:context_rows] * inv_ctx + block[context_rows : context_rows + 1]
    ).astype(BF16)

    def ctx_copy(d):
        return to_peer(
            ctx_kv.at[ctx_place], ctx_kv.at[ctx_place], ctx_send, ctx_recv,
            sp=(sp + d) % sp_size, tp=tp,
        )

    @pl.loop(1, sp_size)
    def _(d):
        ctx_copy(d).start()

    down = to_peer(
        kv.at[pl.ds(halo, below)], kv.at[pl.ds(halo + tokens, below)],
        halo_send.at[0], halo_recv.at[0], sp=jnp.maximum(sp - 1, 0),
    )
    up = to_peer(
        kv.at[pl.ds(tokens, halo)], kv.at[pl.ds(0, halo)],
        halo_send.at[1], halo_recv.at[1], sp=jnp.minimum(sp + 1, sp_size - 1),
    )

    wait_all(arrived, term_send, term_recv)

    sum_terms(arrived, slice(2, 4))
    factor = (small[2:3, :] * (1.0 + vectors[3:4, :])).astype(BF16)
    xs[group_tokens : group_tokens + 16, :] = jnp.where(row16 == 0, vectors[2:3, :], 0.0).astype(BF16)

    upper = tp * 2 >= tp_size

    def unit(k):
        if k == 0:
            return jnp.where(upper, groups - 1, 0)
        if k == groups - 1:
            return jnp.where(upper, groups - 2, 1)
        return jnp.where(upper, k - 1, k + 1)

    def project(i, first, span=1):
        step = span * group_tokens
        rows = pl.ds(aligned(i, group_tokens), step)
        place = pl.ds(aligned(i, group_tokens) + halo, step)
        xs[:step, :] = lat[rows, :] * factor
        scale = jnp.concatenate([inv[rows, :]] * (width // LANES), axis=1)

        def part(n):
            columns = slice(n * width, (n + 1) * width)
            y = jnp.dot(
                xs[: step + 16 if first else step, :], wqkv[:, columns],
                preferred_element_type=F32,
            )
            if first:
                added[0:1, columns] = y[step : step + 1]
            return y[:step] * scale + added[0:1, columns]

        q = part(0) * (HEAD_DIM**-0.5 * LOG2E)
        turned = []
        for r in range(span * GROUP):
            turned.append(q[r * GRID_W + SHIFT : (r + 1) * GRID_W])
            turned.append(q[r * GRID_W : r * GRID_W + SHIFT])
        q_s[rows, :] = jnp.concatenate(turned, axis=0).astype(BF16)
        kv[place, :width] = part(1).astype(BF16)
        kv[place, width:] = part(2).astype(BF16)

    project(unit(0), True)

    steps = (groups - 2) // 2

    @pl.loop(0, steps)
    def _(k):
        project(jnp.where(upper, 2 * k, 2 * k + 2), False, 2)

        @pl.when((k == steps - 1) & (sp > 0))
        def _():
            down.start()

        @pl.when((k == steps - 1) & (sp < sp_size - 1))
        def _():
            up.start()

    @pl.loop(1, ranks)
    def _(d):
        gate_copy(d).start()

    contract = (((1,), (1,)), ((), ()))
    size = GROUP * BLOCK
    stack_head = lax.broadcasted_iota(jnp.int32, (size, width), 1) // HEAD_DIM
    first_head = lax.broadcasted_iota(jnp.int32, (size, LANES), 1) < HEAD_DIM
    blocks = GRID_W // BLOCK
    near_keys = KEY_ROWS * STRIP

    def strips(g, b):
        base = aligned(g, group_tokens)
        found = []
        for j in range(KEY_ROWS):
            if b == blocks - 1:
                found.append(pl.ds(base + (j * GRID_W + b * BLOCK), BLOCK))
                found.append(pl.ds(base + j * GRID_W, BLOCK))
            else:
                found.append(pl.ds(base + (j * GRID_W + b * BLOCK), STRIP))
        return found

    def places(g, b):
        base = aligned(g, group_tokens)
        return [pl.ds(base + (r * GRID_W + b * BLOCK), BLOCK) for r in range(GROUP)]

    def stacked(g, b):
        q = jnp.concatenate([q_s[place, :] for place in places(g, b)], axis=0)
        return jnp.concatenate(
            [jnp.where(stack_head == h, q, jnp.zeros_like(q)) for h in range(heads)], axis=0
        )

    def score_near(g, b):
        global_row = sp * grid_rows + g * GROUP
        top = global_row == 0
        bottom = global_row == sp_size * grid_rows - GROUP
        slots = (
            jnp.where(top, 5, jnp.where(bottom, 3, 0)), 1,
            jnp.where(top, 4, jnp.where(bottom, 5, 2)),
        )
        kind = 1 if b == blocks - 1 else 0
        keys = jnp.concatenate([kv[s, :width] for s in strips(g, b)], axis=0)
        s = lax.dot_general(stacked(g, b), keys, contract, preferred_element_type=F32)
        for t in range(TILES):
            lanes = slice(t * LANES, (t + 1) * LANES)
            scores[b, :, lanes] = s[:, lanes] + table[kind, slots[t]]

    def score_far(g, b):
        scores[b, :, near_keys:] = lax.dot_general(
            stacked(g, b), ctx_kv[:, :width], contract, preferred_element_type=F32
        )

    def soften(b):
        sums = []
        for h in range(heads):
            rows = slice(h * size, (h + 1) * size)
            s = scores[b, rows, :]
            p = jnp.exp2(s - jnp.max(s, axis=1, keepdims=True))
            sums.append(jnp.sum(p, axis=1, keepdims=True))
            probs[b, rows, :] = p.astype(BF16)
        return [1.0 / total for total in sums]

    def merge(column, row=None):
        parts = []
        for c in range(width // LANES):
            low, high = 2 * c, 2 * c + 1
            if row is not None:
                lanes = slice(c * LANES, (c + 1) * LANES)
                first = row[low * size : (low + 1) * size, lanes]
                second = row[high * size : (high + 1) * size, lanes]
                if column is not None:
                    first, second = first * column[low], second * column[high]
            else:
                first, second = column[low], column[high]
            parts.append(jnp.where(first_head, first, second))
        return jnp.concatenate(parts, axis=1)

    def place_merged(g, b, merged):
        merged = merged.astype(BF16)
        for r, place in enumerate(places(g, b)):
            stage[place, :] = merged[r * BLOCK : (r + 1) * BLOCK]

    def mix(g, b, inverses):
        values = jnp.concatenate(
            [kv[s, width:] for s in strips(g, b)] + [ctx_kv[:, width:]], axis=0
        )
        mixed = jnp.dot(probs[b], values, preferred_element_type=F32)
        place_merged(g, b, merge(inverses, mixed))

    def head_rows(h):
        return slice(h * size, (h + 1) * size)

    def attend_near(g, b, slot):
        for h in range(heads):
            s = scores[b, head_rows(h), :near_keys]
            peak = jnp.max(s, axis=1, keepdims=True)
            p = jnp.exp2(s - peak)
            spread = (size, LANES)
            stats[slot, b, 0, head_rows(h), :] = jnp.broadcast_to(peak, spread)
            stats[slot, b, 1, head_rows(h), :] = jnp.broadcast_to(
                jnp.sum(p, axis=1, keepdims=True), spread
            )
            probs[b, head_rows(h), :near_keys] = p.astype(BF16)
        values = jnp.concatenate([kv[s, width:] for s in strips(g, b)], axis=0)
        mixed = jnp.dot(probs[b, :, :near_keys], values, preferred_element_type=F32)
        partial[slot, b] = merge(None, mixed)

    def attend_far(g, b, slot):
        keeps, inverses = [], []
        for h in range(heads):
            old = stats[slot, b, 0, head_rows(h), :]
            s = scores[b, head_rows(h), near_keys:]
            peak = jnp.maximum(old, jnp.max(s, axis=1, keepdims=True))
            p = jnp.exp2(s - jnp.concatenate([peak] * (s.shape[1] // LANES), axis=1))
            keep = jnp.exp2(old - peak)
            total = stats[slot, b, 1, head_rows(h), :] * keep
            total = total + jnp.sum(p, axis=1, keepdims=True)
            inverse = 1.0 / total
            inverses.append(inverse)
            keeps.append(keep * inverse)
            probs[b, head_rows(h), near_keys:] = p.astype(BF16)
        mixed = jnp.dot(
            probs[b, :, near_keys:], ctx_kv[:, width:], preferred_element_type=F32
        )
        place_merged(g, b, partial[slot, b] * merge(keeps) + merge(inverses, mixed))

    def piece_copy(index):
        owner, p = index // pieces, index % pieces
        return to_peer(
            stage.at[pl.ds(aligned(index, piece), piece)],
            recv.at[tp, pl.ds(aligned(p, piece), piece)],
            piece_send, piece_recv.at[tp, p], tp=owner,
        )

    half = groups // 2
    inner = half - 1

    def group_of(own, j):
        early = jnp.where(j == 0, 0, jnp.where(j == 1, inner, j - 1))
        low = (jnp.where(sp == 0, early, j) + 1) % half
        return jnp.where(upper != own, low, half + j)

    def send_pieces(g):
        for n in range(per_group):
            index = g * per_group + n

            @pl.when(index // pieces != tp)
            def _():
                piece_copy(index).start()

    @pl.loop(0, inner)
    def _(k):
        g = group_of(False, k)
        for b in range(blocks):
            score_near(g, b)
        for b in range(blocks):
            attend_near(g, b, k)

    others = ctx_kv.at[pl.ds(0, (sp_size - 1) * context_rows)]
    to_peer(others, others, ctx_send, ctx_recv, sp=(sp + 1) % sp_size).wait()

    @pl.loop(0, inner)
    def _(k):
        g = group_of(False, k)
        for b in range(blocks):
            score_far(g, b)
        for b in range(blocks):
            attend_far(g, b, k)
        send_pieces(g)

    project(unit(groups - 1), False)

    no_halo = jnp.where(upper, sp == 0, sp == sp_size - 1)
    turn = jnp.where(no_halo, 0, jnp.where(sp == 0, groups - inner - 1, inner))

    @pl.loop(0, groups - inner)
    def _(k):
        own = k != turn
        g = group_of(own, jnp.where(own, k - jnp.where(k > turn, 1, 0), inner))

        @pl.when((g == 0) & (sp > 0))
        def _():
            down.wait_send()
            up.wait_recv()

        @pl.when((g == groups - 1) & (sp < sp_size - 1))
        def _():
            up.wait_send()
            down.wait_recv()

        for b in range(blocks):
            score_near(g, b)
            score_far(g, b)
        for b in range(blocks):
            mix(g, b, soften(b))
        send_pieces(g)

    load_wo.wait()

    wait_all(garrived, gate_send, gate_recv)

    gates = []
    for t in range(tp_size):
        total = garrived[t]
        for s in range(1, sp_size):
            total = total + garrived[s * tp_size + t]
        gates.append(total)
    gate = jnp.concatenate(gates, axis=1)
    chips = tp_size // 2
    chip = tp // 2
    partner = tp + 1 - 2 * (tp % 2)

    def arrival(source, p):
        rows = pl.ds(aligned(p, piece), piece)
        return to_peer(
            stage.at[rows], recv.at[source, rows], piece_send,
            piece_recv.at[source, p], tp=source,
        )

    def product(c, rows):
        pair = jnp.concatenate([recv[2 * c, rows, :], recv[2 * c + 1, rows, :]], axis=1)
        return jnp.dot(
            pair, wo[pl.ds(aligned(c, 2 * width), 2 * width), :], preferred_element_type=F32
        )

    def landing(k):
        return jnp.where(tp == 0, (k + per_group) % pieces, k)

    @pl.loop(0, pieces)
    def _(k):
        p = landing(k)
        rows = pl.ds(aligned(p, piece), piece)
        recv[tp, rows, :] = stage[pl.ds(aligned(tp * pieces + p, piece), piece), :]
        arrival(partner, p).wait_recv()
        acc[rows, :] = product(chip, rows)

    @pl.loop(0, pieces)
    def _(k):
        p = landing(k)
        rows = pl.ds(aligned(p, piece), piece)
        own = pl.ds(aligned(tp * pieces + p, piece), piece)
        branch = acc[rows, :]
        for d in range(1, chips):
            c = (chip + d) % chips
            arrival(2 * c, p).wait_recv()
            arrival(2 * c + 1, p).wait_recv()
            branch = branch + product(c, rows)
        turned = []
        for r in range(piece_rows):
            turned.append(branch[(r + 1) * GRID_W - SHIFT : (r + 1) * GRID_W])
            turned.append(branch[r * GRID_W : (r + 1) * GRID_W - SHIFT])
        branch = jnp.concatenate(turned, axis=0)
        out_ref[rows, :] = (lat[own, :].astype(F32) + gate * branch).astype(BF16)

    sent = stage.at[pl.ds(0, tokens - share)]
    to_peer(sent, sent, piece_send, piece_recv.at[0, 0], tp=partner).wait_send()


def local(
    latent, condition, context_tokens, context_condition, shift_weight, scale_weight,
    gate_weight, norm_gain, query_weight, key_weight, value_weight, out_weight, offset_bias,
):
    sp_size, tp_size = lax.axis_size("sp"), lax.axis_size("tp")
    ranks = sp_size * tp_size
    tokens, depth = latent.shape
    context_rows = context_tokens.shape[0]
    input_rows, piece_cols = shift_weight.shape
    width = query_weight.shape[1]
    heads = width // HEAD_DIM
    groups = tokens // GRID_W // GROUP
    group_tokens = GROUP * GRID_W
    share = tokens // tp_size
    piece_rows = gcd(GROUP, share // GRID_W)
    pieces = share // (piece_rows * GRID_W)
    stacked = heads * GROUP * BLOCK
    keys = KEY_ROWS * STRIP + sp_size * context_rows
    bias = jnp.transpose(offset_bias, (1, 0, 2))
    dma = pltpu.SemaphoreType.DMA
    vmem = pltpu.VMEM
    hbm = pl.BlockSpec(memory_space=pl.ANY)
    return pl.pallas_call(
        kernel,
        in_specs=[hbm] * 13,
        out_specs=pl.BlockSpec(memory_space=pltpu.VMEM),
        out_shape=pltpu.VMEM((share, depth), BF16),
        scratch_shapes=[
            vmem((depth,), BF16), vmem((depth,), BF16), vmem((depth,), BF16),
            vmem((8, depth), F32),
            vmem((3, input_rows, piece_cols), BF16),
            vmem(bias.shape, F32),
            vmem((bias.shape[0], heads, LANES), F32),
            vmem((2, 6, heads * GROUP * BLOCK, LANES), F32),
            vmem((context_rows, depth), BF16),
            vmem((context_rows + 16, depth), BF16),
            vmem((tokens, depth), BF16),
            vmem((2 * group_tokens, depth), BF16),
            vmem((depth, 3 * width), BF16),
            vmem(out_weight.shape, BF16),
            vmem((2, piece_cols), BF16),
            vmem((ranks, 2, piece_cols), BF16),
            vmem((2, piece_cols), BF16),
            vmem((ranks, 2, piece_cols), BF16),
            vmem((1, piece_cols), F32),
            vmem((ranks, 1, piece_cols), F32),
            vmem((4, depth), F32),
            vmem((1, 3 * width), F32),
            vmem((tokens, LANES), F32),
            vmem((tokens, width), BF16),
            vmem((tokens + 2 * HALO * GRID_W, 2 * width), BF16),
            vmem((sp_size * context_rows, 2 * width), BF16),
            vmem((GRID_W // BLOCK, stacked, keys), F32),
            vmem((GRID_W // BLOCK, stacked, keys), BF16),
            vmem((groups // 2 - 1, GRID_W // BLOCK, GROUP * BLOCK, width), F32),
            vmem((groups // 2 - 1, GRID_W // BLOCK, 2, stacked, LANES), F32),
            vmem((tokens, width), BF16),
            vmem((tp_size, share, width), BF16),
            vmem((share, depth), F32),
            dma((8,)), dma((groups,)), dma, dma, dma, dma, dma, dma, dma((2,)), dma((2,)),
            dma, dma, dma, dma((tp_size, pieces)),
        ],
        compiler_params=pltpu.CompilerParams(
            vmem_limit_bytes=60 * 2**20, collective_id=0, has_side_effects=True
        ),
        cost_estimate=pl.CostEstimate(
            flops=6 * tokens * depth * width,
            bytes_accessed=2 * (tokens * depth + 3 * depth * width + share * depth),
            transcendentals=0,
        ),
    )(
        condition, context_condition, norm_gain, shift_weight, scale_weight, gate_weight, bias,
        context_tokens, latent, query_weight, key_weight, value_weight, out_weight,
    )


def solution(mesh):
    placed = (
        P(("grp", "sp"), None),
        P("grp"),
        P(("grp", "sp"), None),
        P(),
        P("sp", "tp"),
        P("sp", "tp"),
        P("sp", "tp"),
        P(),
        P(None, "tp"),
        P(None, "tp"),
        P(None, "tp"),
        P(),
        P("tp", None, None),
    )
    return jax.shard_map(
        local, mesh=mesh, in_specs=placed, out_specs=P(("grp", "sp", "tp"), None), check_vma=False
    )
```
